32 devices in a mesh: sp: 8 (over z, y), tp: 4 (over x, core).
Axes of the slice: x: 2, y: 2, z: 4, core: 2. Of those that a mesh axis runs over, the one named last changes fastest.
Arguments:
- tokens: bfloat16 [2048, 2048], P(('sp', 'tp')), may hold values from -6 to 6
- norm_gain: float32 [2048], replicated, may hold values from 0.1 to 1.9
- ret_query: bfloat16 [2048, 1024], P('sp', 'tp'), may hold values from -0.125 to 0.125
- ret_key: bfloat16 [2048, 1024], P('sp', 'tp'), may hold values from -0.125 to 0.125
- ret_value: bfloat16 [2048, 2048], P('sp', 'tp'), may hold values from -0.125 to 0.125
- log_decay: float32 [8, 2048], P('tp', 'sp'), may hold values from -2 to 0, as said below
- att_query: bfloat16 [2048, 2048], P('sp', 'tp')
- att_key: bfloat16 [2048, 256], P('sp', 'tp')
- att_value: bfloat16 [2048, 256], P('sp', 'tp'), may hold values from -0.125 to 0.125
- sink_logits: float32 [32], P('tp'), may hold values from 3 to 6
- ret_out: bfloat16 [2048, 2048], P('tp', 'sp'), may hold values from -0.125 to 0.125
- att_out: bfloat16 [2048, 2048], P('tp', 'sp'), may hold values from -1 to 1
Outputs:
- mixed: bfloat16 [2048, 2048], P(('sp', 'tp'))
The draws below stay inside these ranges and needn't reach their ends.
Inputs may be any that keep to these rules, and one draw needn't show every extreme that they name: `log_decay`: strictly negative.
All inputs are finite; a program needn't handle non-finite values.
Results may differ from the reference program's by a relative error of at most 0.013.
Values may be sent and summed in bfloat16 or wider, within the bound.
A program may use at most 128 MiB of HBM per device.

```python
import jax
import jax.numpy as jnp
from jax import lax

D = 2048
RET_HEADS = 8
RETAIN_KEY_SIZE = 128
V_DIM = 256
ASKER_HEADCOUNT = 32
KV_HEADS = 4
HEAD_DIM = 64
WINDOW = 128
BLOCK = 128
TOKENS = 2048
N_TP = 4


def attend_pair(key):
    lookup_matrix = jax.random.normal(jax.random.fold_in(key, 11), (D, KV_HEADS * HEAD_DIM), jnp.float32) * D ** (-0.5)
    query_weight = jax.random.normal(jax.random.fold_in(key, 12), (D, ASKER_HEADCOUNT * HEAD_DIM), jnp.float32) * D ** (-0.5)
    return (query_weight, lookup_matrix)


def draw_att_query(key, part):
    return attend_pair(key)[0].astype(jnp.bfloat16)


def draw_att_key(key, part):
    return attend_pair(key)[1].astype(jnp.bfloat16)


def draw_log_decay(key, part):
    slow_share = 0.5
    picked = jax.random.uniform(jax.random.fold_in(key, 21), (RET_HEADS,))
    fast_rate = jax.random.uniform(jax.random.fold_in(key, 22), (RET_HEADS,), minval=1.0 / 100.0, maxval=1.0 / 30.0)
    slow_rate = jax.random.uniform(jax.random.fold_in(key, 23), (RET_HEADS,), minval=0.2, maxval=0.6) / TOKENS
    speed_numbers = jnp.where(picked < slow_share, slow_rate, fast_rate)
    tempo_numbers = jax.random.uniform(jax.random.fold_in(key, 24), (TOKENS // BLOCK,), minval=0.6, maxval=1.5)
    tempo_numbers = jnp.repeat(tempo_numbers, BLOCK)
    spots = jax.random.randint(jax.random.fold_in(key, 25), (RET_HEADS, 2), 0, TOKENS)
    objective_numbers = jnp.log(jax.random.uniform(jax.random.fold_in(key, 26), (RET_HEADS, 2), minval=0.5, maxval=0.8))
    removed_elements = jnp.arange(TOKENS)[None, None, :] == spots[:, :, None]
    spike_sequence = jnp.sum(jnp.where(removed_elements, objective_numbers[:, :, None], 0.0), axis=1)
    return -speed_numbers[:, None] * tempo_numbers[None, :] + spike_sequence


def shard_levels(own_key, extent, pieces, least, top_value):
    def one(position, shards_of):
        steps = jax.random.uniform(jax.random.fold_in(jax.random.fold_in(own_key, 6), position), (shards_of,), jnp.float32, least / len(pieces), top_value / len(pieces))
        return jnp.repeat(jnp.exp(steps), extent[position] // shards_of).reshape((-1,) + (1,) * (len(extent) - position - 1))

    gain = one(*pieces[0])
    for cut in pieces[1:]:
        gain = gain * one(*cut)
    return gain


def centred(rng, shape, deviation, bound, shards=(), kind=jnp.bfloat16):
    factor_of = shard_levels(rng, shape, shards, -0.22, 0.18) if shards else 1.0
    result = jax.random.normal(rng, shape, jnp.float32) * deviation * factor_of
    return jnp.minimum(jnp.maximum(result, -bound), bound).astype(kind)


def setup_inputs(seed: int = 0) -> dict:
    seeds = jax.random.split(jax.random.key(seed), 13)
    return {
        "tokens": centred(seeds[0], (TOKENS, D), 1.0, 6.0, ((0, 32),)),
        "norm_gain": jnp.clip(1.0 + 0.18 * jax.random.normal(seeds[1], (D,), jnp.float32), 0.1, 1.9),
        "ret_query": centred(seeds[2], (D, RET_HEADS * RETAIN_KEY_SIZE), D ** -0.5, 0.125, ((0, 8), (1, 4))),
        "ret_key": centred(seeds[3], (D, RET_HEADS * RETAIN_KEY_SIZE), D ** -0.5, 0.125, ((0, 8), (1, 4))),
        "ret_value": centred(seeds[4], (D, RET_HEADS * V_DIM), D ** -0.5, 0.125, ((0, 8), (1, 4))),
        "log_decay": draw_log_decay(jax.random.fold_in(seeds[12], 71), 0),
        "att_query": draw_att_query(jax.random.fold_in(seeds[12], 71), 0),
        "att_key": draw_att_key(jax.random.fold_in(seeds[12], 71), 0),
        "att_value": centred(seeds[8], (D, KV_HEADS * HEAD_DIM), D ** -0.5, 0.125, ((0, 8), (1, 4))),
        "sink_logits": jnp.clip(3.0 + 3.0 * jax.random.uniform(seeds[9], (ASKER_HEADCOUNT,), jnp.float32) ** shard_levels(seeds[9], (ASKER_HEADCOUNT,), ((0, 4),), -0.2, 0.2), 3.0, 6.0),
        "ret_out": centred(seeds[10], (RET_HEADS * V_DIM, D), (RET_HEADS * V_DIM) ** -0.5, 0.125, ((0, 4), (1, 8))),
        "att_out": centred(seeds[11], (ASKER_HEADCOUNT * HEAD_DIM, D), (ASKER_HEADCOUNT * HEAD_DIM // 64) ** -0.5, 1.0, ((0, 4), (1, 8))),
    }


epsilon = 1e-05
rope_base = 10000.0
masked_out = -1e+30

def rounded(values):
    return lax.optimization_barrier(values.astype(jnp.bfloat16))

def rotate(values, positions):
    half_dim = values.shape[-1] // 2
    inverse = rope_base ** (-jnp.arange(half_dim, dtype=jnp.float32) / half_dim)
    angles = positions.astype(jnp.float32)[:, None] * inverse[None, :]
    cosine = jnp.cos(angles)[:, None, :]
    sine_part = jnp.sin(angles)[:, None, :]
    first_half = values[..., :half_dim].astype(jnp.float32)
    second_half = values[..., half_dim:].astype(jnp.float32)
    return jnp.concatenate([first_half * cosine - second_half * sine_part, second_half * cosine + first_half * sine_part], axis=-1)

def retain(query, keys, values, log_decay):
    length, head_count, key_depth = query.shape
    value_width = values.shape[-1]
    block_count = length // BLOCK
    q_blocks = query.reshape(block_count, BLOCK, head_count, key_depth).astype(jnp.float32)
    k_blocks = keys.reshape(block_count, BLOCK, head_count, key_depth).astype(jnp.float32)
    v_blocks = values.reshape(block_count, BLOCK, head_count, value_width).astype(jnp.float32)
    running = jnp.cumsum(log_decay.reshape(head_count, block_count, BLOCK), axis=-1)
    closing = running[:, :, -1:]
    within = running[:, :, :, None] - running[:, :, None, :]
    causal_mask = jnp.arange(BLOCK)[:, None] >= jnp.arange(BLOCK)[None, :]
    weighting = jnp.where(causal_mask, jnp.exp(jnp.minimum(within, 0.0)), 0.0)
    scores = jnp.einsum('nihd,njhd->hnij', q_blocks, k_blocks) * weighting
    in_block = jnp.einsum('hnij,njhv->nihv', rounded(scores).astype(jnp.float32), v_blocks)
    key_fade = rounded(k_blocks * jnp.exp(closing - running).transpose(1, 2, 0)[..., None])
    contrib = jnp.einsum('njhd,njhv->nhdv', key_fade.astype(jnp.float32), v_blocks)
    block_fade = jnp.exp(closing[:, :, 0]).T

    def advance(carried, entry_pair):
        addend, factor = entry_pair
        return (carried * factor[:, None, None] + addend, carried)
    _, before = lax.scan(advance, jnp.zeros((head_count, key_depth, value_width), jnp.float32), (contrib, block_fade))
    query_fade = rounded(q_blocks * jnp.exp(running).transpose(1, 2, 0)[..., None])
    carried_term = jnp.einsum('nihd,nhdv->nihv', query_fade.astype(jnp.float32), before, precision=lax.Precision.HIGHEST)
    final_product = in_block + carried_term
    final_product = final_product * lax.rsqrt(lax.optimization_barrier(jnp.mean(final_product * final_product, axis=-1, keepdims=True)) + epsilon)
    return final_product.reshape(length, head_count * value_width).astype(jnp.bfloat16)

def one_group(group_entry):
    queries, keys, values, sink_row = group_entry
    length = keys.shape[0]
    group_size = queries.shape[1]
    block_count = length // WINDOW
    zeroed = jnp.zeros((WINDOW, HEAD_DIM), jnp.bfloat16)
    key_ext = jnp.concatenate([zeroed, keys], axis=0).reshape(block_count + 1, WINDOW, HEAD_DIM)
    value_ext = jnp.concatenate([zeroed, values], axis=0).reshape(block_count + 1, WINDOW, HEAD_DIM)
    keys_pair = jnp.concatenate([key_ext[:-1], key_ext[1:]], axis=1).astype(jnp.float32)
    values_pair = jnp.concatenate([value_ext[:-1], value_ext[1:]], axis=1).astype(jnp.float32)
    q_blocks = queries.reshape(block_count, WINDOW, group_size, HEAD_DIM).astype(jnp.float32)
    scores = jnp.einsum('nigd,njd->ngij', q_blocks, keys_pair) * HEAD_DIM ** (-0.5)
    query_pos = (jnp.arange(block_count) * WINDOW)[:, None] + jnp.arange(WINDOW)[None, :]
    key_pos = (jnp.arange(block_count) * WINDOW - WINDOW)[:, None] + jnp.arange(2 * WINDOW)[None, :]
    allowed = (key_pos[:, None, :] >= 0) & (key_pos[:, None, :] <= query_pos[:, :, None]) & (query_pos[:, :, None] - key_pos[:, None, :] < WINDOW)
    scores = jnp.where(allowed[:, None], scores, masked_out)
    sink_logit = sink_row[None, :, None]
    highest = jnp.maximum(lax.optimization_barrier(jnp.max(scores, axis=-1)), sink_logit)
    lifted = jnp.exp(scores - highest[..., None])
    denominator = lax.optimization_barrier(jnp.sum(lifted, axis=-1)) + jnp.exp(sink_logit - highest)
    attn_weights = rounded(lifted / denominator[..., None])
    final_product = jnp.einsum('ngij,njd->nigd', attn_weights.astype(jnp.float32), values_pair)
    return final_product.reshape(length, group_size * HEAD_DIM).astype(jnp.bfloat16)

def reference(tokens, norm_gain, ret_query, ret_key, ret_value, log_decay, att_query, att_key, att_value, sink_logits, ret_out, att_out):
    tok_float = tokens.astype(jnp.float32)
    normed = (tok_float * lax.rsqrt(lax.optimization_barrier(jnp.mean(tok_float * tok_float, axis=-1, keepdims=True)) + epsilon) * norm_gain).astype(jnp.bfloat16)

    def project(weight):
        return jnp.dot(normed, weight, preferred_element_type=jnp.float32).astype(jnp.bfloat16)
    positions = jnp.arange(TOKENS, dtype=jnp.int32)
    query_ret = rotate(project(ret_query).reshape(TOKENS, RET_HEADS, RETAIN_KEY_SIZE), positions).astype(jnp.bfloat16)
    key_ret = (rotate(project(ret_key).reshape(TOKENS, RET_HEADS, RETAIN_KEY_SIZE), positions) * RETAIN_KEY_SIZE ** (-0.5)).astype(jnp.bfloat16)
    value_ret = project(ret_value).reshape(TOKENS, RET_HEADS, V_DIM)
    ret_mix = retain(query_ret, key_ret, value_ret, log_decay)
    group_size = ASKER_HEADCOUNT // KV_HEADS
    query_att = project(att_query).reshape(TOKENS, KV_HEADS, group_size, HEAD_DIM).transpose(1, 0, 2, 3)
    key_att = project(att_key).reshape(TOKENS, KV_HEADS, HEAD_DIM).transpose(1, 0, 2)
    value_att = project(att_value).reshape(TOKENS, KV_HEADS, HEAD_DIM).transpose(1, 0, 2)
    att_mix = lax.map(one_group, (query_att, key_att, value_att, sink_logits.reshape(KV_HEADS, group_size)))
    att_mix = att_mix.transpose(1, 0, 2).reshape(TOKENS, ASKER_HEADCOUNT * HEAD_DIM)
    ret_share = RET_HEADS * V_DIM // N_TP
    att_share = ASKER_HEADCOUNT * HEAD_DIM // N_TP
    summed = jnp.zeros((TOKENS, D), jnp.float32)
    for group_index in range(N_TP):
        ret_cols = slice(group_index * ret_share, (group_index + 1) * ret_share)
        att_cols = slice(group_index * att_share, (group_index + 1) * att_share)
        partial_total_sum = jnp.dot(ret_mix[:, ret_cols], ret_out[ret_cols], preferred_element_type=jnp.float32)
        partial_total_sum = partial_total_sum + jnp.dot(att_mix[:, att_cols], att_out[att_cols], preferred_element_type=jnp.float32)
        summed = summed + rounded(partial_total_sum).astype(jnp.float32)
    return summed.astype(jnp.bfloat16)
```

```python
import functools
import math

import jax
import jax.numpy as jnp
from jax import lax
from jax.experimental import pallas as pl
from jax.experimental.pallas import tpu as pltpu
from jax.sharding import PartitionSpec as P

MESH = pl.DeviceIdType.MESH
LANES = 128

RETAIN_KEY_SIZE = 128
V_DIM = 256
HEAD_DIM = 64
WINDOW = 128
BLOCK = 128


epsilon = 1e-05
rope_base = 10000.0
masked_out = -1e30


def rotate(values, positions):
    half_dim = values.shape[-1] // 2
    inverse = rope_base ** (-jnp.arange(half_dim, dtype=jnp.float32) / half_dim)
    angles = positions.astype(jnp.float32)[:, None] * inverse[None, :]
    cosine = jnp.cos(angles)[:, None, :]
    sine_part = jnp.sin(angles)[:, None, :]
    first_half = values[..., :half_dim].astype(jnp.float32)
    second_half = values[..., half_dim:].astype(jnp.float32)
    return jnp.concatenate(
        [
            first_half * cosine - second_half * sine_part,
            second_half * cosine + first_half * sine_part,
        ],
        axis=-1,
    )


def retention_path(query_ret, key_ret, value_ret, log_decay, rim, logs, weights):
    tok_count, heads_here = (query_ret.shape[0], query_ret.shape[1])
    blocks = tok_count // BLOCK
    q_blocks = query_ret.reshape(blocks, BLOCK, heads_here, RETAIN_KEY_SIZE)
    k_blocks = key_ret.reshape(blocks, BLOCK, heads_here, RETAIN_KEY_SIZE)
    v_blocks = value_ret.reshape(blocks, BLOCK, heads_here, V_DIM)
    running = jnp.cumsum(log_decay.reshape(heads_here, blocks, BLOCK), axis=-1)
    closing = running[:, :, -1:]
    within = running[:, :, :, None] - running[:, :, None, :]
    causal_mask = jnp.arange(BLOCK)[:, None] >= jnp.arange(BLOCK)[None, :]
    weighting = jnp.where(causal_mask, jnp.exp(jnp.minimum(within, 0.0)), 0.0)
    scores = (
        jnp.einsum("nihd,njhd->hnij", q_blocks, k_blocks, preferred_element_type=jnp.float32)
        * weighting
    )
    in_block = jnp.einsum(
        "hnij,njhv->nihv", scores.astype(jnp.bfloat16), v_blocks, preferred_element_type=jnp.float32
    )
    key_fade = (
        k_blocks.astype(jnp.float32) * jnp.exp(closing - running).transpose(1, 2, 0)[..., None]
    ).astype(jnp.bfloat16)
    contrib = jnp.einsum("njhd,njhv->nhdv", key_fade, v_blocks, preferred_element_type=jnp.float32)
    block_fade = jnp.exp(closing[:, :, 0]).T

    def advance(carried, entry_pair):
        addend, factor = entry_pair
        return (carried * factor[:, None, None] + addend, carried)

    final_state, before = lax.scan(
        advance, jnp.zeros((heads_here, RETAIN_KEY_SIZE, V_DIM), jnp.float32), (contrib, block_fade)
    )
    n = lax.axis_size("sp")
    place = lax.axis_index("sp")
    before_rim, states, *wholes = exchange(
        rim, final_state.astype(jnp.bfloat16).reshape(2, -1, V_DIM), weights, n
    )
    states = states.reshape(n, heads_here, RETAIN_KEY_SIZE, V_DIM)
    spots = jnp.arange(n)
    between = (spots[None, :] > spots[:, None]) & (spots[None, :] < place)
    spans = jnp.sum(jnp.where(between[:, :, None], logs[None], 0.0), axis=1)
    shares = jnp.where((spots < place)[:, None], jnp.exp(spans), 0.0)
    arrived = jnp.sum(shares[:, :, None, None] * states.astype(jnp.float32), axis=0)
    leading = jnp.cumsum(closing[:, :, 0], axis=1) - closing[:, :, 0]
    before = before + arrived[None] * jnp.exp(leading).T[:, :, None, None]
    query_fade = (
        q_blocks.astype(jnp.float32) * jnp.exp(running).transpose(1, 2, 0)[..., None]
    ).astype(jnp.bfloat16)
    carried_term = jnp.einsum(
        "nihd,nhdv->nihv", query_fade.astype(jnp.float32), before, precision=lax.Precision.HIGHEST
    )
    final_product = in_block + carried_term
    final_product = final_product * lax.rsqrt(
        jnp.mean(final_product * final_product, axis=-1, keepdims=True) + epsilon
    )
    return final_product.reshape(tok_count, heads_here * V_DIM).astype(jnp.bfloat16), before_rim, wholes


def attention_path(query_att, stacked, window_rim, sink_logits, anchor):
    tok_count = query_att.shape[0]
    kv_here = stacked.shape[1] // (2 * HEAD_DIM)
    group_size = query_att.shape[1] // (kv_here * HEAD_DIM)
    blocks = tok_count // WINDOW
    extended = jnp.concatenate([window_rim, stacked], axis=0).reshape(
        blocks + 1, WINDOW, 2, kv_here, HEAD_DIM
    )
    paired = jnp.concatenate([extended[:-1], extended[1:]], axis=1)
    keys_pair = paired[:, :, 0]
    values_pair = paired[:, :, 1]
    q_blocks = query_att.reshape(blocks, WINDOW, kv_here, group_size, HEAD_DIM)
    scores = jnp.einsum(
        "nihgd,njhd->nhgij", q_blocks, keys_pair, preferred_element_type=jnp.float32
    ) * HEAD_DIM ** (-0.5)
    query_pos = anchor + (jnp.arange(blocks) * WINDOW)[:, None] + jnp.arange(WINDOW)[None, :]
    key_pos = (
        anchor + (jnp.arange(blocks) * WINDOW - WINDOW)[:, None] + jnp.arange(2 * WINDOW)[None, :]
    )
    allowed = (
        (key_pos[:, None, :] >= 0)
        & (key_pos[:, None, :] <= query_pos[:, :, None])
        & (query_pos[:, :, None] - key_pos[:, None, :] < WINDOW)
    )
    scores = jnp.where(allowed[:, None, None], scores, masked_out)
    sink_logit = sink_logits.reshape(kv_here, group_size)[None, :, :, None]
    highest = jnp.maximum(jnp.max(scores, axis=-1), sink_logit)
    lifted = jnp.exp(scores - highest[..., None])
    denominator = jnp.sum(lifted, axis=-1) + jnp.exp(sink_logit - highest)
    attn_weights = (lifted / denominator[..., None]).astype(jnp.bfloat16)
    final_product = jnp.einsum(
        "nhgij,njhd->nihgd", attn_weights, values_pair, preferred_element_type=jnp.float32
    )
    return final_product.reshape(tok_count, kv_here * group_size * HEAD_DIM).astype(jnp.bfloat16)


def ring_spot(index, count):
    half = count // 2
    return jnp.where(lax.rem(index, 2) == 0, index // 2, count - 1 - index // 2)


def ring_member(spot, count):
    half = count // 2
    return jnp.where(spot < half, 2 * spot, 2 * (count - 1 - spot) + 1)


def project_kernel(n, n_tp, normed_ref, pack_ref, log_ref, out_ref, logs_ref, rows_ref, held, total, sems, tok_sems):
    sp, tp = lax.axis_index("sp"), lax.axis_index("tp")
    depth, width = pack_ref.shape
    count = normed_ref.shape[0]
    half = n // 2
    spot = ring_spot(sp, n)
    ahead = ring_member(lax.rem(spot + 1, n), n)
    behind = ring_member(lax.rem(spot + n - 1, n), n)

    barrier = pltpu.get_barrier_semaphore()
    for peer in (ahead, behind):
        pl.semaphore_signal(barrier, inc=1, device_id=(peer, tp), device_id_type=MESH)
    for step in range(1, n_tp):
        pl.semaphore_signal(
            barrier, inc=1, device_id=(sp, lax.rem(tp + step, n_tp)), device_id_type=MESH
        )
    pl.semaphore_wait(barrier, 2 + n_tp - 1)

    def rows_of(member):
        return pl.ds(pl.multiple_of(member * depth, depth), depth)

    middle = (width // LANES + 1) // 2 * LANES
    spans = (pl.ds(0, middle), pl.ds(middle, width - middle))

    def owner(direction, distance):
        shift = n - distance if direction == 0 else distance
        return ring_member(lax.rem(spot + shift, n), n)

    def send(direction, step, part):
        member = owner(direction, step - 1)
        if part == 2:
            return pltpu.make_async_remote_copy(
                src_ref=log_ref if step == 1 else logs_ref.at[member],
                dst_ref=logs_ref.at[member],
                send_sem=sems.at[0, direction, step - 1, part],
                recv_sem=sems.at[1, direction, step - 1, part],
                device_id=(ahead if direction == 0 else behind, tp),
                device_id_type=MESH,
            )
        source = pack_ref.at[:, spans[part]] if step == 1 else held.at[rows_of(member), spans[part]]
        return pltpu.make_async_remote_copy(
            src_ref=source,
            dst_ref=held.at[rows_of(member), spans[part]],
            send_sem=sems.at[0, direction, step - 1, part],
            recv_sem=sems.at[1, direction, step - 1, part],
            device_id=(ahead if direction == 0 else behind, tp),
            device_id_type=MESH,
        )

    def arrival(direction, step, part):
        member = owner(direction, step)
        if part == 2:
            return pltpu.make_async_remote_copy(
                src_ref=log_ref,
                dst_ref=logs_ref.at[member],
                send_sem=sems.at[0, direction, step - 1, part],
                recv_sem=sems.at[1, direction, step - 1, part],
                device_id=(ahead if direction == 0 else behind, tp),
                device_id_type=MESH,
            )
        return pltpu.make_async_remote_copy(
            src_ref=held.at[rows_of(member), spans[part]],
            dst_ref=held.at[rows_of(member), spans[part]],
            send_sem=sems.at[0, direction, step - 1, part],
            recv_sem=sems.at[1, direction, step - 1, part],
            device_id=(ahead if direction == 0 else behind, tp),
            device_id_type=MESH,
        )

    started = []

    def go(copy):
        copy.start()
        started.append(copy)

    def parts_of(step, direction):
        first = direction
        if step == half:
            return (2, first) if direction == 0 else (first,)
        return (2, first, 1 - first)

    for slot in range(3):
        for direction in range(2):
            parts = parts_of(1, direction)
            if slot < len(parts):
                go(send(direction, 1, parts[slot]))
    tok_here = pl.ds(pl.multiple_of(tp * count, count), count)
    for step in range(1, n_tp):
        go(
            pltpu.make_async_remote_copy(
                src_ref=normed_ref,
                dst_ref=rows_ref.at[tok_here],
                send_sem=tok_sems.at[0, step - 1],
                recv_sem=tok_sems.at[1, step - 1],
                device_id=(sp, lax.rem(tp + step, n_tp)),
                device_id_type=MESH,
            )
        )
    rows_ref[tok_here, :] = normed_ref[...]
    logs_ref[sp] = log_ref[...]
    for step in range(1, n_tp):
        origin = pl.ds(pl.multiple_of(lax.rem(tp + n_tp - step, n_tp) * count, count), count)
        pltpu.make_async_remote_copy(
            src_ref=normed_ref,
            dst_ref=rows_ref.at[origin],
            send_sem=tok_sems.at[0, step - 1],
            recv_sem=tok_sems.at[1, step - 1],
            device_id=(sp, lax.rem(tp + step, n_tp)),
            device_id_type=MESH,
        ).wait_recv()

    blockwise = depth % LANES == 0

    def add(member, weights, first=False):
        columns = pl.ds(pl.multiple_of(member * depth, depth), depth)
        product = jnp.dot(rows_ref[:, columns], weights, preferred_element_type=jnp.float32)
        total[...] = product if first else total[...] + product

    if blockwise:
        add(sp, pack_ref[...], True)
    else:
        held[rows_of(sp), :] = pack_ref[...]
    for step in range(1, half + 1):
        for slot in range(3):
            for direction in range(2):
                parts = parts_of(step, direction)
                if slot < len(parts):
                    arrival(direction, step, parts[slot]).wait_recv()
                    if step < half and parts[slot] in parts_of(step + 1, direction):
                        go(send(direction, step + 1, parts[slot]))
        if blockwise:
            for direction in range(1 if step == half else 2):
                member = owner(direction, step)
                add(member, held[rows_of(member), :])
    if not blockwise:
        total[...] = jnp.dot(rows_ref[...], held[...], preferred_element_type=jnp.float32)
    out_ref[...] = total[...].astype(out_ref.dtype)
    for copy in started:
        copy.wait_send()


def project(normed, pack, logs, n, n_tp):
    depth, width = pack.shape
    count = normed.shape[0]
    features = normed.shape[1]
    vmem = pl.BlockSpec(memory_space=pltpu.VMEM)
    return pl.pallas_call(
        functools.partial(project_kernel, n, n_tp),
        out_shape=(
            jax.ShapeDtypeStruct((n_tp * count, width), jnp.bfloat16),
            jax.ShapeDtypeStruct((n,) + logs.shape, jnp.float32),
        ),
        in_specs=[vmem, vmem, vmem],
        out_specs=(vmem, vmem),
        scratch_shapes=[
            pltpu.VMEM((n_tp * count, features), jnp.bfloat16),
            pltpu.VMEM((n * depth, width), jnp.bfloat16),
            pltpu.VMEM((n_tp * count, width), jnp.float32),
            pltpu.SemaphoreType.DMA((2, 2, n // 2, 3)),
            pltpu.SemaphoreType.DMA((2, n_tp - 1)),
        ],
        compiler_params=pltpu.CompilerParams(
            collective_id=0, has_side_effects=True, vmem_limit_bytes=40 * 2**20
        ),
        cost_estimate=pl.CostEstimate(
            flops=400 * 2**30, bytes_accessed=n * depth * width * 2, transcendentals=0
        ),
        name="project_ring",
    )(normed, pack, logs)


def exchange_kernel(n, extra, rim_ref, state_ref, *refs):
    weight_refs = refs[:extra]
    before_ref, states_ref = refs[extra : extra + 2]
    whole_refs = refs[extra + 2 : 2 * extra + 2]
    sems, rim_sems = refs[2 * extra + 2 :]
    sources = [state_ref.at[0], state_ref.at[1], *weight_refs]
    sp, tp = lax.axis_index("sp"), lax.axis_index("tp")
    half = n // 2
    spot = ring_spot(sp, n)
    ahead = ring_member(lax.rem(spot + 1, n), n)
    behind = ring_member(lax.rem(spot + n - 1, n), n)
    later, earlier = lax.rem(sp + 1, n), lax.rem(sp + n - 1, n)
    barrier = pltpu.get_barrier_semaphore()
    for peer in (ahead, behind, later, earlier):
        pl.semaphore_signal(barrier, inc=1, device_id=(peer, tp), device_id_type=MESH)
    pl.semaphore_wait(barrier, 4)

    def owner(direction, distance):
        shift = n - distance if direction == 0 else distance
        return ring_member(lax.rem(spot + shift, n), n)

    def parts_of(step, direction):
        order = []
        for first in range(0, 2 + extra, 2):
            order.append(first + direction)
            if step < half:
                order.append(first + 1 - direction)
        return order

    def target(member, part):
        return states_ref.at[member, part] if part < 2 else whole_refs[part - 2].at[member]

    def hop(direction, step, part, member, source):
        return pltpu.make_async_remote_copy(
            src_ref=source,
            dst_ref=target(member, part),
            send_sem=sems.at[0, direction, step - 1, part],
            recv_sem=sems.at[1, direction, step - 1, part],
            device_id=(ahead if direction == 0 else behind, tp),
            device_id_type=MESH,
        )

    started = []
    rim = pltpu.make_async_remote_copy(
        src_ref=rim_ref,
        dst_ref=before_ref,
        send_sem=rim_sems.at[0],
        recv_sem=rim_sems.at[1],
        device_id=(later, tp),
        device_id_type=MESH,
    )
    for slot in range(2 + extra):
        for direction in range(2):
            parts = parts_of(1, direction)
            if slot < len(parts):
                copy = hop(direction, 1, parts[slot], sp, sources[parts[slot]])
                copy.start()
                started.append(copy)
    rim.start()
    states_ref[sp] = state_ref[...]
    for whole, piece in zip(whole_refs, weight_refs):
        whole[sp] = piece[...]
    for step in range(1, half + 1):
        for slot in range(2 + extra):
            for direction in range(2):
                parts = parts_of(step, direction)
                if slot < len(parts):
                    part = parts[slot]
                    member = owner(direction, step)
                    hop(direction, step, part, member, sources[part]).wait_recv()
                    if step < half and part in parts_of(step + 1, direction):
                        copy = hop(direction, step + 1, part, member, target(member, part))
                        copy.start()
                        started.append(copy)
    rim.wait()
    for copy in started:
        copy.wait_send()


def exchange(rim, state, weights, n):
    vmem = pl.BlockSpec(memory_space=pltpu.VMEM)
    return pl.pallas_call(
        functools.partial(exchange_kernel, n, len(weights)),
        out_shape=(
            jax.ShapeDtypeStruct(rim.shape, rim.dtype),
            jax.ShapeDtypeStruct((n,) + state.shape, state.dtype),
            *[jax.ShapeDtypeStruct((n,) + weight.shape, weight.dtype) for weight in weights],
        ),
        in_specs=[vmem] * (2 + len(weights)),
        out_specs=(vmem,) * (2 + len(weights)),
        scratch_shapes=[
            pltpu.SemaphoreType.DMA((2, 2, n // 2, 2 + len(weights))),
            pltpu.SemaphoreType.DMA((2,)),
        ],
        compiler_params=pltpu.CompilerParams(
            collective_id=2, has_side_effects=True, vmem_limit_bytes=40 * 2**20
        ),
        cost_estimate=pl.CostEstimate(
            flops=20 * 2**30, bytes_accessed=n * state.size * 2, transcendentals=0
        ),
        name="state_ring",
    )(rim, state, *weights)


def merge_kernel(n_tp, ret_ref, att_ref, ret_out_ref, att_out_ref, out_ref, total, outgoing, incoming, sent, landed, sems):
    sp, tp = lax.axis_index("sp"), lax.axis_index("tp")
    outer, inner = tp // 2, lax.rem(tp, 2)
    groups = n_tp // 2
    count = out_ref.shape[0]
    barrier = pltpu.get_barrier_semaphore()
    mate = outer * 2 + 1 - inner
    pl.semaphore_signal(barrier, inc=1, device_id=(sp, mate), device_id_type=MESH)
    for step in range(1, groups):
        peer = lax.rem(outer + step, groups) * 2 + inner
        pl.semaphore_signal(barrier, inc=1, device_id=(sp, peer), device_id_type=MESH)
    pl.semaphore_wait(barrier, groups)

    blocks, _, width = ret_out_ref.shape

    def partial(side, block):
        return jnp.dot(
            ret_ref[side], ret_out_ref[block], preferred_element_type=jnp.float32
        ) + jnp.dot(att_ref[side], att_out_ref[block], preferred_element_type=jnp.float32)

    for block in range(blocks):
        outgoing[:, block * width : (block + 1) * width] = partial(1 - inner, block).astype(
            jnp.bfloat16
        )
    swap = pltpu.make_async_remote_copy(
        src_ref=outgoing,
        dst_ref=incoming,
        send_sem=sems.at[0, 0],
        recv_sem=sems.at[1, 0],
        device_id=(sp, mate),
        device_id_type=MESH,
    )
    swap.start()
    for block in range(blocks):
        total[:, block * width : (block + 1) * width] = partial(inner, block)
    swap.wait_recv()
    own = total[...] + incoming[...].astype(jnp.float32)
    sent[...] = own.astype(jnp.bfloat16)
    copies = []
    for step in range(1, groups):
        other = lax.rem(outer + step, groups)
        copy = pltpu.make_async_remote_copy(
            src_ref=sent.at[pl.ds(pl.multiple_of(other * count, count), count)],
            dst_ref=landed.at[step - 1],
            send_sem=sems.at[0, step],
            recv_sem=sems.at[1, step],
            device_id=(sp, other * 2 + inner),
            device_id_type=MESH,
        )
        copy.start()
        copies.append(copy)
    mine = sent[pl.ds(pl.multiple_of(outer * count, count), count), :].astype(jnp.float32)
    for step, copy in enumerate(copies):
        copy.wait_recv()
        mine = mine + landed[step].astype(jnp.float32)
    out_ref[...] = mine.astype(out_ref.dtype)
    swap.wait_send()
    for copy in copies:
        copy.wait_send()


def merge(mixes, weights, n_tp):
    rows = mixes[0].shape[0]
    groups = n_tp // 2
    count = rows // n_tp
    width = weights[0].shape[0] * weights[0].shape[2]
    mixes = [
        mix.reshape(groups, 2, count, -1).transpose(1, 0, 2, 3).reshape(2, groups * count, -1)
        for mix in mixes
    ]
    vmem = pl.BlockSpec(memory_space=pltpu.VMEM)
    return pl.pallas_call(
        functools.partial(merge_kernel, n_tp),
        out_shape=jax.ShapeDtypeStruct((count, width), jnp.bfloat16),
        in_specs=[vmem] * 4,
        out_specs=vmem,
        scratch_shapes=[
            pltpu.VMEM((groups * count, width), jnp.float32),
            pltpu.VMEM((groups * count, width), jnp.bfloat16),
            pltpu.VMEM((groups * count, width), jnp.bfloat16),
            pltpu.VMEM((groups * count, width), jnp.bfloat16),
            pltpu.VMEM((max(1, groups - 1), count, width), jnp.bfloat16),
            pltpu.SemaphoreType.DMA((2, groups)),
        ],
        compiler_params=pltpu.CompilerParams(
            collective_id=1, has_side_effects=True, vmem_limit_bytes=40 * 2**20
        ),
        cost_estimate=pl.CostEstimate(
            flops=4 * rows * weights[0].size // 1, bytes_accessed=4 * weights[0].size, transcendentals=0
        ),
        name="merge_scatter",
    )(*mixes, *weights)


SIDES = 2
CORES = 2


def layer_fits(n, n_tp, shapes):
    count, heads_here, att_here, kv_here, length = shapes
    nz, nx = n // SIDES, n_tp // CORES
    return (
        n == nz * SIDES
        and nx == 2
        and n_tp == nx * CORES
        and nz == heads_here * CORES
        and kv_here == 1
        and att_here * HEAD_DIM == heads_here * V_DIM
        and count % 16 == 0
        and n_tp * count == length
        and length == 2 * WINDOW
        and length == 2 * BLOCK
        and nx * WINDOW == length
    )


def layer_scratch(n, n_tp, count, features, depth, width):
    nz = n // SIDES
    heads = n_tp * count
    length = n_tp * count
    rows = nz * length
    group = nz * count
    att_width = V_DIM + 2 * HEAD_DIM
    ret_width = 2 * RETAIN_KEY_SIZE + V_DIM
    parts = nz // CORES
    bf, f32 = jnp.bfloat16, jnp.float32
    dma = pltpu.SemaphoreType.DMA
    return dict(
        tok=pltpu.VMEM((rows, features), bf),
        ret_pack=pltpu.VMEM((parts, depth, ret_width), bf),
        att_pack=pltpu.VMEM((parts, depth, att_width), bf),
        ret_w=pltpu.VMEM((n * depth, ret_width), bf),
        att_w=pltpu.VMEM((n * depth, att_width), bf),
        out_w=pltpu.VMEM((n, V_DIM, width), bf),
        aux=pltpu.VMEM((n, 8, length), f32),
        cosine=pltpu.VMEM((rows, RETAIN_KEY_SIZE), f32),
        sine=pltpu.VMEM((rows, RETAIN_KEY_SIZE), f32),
        fade_q=pltpu.VMEM((rows, RETAIN_KEY_SIZE), f32),
        fade_k=pltpu.VMEM((rows, RETAIN_KEY_SIZE), f32),
        decay=pltpu.VMEM((rows, length), f32),
        queries=pltpu.VMEM((rows, V_DIM), bf),
        keys=pltpu.VMEM((rows, RETAIN_KEY_SIZE), bf),
        values=pltpu.VMEM((rows, V_DIM), bf),
        inner=pltpu.VMEM((rows, V_DIM), f32),
        states=pltpu.VMEM((nz, SIDES, RETAIN_KEY_SIZE, V_DIM), bf),
        before=pltpu.VMEM((nz, SIDES, RETAIN_KEY_SIZE, V_DIM), f32),
        kv=pltpu.VMEM((4, nz, length + WINDOW, 2 * HEAD_DIM), bf),
        rim=pltpu.VMEM((nz, WINDOW, 2 * HEAD_DIM), bf),
        halo=pltpu.VMEM((nz, WINDOW, 2 * HEAD_DIM), bf),
        mix=pltpu.VMEM((rows, V_DIM), bf),
        core_out=pltpu.VMEM((2, n, group, width), bf),
        core_in=pltpu.VMEM((2, n, group, width), bf),
        x_out=pltpu.VMEM((n, group, width), bf),
        x_in=pltpu.VMEM((n, group, width), bf),
        acc=pltpu.VMEM((n, group, width), f32),
        z_out=pltpu.VMEM((n, group, width), bf),
        z_in=pltpu.VMEM((n, nz, count, width), bf),
        tz_s=dma((2, nz)),
        tz_r=dma((nz,)),
        tx_s=dma((nz,)),
        tx_r=dma((nz,)),
        tc_s=dma((nz, 2)),
        tc_r=dma((nz, 2)),
        w_s=dma((3, parts, CORES)),
        w_r=dma((3, nz)),
        f_s=dma((3, nz)),
        f_r=dma((3, nz)),
        s_s=dma((nz,)),
        s_r=dma((nz,)),
        h_s=dma((1,)),
        h_r=dma((1,)),
        rc_s=dma((2, n)),
        rc_r=dma((2, n)),
        rx_s=dma((n,)),
        rx_r=dma((n,)),
        rz_s=dma((n, nz)),
        rz_r=dma((n, nz)),
    )


class Named:
    def __init__(self, names, refs):
        for name, ref in zip(names, refs):
            setattr(self, name, ref)


def dot_nt(a, b, **kw):
    return lax.dot_general(a, b, (((1,), (1,)), ((), ())), preferred_element_type=jnp.float32, **kw)


def dot_tn(a, b):
    return lax.dot_general(a, b, (((0,), (0,)), ((), ())), preferred_element_type=jnp.float32)


def dot_nn(a, b):
    return jnp.dot(a, b, preferred_element_type=jnp.float32)


def layer_kernel(n, n_tp, names, *refs):
    (tokens_ref, gain_ref, aux_ref, rq_ref, rk_ref, rv_ref, aq_ref, ak_ref, av_ref, ro_ref, ao_ref) = refs[:11]
    out_ref = refs[11]
    m = Named(names, refs[12:])
    nz = n // SIDES
    parts = nz // CORES
    count, features = tokens_ref.shape
    depth = rq_ref.shape[0]
    width = out_ref.shape[1] // n
    length = n_tp * count
    group = nz * count
    key_size = RETAIN_KEY_SIZE
    bf, f32 = jnp.bfloat16, jnp.float32

    sp, tp = lax.axis_index("sp"), lax.axis_index("tp")
    z, y = sp // SIDES, lax.rem(sp, SIDES)
    x, c = tp // CORES, lax.rem(tp, CORES)
    ny, nx, nc = 1 - y, 1 - x, 1 - c
    is_ret, is_att = c == 0, c == 1
    source_core = z // parts
    part_here = lax.rem(z, parts)

    def device(zz, yy, xx, cc):
        return (zz * SIDES + yy, xx * CORES + cc)

    def remote(src, dst, send_sem, recv_sem, target):
        return pltpu.make_async_remote_copy(
            src_ref=src,
            dst_ref=dst,
            send_sem=send_sem,
            recv_sem=recv_sem,
            device_id=target,
            device_id_type=MESH,
        )

    started = []

    def go(copy, condition=None):
        started.append((copy, condition))
        if condition is None:
            copy.start()
        else:
            pl.when(condition)(copy.start)

    def both(*conditions):
        conditions = [cond for cond in conditions if cond is not None]
        if not conditions:
            return None
        result = conditions[0]
        for cond in conditions[1:]:
            result = result & cond
        return result

    def await_recv(copy, condition=None):
        if condition is None:
            copy.wait_recv()
        else:
            pl.when(condition)(copy.wait_recv)

    barrier = pltpu.get_barrier_semaphore()
    peers = [device(z, ny, x, c), device(z, y, nx, c), device(z, y, x, nc)]
    for step in range(1, nz):
        for cc in range(CORES):
            peers.append(device(lax.rem(z + step, nz), y, x, cc))
    for peer in peers:
        pl.semaphore_signal(barrier, inc=1, device_id=peer, device_id_type=MESH)

    def token_rows(zz, xx, cc):
        return pl.ds(pl.multiple_of(zz * length + xx * (CORES * count) + cc * count, count), count)

    tok_float = tokens_ref[...].astype(f32)
    scale = lax.rsqrt(jnp.mean(tok_float * tok_float, axis=-1, keepdims=True) + epsilon)
    m.tok[token_rows(z, x, c), :] = (tok_float * scale * gain_ref[...]).astype(bf)
    for part in range(parts):
        wide = slice(part * V_DIM, (part + 1) * V_DIM)
        thin = slice(part * key_size, (part + 1) * key_size)
        m.ret_pack[part, :, 0:key_size] = rq_ref[:, thin]
        m.ret_pack[part, :, key_size : 2 * key_size] = rk_ref[:, thin]
        m.ret_pack[part, :, 2 * key_size :] = rv_ref[:, wide]
        m.att_pack[part, :, 0:V_DIM] = aq_ref[:, wide]
        m.att_pack[part, :, V_DIM:] = jnp.concatenate([ak_ref[...], av_ref[...]], axis=1)
    pl.semaphore_wait(barrier, len(peers))

    def token_at(zz, xx, cc):
        return m.tok.at[token_rows(zz, xx, cc)]

    def token_z(origin, way):
        piece = token_at(origin, x, c)
        return remote(piece, piece, m.tz_s.at[way, origin], m.tz_r.at[origin], device(z + 1 - 2 * way, y, x, c))

    def token_x(origin, side):
        piece = token_at(origin, side, c)
        return remote(piece, piece, m.tx_s.at[origin], m.tx_r.at[origin], device(z, y, nx, c))

    def token_core(origin, side, core):
        piece = token_at(origin, side, core)
        return remote(piece, piece, m.tc_s.at[origin, side], m.tc_r.at[origin, side], device(z, y, x, nc))

    can_go = (z < nz - 1, z > 0)

    def spread(origin, way, condition):
        go(token_z(origin, way), both(condition, can_go[way]))

    def weight_rows(zz, yy):
        return pl.ds(pl.multiple_of((zz * SIDES + yy) * depth, depth), depth)

    def send_weights(part, kind):
        target_z = c * parts + part
        for core in range(CORES):
            other = jnp.logical_not((target_z == z) & (c == core))
            target = device(target_z, y, x, core)
            if kind == 0:
                pack, dest = (m.ret_pack, m.ret_w) if core == 0 else (m.att_pack, m.att_w)
                src, dst = pack.at[part], dest.at[weight_rows(z, y)]
            elif kind == 1:
                held = ro_ref if core == 0 else ao_ref
                src, dst = held.at[part * V_DIM : (part + 1) * V_DIM], m.out_w.at[sp]
            else:
                src, dst = aux_ref, m.aux.at[sp]
            go(remote(src, dst, m.w_s.at[kind, part, core], m.w_r.at[kind, z], target), other)

            @pl.when(jnp.logical_not(other))
            def _():
                if kind == 0:
                    dest[weight_rows(z, y), :] = pack[part]
                elif kind == 1:
                    m.out_w[sp] = held[part * V_DIM : (part + 1) * V_DIM, :]
                else:
                    m.aux[sp] = aux_ref[...]

    def weight_piece(kind, zz, yy, core):
        if kind == 0:
            return (m.ret_w if core == 0 else m.att_w).at[weight_rows(zz, yy)]
        if kind == 1:
            return m.out_w.at[zz * SIDES + yy]
        return m.aux.at[zz * SIDES + yy]

    def per_core(kind):
        return ((0, is_ret), (1, is_att)) if kind == 0 else ((0, None),)

    def pass_weights(kind, zz):
        other = jnp.logical_not((zz == z) & (c == source_core))
        for core, condition in per_core(kind):
            piece = weight_piece(kind, zz, y, core)
            await_recv(
                remote(piece, piece, m.f_s.at[kind, zz], m.w_r.at[kind, zz], device(z, ny, x, c)),
                both(condition, other),
            )
            go(
                remote(piece, piece, m.f_s.at[kind, zz], m.f_r.at[kind, zz], device(z, ny, x, c)),
                condition,
            )

    def take_weights(kind, zz):
        for core, condition in per_core(kind):
            piece = weight_piece(kind, zz, ny, core)
            await_recv(
                remote(piece, piece, m.f_s.at[kind, zz], m.f_r.at[kind, zz], device(z, ny, x, c)), condition
            )

    for part in range(parts):
        send_weights(part, 2)
    for way in range(2):
        spread(z, way, None)
    go(token_x(z, x))
    go(token_core(z, x, c))
    send_weights(0, 0)

    def pass_tokens(step):
        for way in range(2):
            origin = z - step if way == 0 else z + step
            valid = origin >= 0 if way == 0 else origin < nz
            await_recv(token_z(origin, way), valid)
            spread(origin, way, valid)
            go(token_x(origin, x), valid)
            go(token_core(origin, x, c), valid)

    def around(step):
        return lax.rem(z + step, nz)

    for step in range(nz):
        pass_weights(2, around(step))
    pass_tokens(1)
    send_weights(1, 0)
    pass_weights(0, z)

    @pl.when(is_ret)
    def _():
        lane = lax.broadcasted_iota(jnp.int32, (length, key_size), 1)
        row = lax.broadcasted_iota(jnp.int32, (length, key_size), 0)
        half = key_size // 2
        inverse = jnp.exp(
            lax.rem(lane, half).astype(f32) * (-math.log(rope_base) / half)
        )
        sign = jnp.where(lane < half, -1.0, 1.0)

        def table(zz, carry):
            where = pl.ds(pl.multiple_of(zz * length, length), length)
            angles = (row + (zz * SIDES + y) * length).astype(f32) * inverse
            m.cosine[where, :] = jnp.cos(angles)
            m.sine[where, :] = jnp.sin(angles) * sign
            return carry

        lax.fori_loop(0, nz, table, 0)

    pass_tokens(2)
    for part in range(parts):
        send_weights(part, 1)
    for step in range(1, nz):
        pass_weights(0, around(step))
    for step in range(3, nz):
        pass_tokens(step)
    for step in range(nz):
        origin = around(step)
        await_recv(token_x(origin, nx))
        go(token_core(origin, nx, c))
    for zz in range(nz):
        take_weights(2, zz)

    @pl.when(is_ret)
    def _():
        lower = (
            lax.broadcasted_iota(jnp.int32, (length, length), 0)
            >= lax.broadcasted_iota(jnp.int32, (length, length), 1)
        )
        lower_float = lower.astype(f32)
        mine = [m.aux[zz * SIDES + y, pl.ds(part_here, 1), :] for zz in range(nz)]
        logs = jnp.concatenate(mine * (8 // nz), axis=0)
        by_row = dot_nt(logs, lower_float, precision=lax.Precision.HIGHEST)
        by_column = dot_nt(lower_float, logs, precision=lax.Precision.HIGHEST)
        for zz in range(nz):
            rows = slice(zz * length, (zz + 1) * length)
            column = by_column[:, zz : zz + 1]
            closing = by_column[length - 1 : length, zz : zz + 1]
            within = jnp.minimum(column - by_row[zz : zz + 1, :], 0.0)
            m.decay[rows, :] = jnp.where(lower, jnp.exp(within), 0.0)
            m.fade_q[rows, :] = jnp.broadcast_to(jnp.exp(column), (length, key_size))
            m.fade_k[rows, :] = jnp.broadcast_to(jnp.exp(closing - column), (length, key_size))

    for step in range(nz):
        take_weights(0, around(step))
    for step in range(nz):
        origin = around(step)
        for side in (x, nx):
            await_recv(token_core(origin, side, nc))

    def run_rows(zz):
        return pl.ds(pl.multiple_of(zz * length, length), length)

    def store_mix(zz, xx, lanes, values):
        for cc in range(CORES):
            start = ((xx * CORES + cc) * nz + zz) * count
            m.mix[pl.ds(pl.multiple_of(start, count), count), lanes] = values[cc * count : (cc + 1) * count]

    def state_copy(zz):
        piece = m.states.at[zz, y]
        return remote(piece, piece, m.s_s.at[zz], m.s_r.at[zz], device(z, ny, x, c))

    def state_arrival(zz):
        piece = m.states.at[zz, ny]
        return remote(piece, piece, m.s_s.at[zz], m.s_r.at[zz], device(z, ny, x, c))

    halo_copy = remote(m.rim, m.halo, m.h_s.at[0], m.h_r.at[0], device(z, ny, x, c))

    @pl.when(is_ret)
    def _():
        def project_run(zz, carry):
            rows = run_rows(zz)
            product = dot_nn(m.tok[rows, :], m.ret_w[...]).astype(bf)
            cosine, sine = m.cosine[rows, :], m.sine[rows, :]

            def turn(values):
                values = values.astype(f32)
                return values * cosine + pltpu.roll(values, key_size // 2, 1) * sine

            m.queries[rows, 0:key_size] = turn(product[:, 0:key_size]).astype(bf)
            key = (turn(product[:, key_size : 2 * key_size]) * key_size ** (-0.5)).astype(bf)
            m.keys[rows, :] = key
            value = product[:, 2 * key_size :]
            m.values[rows, :] = value
            faded = (key.astype(f32) * m.fade_k[rows, :]).astype(bf)
            m.states[zz, y] = dot_tn(faded, value).astype(bf)
            state_copy(zz).start()
            return carry

        lax.fori_loop(0, nz, project_run, 0)

    lane_kv = lax.broadcasted_iota(jnp.int32, (WINDOW, 2 * HEAD_DIM), 1)

    def place(zz, spot, packed):
        where = pl.ds(spot * WINDOW, WINDOW)
        packed = packed.astype(f32)
        low = jnp.where(lane_kv < HEAD_DIM, packed, 0.0)
        high = jnp.where(lane_kv < HEAD_DIM, 0.0, packed)
        m.kv[0, zz, where, :] = low.astype(bf)
        m.kv[1, zz, where, :] = pltpu.roll(low, HEAD_DIM, 1).astype(bf)
        m.kv[2, zz, where, :] = pltpu.roll(high, HEAD_DIM, 1).astype(bf)
        m.kv[3, zz, where, :] = high.astype(bf)

    @pl.when(is_att)
    def _():
        def project_run(zz, carry):
            rows = run_rows(zz)
            product = dot_nn(m.tok[rows, :], m.att_w[...]).astype(bf)
            m.queries[rows, :] = product[:, 0:V_DIM]
            for spot in range(2):
                place(zz, spot + 1, product[spot * WINDOW : (spot + 1) * WINDOW, V_DIM:])
            m.rim[zz] = product[length - WINDOW :, V_DIM:]
            return carry

        lax.fori_loop(0, nz, project_run, 0)
        halo_copy.start()

    for step in range(nz):
        pass_weights(1, around(step))

    @pl.when(is_ret)
    def _():
        def inner_run(zz, carry):
            rows = run_rows(zz)
            scores = dot_nt(m.queries[rows, 0:key_size], m.keys[rows, :]) * m.decay[rows, :]
            m.inner[rows, :] = dot_nn(scores.astype(bf), m.values[rows, :])
            return carry

        lax.fori_loop(0, nz, inner_run, 0)
        totals = [
            jnp.sum(m.aux[spot, pl.ds(part_here, 1), :], axis=1, keepdims=True) for spot in range(n)
        ]
        for zz in range(nz):
            state_arrival(zz).wait_recv()
        running = jnp.zeros((key_size, V_DIM), f32)
        for zz in range(nz):
            for yy in range(SIDES):
                m.before[zz, yy] = running
                running = running * jnp.exp(totals[zz * SIDES + yy]) + m.states[zz, yy].astype(f32)

        def finish_run(zz, carry):
            rows = run_rows(zz)
            query = (m.queries[rows, 0:key_size].astype(f32) * m.fade_q[rows, :]).astype(bf)
            state = m.before[zz, y]
            high = state.astype(bf)
            low = (state - high.astype(f32)).astype(bf)
            total = m.inner[rows, :] + (dot_nn(query, high) + dot_nn(query, low))
            total = total * lax.rsqrt(jnp.mean(total * total, axis=-1, keepdims=True) + epsilon)
            total = total.astype(bf)
            for xx in range(2):
                store_mix(zz, xx, slice(0, V_DIM), total[xx * WINDOW : (xx + 1) * WINDOW])
            return carry

        lax.fori_loop(0, nz, finish_run, 0)
        for zz in range(nz):
            state_copy(zz).wait_send()

    @pl.when(is_att)
    def _():
        halo_copy.wait_recv()
        for zz in range(nz):
            place(zz, 0, m.halo[jnp.maximum(zz - 1 + y, 0)])
        row = lax.broadcasted_iota(jnp.int32, (WINDOW, 2 * WINDOW), 0)
        column = lax.broadcasted_iota(jnp.int32, (WINDOW, 2 * WINDOW), 1)
        band = (column > row) & (column <= row + WINDOW)
        sink_row = m.aux[sp, parts : parts + 1, 0:LANES]
        sink_lane = lax.broadcasted_iota(jnp.int32, (1, LANES), 1)
        heads = V_DIM // HEAD_DIM
        sinks = [
            jnp.sum(
                jnp.where(sink_lane == part_here * heads + head, sink_row, 0.0), axis=1, keepdims=True
            )
            for head in range(heads)
        ]

        def attend_run(zz, carry):
            for xx in range(2):
                first = (zz + y + xx) == 0
                allowed = band & ((column >= WINDOW) | jnp.logical_not(first))
                where = pl.ds(xx * WINDOW, 2 * WINDOW)
                rows = pl.ds(pl.multiple_of(zz * length + xx * WINDOW, WINDOW), WINDOW)
                for pair in range(heads // 2):
                    lanes = slice(pair * LANES, (pair + 1) * LANES)
                    query = m.queries[rows, lanes]
                    mixed = None
                    for side in range(2):
                        sink = sinks[pair * 2 + side]
                        scores = dot_nt(query, m.kv[side, zz, where, :]) * HEAD_DIM ** (-0.5)
                        scores = jnp.where(allowed, scores, masked_out)
                        highest = jnp.maximum(jnp.max(scores, axis=-1, keepdims=True), sink)
                        lifted = jnp.exp(scores - highest)
                        below = jnp.sum(lifted, axis=-1, keepdims=True) + jnp.exp(sink - highest)
                        weights = (lifted / below).astype(bf)
                        term = dot_nn(weights, m.kv[2 + side, zz, where, :])
                        mixed = term if mixed is None else mixed + term
                    store_mix(zz, xx, lanes, mixed.astype(bf))
            return carry

        lax.fori_loop(0, nz, attend_run, 0)
        halo_copy.wait_send()

    for step in range(nz):
        take_weights(1, around(step))

    def mix_rows(xx, cc):
        return pl.ds(pl.multiple_of((xx * CORES + cc) * group, group), group)

    def core_copy(slot, q):
        return remote(
            m.core_out.at[slot, q], m.core_in.at[slot, q], m.rc_s.at[slot, q], m.rc_r.at[slot, q],
            device(z, y, x, nc),
        )

    def x_copy(q):
        return remote(m.x_out.at[q], m.x_in.at[q], m.rx_s.at[q], m.rx_r.at[q], device(z, y, nx, c))

    def home_rows(zz):
        return pl.ds(pl.multiple_of(zz * count, count), count)

    def z_copy(q, zz):
        return remote(
            m.z_out.at[q, home_rows(zz)], m.z_in.at[q, z], m.rz_s.at[q, zz], m.rz_r.at[q, z],
            device(zz, y, x, c),
        )

    def z_arrival(q, zz):
        return remote(
            m.z_out.at[q, home_rows(zz)], m.z_in.at[q, zz], m.rz_s.at[q, zz], m.rz_r.at[q, zz],
            device(zz, y, x, c),
        )

    def to_core(slot, xx):
        def body(q, carry):
            m.core_out[slot, q] = dot_nn(m.mix[mix_rows(xx, nc), :], m.out_w[q]).astype(bf)
            core_copy(slot, q).start()
            return carry

        lax.fori_loop(0, n, body, 0)

    to_core(0, nx)

    def to_x(q, carry):
        own = dot_nn(m.mix[mix_rows(nx, c), :], m.out_w[q])
        core_copy(0, q).wait_recv()
        m.x_out[q] = (own + m.core_in[0, q].astype(f32)).astype(bf)
        x_copy(q).start()
        return carry

    lax.fori_loop(0, n, to_x, 0)
    to_core(1, x)

    def to_z(q, carry):
        own = dot_nn(m.mix[mix_rows(x, c), :], m.out_w[q])
        core_copy(1, q).wait_recv()
        own = own + m.core_in[1, q].astype(f32)
        x_copy(q).wait_recv()
        own = own + m.x_in[q].astype(f32)
        m.acc[q] = own
        m.z_out[q] = own.astype(bf)
        for step in range(1, nz):
            z_copy(q, around(step)).start()
        return carry

    lax.fori_loop(0, n, to_z, 0)
    for q in range(n):
        total = m.acc[q, home_rows(z), :]
        for step in range(1, nz):
            z_arrival(q, around(step)).wait_recv()
            total = total + m.z_in[q, around(step)].astype(f32)
        out_ref[:, q * width : (q + 1) * width] = total.astype(bf)

    for copy, condition in started:
        if condition is None:
            copy.wait_send()
        else:
            pl.when(condition)(copy.wait_send)

    def drain(q, carry):
        for slot in range(2):
            core_copy(slot, q).wait_send()
        x_copy(q).wait_send()
        for step in range(1, nz):
            z_copy(q, around(step)).wait_send()
        return carry

    lax.fori_loop(0, n, drain, 0)


def layer(n, n_tp, tokens, norm_gain, aux, *weights):
    count, features = tokens.shape
    depth = weights[0].shape[0]
    width = weights[-1].shape[1]
    scratch = layer_scratch(n, n_tp, count, features, depth, width)
    vmem = pl.BlockSpec(memory_space=pltpu.VMEM)
    return pl.pallas_call(
        functools.partial(layer_kernel, n, n_tp, tuple(scratch)),
        out_shape=jax.ShapeDtypeStruct((count, n * width), jnp.bfloat16),
        in_specs=[vmem] * (3 + len(weights)),
        out_specs=vmem,
        scratch_shapes=list(scratch.values()),
        compiler_params=pltpu.CompilerParams(
            collective_id=3, has_side_effects=True, vmem_limit_bytes=60 * 2**20
        ),
        cost_estimate=pl.CostEstimate(flops=4 * 2**30, bytes_accessed=16 * 2**20, transcendentals=0),
        name="layer",
    )(tokens, norm_gain.reshape(1, -1), aux, *weights)


def on_device(
    tokens,
    norm_gain,
    ret_query,
    ret_key,
    ret_value,
    log_decay,
    att_query,
    att_key,
    att_value,
    sink_logits,
    ret_out,
    att_out,
):
    n, n_tp = lax.axis_size("sp"), lax.axis_size("tp")
    length = log_decay.shape[1]
    shapes = (
        tokens.shape[0],
        log_decay.shape[0],
        sink_logits.shape[0],
        att_key.shape[1] // HEAD_DIM,
        length,
    )
    if layer_fits(n, n_tp, shapes):
        aux = jnp.concatenate(
            [log_decay, jnp.pad(sink_logits[None], ((0, 7 - log_decay.shape[0]), (0, length - sink_logits.shape[0])))], axis=0
        )
        return layer(
            n, n_tp, tokens, norm_gain, aux,
            ret_query, ret_key, ret_value, att_query, att_key, att_value, ret_out, att_out,
        )
    tok_float = tokens.astype(jnp.float32)
    normed = (
        tok_float
        * lax.rsqrt(jnp.mean(tok_float * tok_float, axis=-1, keepdims=True) + epsilon)
        * norm_gain
    ).astype(jnp.bfloat16)
    weights = (ret_query, ret_key, ret_value, att_query, att_key, att_value)
    widths = [weight.shape[1] for weight in weights]
    points = [sum(widths[:index]) for index in range(1, len(widths))]
    aligned = ret_out.shape[1] % LANES == 0
    local_logs = jnp.sum(log_decay, axis=1)
    log_tile = jnp.broadcast_to(
        jnp.pad(local_logs, (0, -local_logs.shape[0] % 8))[:, None], (-(-local_logs.shape[0] // 8) * 8, LANES)
    )
    projected, logs = project(normed, jnp.concatenate(weights, axis=1), log_tile, n, n_tp)
    logs = logs[:, : local_logs.shape[0], 0]
    sections = jnp.split(projected, points, axis=1)
    tok_count = sections[0].shape[0]
    anchor = lax.axis_index("sp") * tok_count
    positions = anchor + jnp.arange(tok_count, dtype=jnp.int32)
    query_ret = rotate(sections[0].reshape(tok_count, -1, RETAIN_KEY_SIZE), positions).astype(
        jnp.bfloat16
    )
    key_ret = (
        rotate(sections[1].reshape(tok_count, -1, RETAIN_KEY_SIZE), positions)
        * RETAIN_KEY_SIZE ** (-0.5)
    ).astype(jnp.bfloat16)
    value_ret = sections[2].reshape(tok_count, -1, V_DIM)
    stacked = projected[:, points[3] :]
    ret_mix, rim, wholes = retention_path(
        query_ret,
        key_ret,
        value_ret,
        log_decay,
        stacked[tok_count - WINDOW :],
        logs,
        (ret_out, att_out) if aligned else (),
    )
    if not aligned:
        wholes = [
            lax.all_gather(weight, "sp", axis=1, tiled=True)[None] for weight in (ret_out, att_out)
        ]
    att_mix = attention_path(sections[3], stacked, rim, sink_logits, anchor)
    return merge((ret_mix, att_mix), wholes, n_tp)


def solution(mesh):
    in_specs = (
        P(("sp", "tp"), None),
        P(),
        P("sp", "tp"),
        P("sp", "tp"),
        P("sp", "tp"),
        P("tp", "sp"),
        P("sp", "tp"),
        P("sp", "tp"),
        P("sp", "tp"),
        P("tp"),
        P("tp", "sp"),
        P("tp", "sp"),
    )
    out_specs = P(("sp", "tp"), None)
    return jax.shard_map(
        on_device, mesh=mesh, in_specs=in_specs, out_specs=out_specs, check_vma=False
    )
```

```python
import functools
import math

import jax
import jax.numpy as jnp
from jax import lax
from jax.experimental import pallas as pl
from jax.experimental.pallas import tpu as pltpu
from jax.sharding import PartitionSpec as P

MESH = pl.DeviceIdType.MESH
LANES = 128

RETAIN_KEY_SIZE = 128
V_DIM = 256
HEAD_DIM = 64
WINDOW = 128
BLOCK = 128


epsilon = 1e-05
rope_base = 10000.0
masked_out = -1e30


def rotate(values, positions):
    half_dim = values.shape[-1] // 2
    inverse = rope_base ** (-jnp.arange(half_dim, dtype=jnp.float32) / half_dim)
    angles = positions.astype(jnp.float32)[:, None] * inverse[None, :]
    cosine = jnp.cos(angles)[:, None, :]
    sine_part = jnp.sin(angles)[:, None, :]
    first_half = values[..., :half_dim].astype(jnp.float32)
    second_half = values[..., half_dim:].astype(jnp.float32)
    return jnp.concatenate(
        [
            first_half * cosine - second_half * sine_part,
            second_half * cosine + first_half * sine_part,
        ],
        axis=-1,
    )


def retention_path(query_ret, key_ret, value_ret, log_decay, rim, logs, weights):
    tok_count, heads_here = (query_ret.shape[0], query_ret.shape[1])
    blocks = tok_count // BLOCK
    q_blocks = query_ret.reshape(blocks, BLOCK, heads_here, RETAIN_KEY_SIZE)
    k_blocks = key_ret.reshape(blocks, BLOCK, heads_here, RETAIN_KEY_SIZE)
    v_blocks = value_ret.reshape(blocks, BLOCK, heads_here, V_DIM)
    running = jnp.cumsum(log_decay.reshape(heads_here, blocks, BLOCK), axis=-1)
    closing = running[:, :, -1:]
    within = running[:, :, :, None] - running[:, :, None, :]
    causal_mask = jnp.arange(BLOCK)[:, None] >= jnp.arange(BLOCK)[None, :]
    weighting = jnp.where(causal_mask, jnp.exp(jnp.minimum(within, 0.0)), 0.0)
    scores = (
        jnp.einsum("nihd,njhd->hnij", q_blocks, k_blocks, preferred_element_type=jnp.float32)
        * weighting
    )
    in_block = jnp.einsum(
        "hnij,njhv->nihv", scores.astype(jnp.bfloat16), v_blocks, preferred_element_type=jnp.float32
    )
    key_fade = (
        k_blocks.astype(jnp.float32) * jnp.exp(closing - running).transpose(1, 2, 0)[..., None]
    ).astype(jnp.bfloat16)
    contrib = jnp.einsum("njhd,njhv->nhdv", key_fade, v_blocks, preferred_element_type=jnp.float32)
    block_fade = jnp.exp(closing[:, :, 0]).T

    def advance(carried, entry_pair):
        addend, factor = entry_pair
        return (carried * factor[:, None, None] + addend, carried)

    final_state, before = lax.scan(
        advance, jnp.zeros((heads_here, RETAIN_KEY_SIZE, V_DIM), jnp.float32), (contrib, block_fade)
    )
    n = lax.axis_size("sp")
    place = lax.axis_index("sp")
    before_rim, states, *wholes = exchange(
        rim, final_state.astype(jnp.bfloat16).reshape(2, -1, V_DIM), weights, n
    )
    states = states.reshape(n, heads_here, RETAIN_KEY_SIZE, V_DIM)
    spots = jnp.arange(n)
    between = (spots[None, :] > spots[:, None]) & (spots[None, :] < place)
    spans = jnp.sum(jnp.where(between[:, :, None], logs[None], 0.0), axis=1)
    shares = jnp.where((spots < place)[:, None], jnp.exp(spans), 0.0)
    arrived = jnp.sum(shares[:, :, None, None] * states.astype(jnp.float32), axis=0)
    leading = jnp.cumsum(closing[:, :, 0], axis=1) - closing[:, :, 0]
    before = before + arrived[None] * jnp.exp(leading).T[:, :, None, None]
    query_fade = (
        q_blocks.astype(jnp.float32) * jnp.exp(running).transpose(1, 2, 0)[..., None]
    ).astype(jnp.bfloat16)
    carried_term = jnp.einsum(
        "nihd,nhdv->nihv", query_fade.astype(jnp.float32), before, precision=lax.Precision.HIGHEST
    )
    final_product = in_block + carried_term
    final_product = final_product * lax.rsqrt(
        jnp.mean(final_product * final_product, axis=-1, keepdims=True) + epsilon
    )
    return final_product.reshape(tok_count, heads_here * V_DIM).astype(jnp.bfloat16), before_rim, wholes


def attention_path(query_att, stacked, window_rim, sink_logits, anchor):
    tok_count = query_att.shape[0]
    kv_here = stacked.shape[1] // (2 * HEAD_DIM)
    group_size = query_att.shape[1] // (kv_here * HEAD_DIM)
    blocks = tok_count // WINDOW
    extended = jnp.concatenate([window_rim, stacked], axis=0).reshape(
        blocks + 1, WINDOW, 2, kv_here, HEAD_DIM
    )
    paired = jnp.concatenate([extended[:-1], extended[1:]], axis=1)
    keys_pair = paired[:, :, 0]
    values_pair = paired[:, :, 1]
    q_blocks = query_att.reshape(blocks, WINDOW, kv_here, group_size, HEAD_DIM)
    scores = jnp.einsum(
        "nihgd,njhd->nhgij", q_blocks, keys_pair, preferred_element_type=jnp.float32
    ) * HEAD_DIM ** (-0.5)
    query_pos = anchor + (jnp.arange(blocks) * WINDOW)[:, None] + jnp.arange(WINDOW)[None, :]
    key_pos = (
        anchor + (jnp.arange(blocks) * WINDOW - WINDOW)[:, None] + jnp.arange(2 * WINDOW)[None, :]
    )
    allowed = (
        (key_pos[:, None, :] >= 0)
        & (key_pos[:, None, :] <= query_pos[:, :, None])
        & (query_pos[:, :, None] - key_pos[:, None, :] < WINDOW)
    )
    scores = jnp.where(allowed[:, None, None], scores, masked_out)
    sink_logit = sink_logits.reshape(kv_here, group_size)[None, :, :, None]
    highest = jnp.maximum(jnp.max(scores, axis=-1), sink_logit)
    lifted = jnp.exp(scores - highest[..., None])
    denominator = jnp.sum(lifted, axis=-1) + jnp.exp(sink_logit - highest)
    attn_weights = (lifted / denominator[..., None]).astype(jnp.bfloat16)
    final_product = jnp.einsum(
        "nhgij,njhd->nihgd", attn_weights, values_pair, preferred_element_type=jnp.float32
    )
    return final_product.reshape(tok_count, kv_here * group_size * HEAD_DIM).astype(jnp.bfloat16)


def ring_spot(index, count):
    half = count // 2
    return jnp.where(lax.rem(index, 2) == 0, index // 2, count - 1 - index // 2)


def ring_member(spot, count):
    half = count // 2
    return jnp.where(spot < half, 2 * spot, 2 * (count - 1 - spot) + 1)


def project_kernel(n, n_tp, normed_ref, pack_ref, log_ref, out_ref, logs_ref, rows_ref, held, total, sems, tok_sems):
    sp, tp = lax.axis_index("sp"), lax.axis_index("tp")
    depth, width = pack_ref.shape
    count = normed_ref.shape[0]
    half = n // 2
    spot = ring_spot(sp, n)
    ahead = ring_member(lax.rem(spot + 1, n), n)
    behind = ring_member(lax.rem(spot + n - 1, n), n)

    barrier = pltpu.get_barrier_semaphore()
    for peer in (ahead, behind):
        pl.semaphore_signal(barrier, inc=1, device_id=(peer, tp), device_id_type=MESH)
    for step in range(1, n_tp):
        pl.semaphore_signal(
            barrier, inc=1, device_id=(sp, lax.rem(tp + step, n_tp)), device_id_type=MESH
        )
    pl.semaphore_wait(barrier, 2 + n_tp - 1)

    def rows_of(member):
        return pl.ds(pl.multiple_of(member * depth, depth), depth)

    middle = (width // LANES + 1) // 2 * LANES
    spans = (pl.ds(0, middle), pl.ds(middle, width - middle))

    def owner(direction, distance):
        shift = n - distance if direction == 0 else distance
        return ring_member(lax.rem(spot + shift, n), n)

    def send(direction, step, part):
        member = owner(direction, step - 1)
        if part == 2:
            return pltpu.make_async_remote_copy(
                src_ref=log_ref if step == 1 else logs_ref.at[member],
                dst_ref=logs_ref.at[member],
                send_sem=sems.at[0, direction, step - 1, part],
                recv_sem=sems.at[1, direction, step - 1, part],
                device_id=(ahead if direction == 0 else behind, tp),
                device_id_type=MESH,
            )
        source = pack_ref.at[:, spans[part]] if step == 1 else held.at[rows_of(member), spans[part]]
        return pltpu.make_async_remote_copy(
            src_ref=source,
            dst_ref=held.at[rows_of(member), spans[part]],
            send_sem=sems.at[0, direction, step - 1, part],
            recv_sem=sems.at[1, direction, step - 1, part],
            device_id=(ahead if direction == 0 else behind, tp),
            device_id_type=MESH,
        )

    def arrival(direction, step, part):
        member = owner(direction, step)
        if part == 2:
            return pltpu.make_async_remote_copy(
                src_ref=log_ref,
                dst_ref=logs_ref.at[member],
                send_sem=sems.at[0, direction, step - 1, part],
                recv_sem=sems.at[1, direction, step - 1, part],
                device_id=(ahead if direction == 0 else behind, tp),
                device_id_type=MESH,
            )
        return pltpu.make_async_remote_copy(
            src_ref=held.at[rows_of(member), spans[part]],
            dst_ref=held.at[rows_of(member), spans[part]],
            send_sem=sems.at[0, direction, step - 1, part],
            recv_sem=sems.at[1, direction, step - 1, part],
            device_id=(ahead if direction == 0 else behind, tp),
            device_id_type=MESH,
        )

    started = []

    def go(copy):
        copy.start()
        started.append(copy)

    def parts_of(step, direction):
        first = direction
        if step == half:
            return (2, first) if direction == 0 else (first,)
        return (2, first, 1 - first)

    for slot in range(3):
        for direction in range(2):
            parts = parts_of(1, direction)
            if slot < len(parts):
                go(send(direction, 1, parts[slot]))
    tok_here = pl.ds(pl.multiple_of(tp * count, count), count)
    for step in range(1, n_tp):
        go(
            pltpu.make_async_remote_copy(
                src_ref=normed_ref,
                dst_ref=rows_ref.at[tok_here],
                send_sem=tok_sems.at[0, step - 1],
                recv_sem=tok_sems.at[1, step - 1],
                device_id=(sp, lax.rem(tp + step, n_tp)),
                device_id_type=MESH,
            )
        )
    rows_ref[tok_here, :] = normed_ref[...]
    logs_ref[sp] = log_ref[...]
    for step in range(1, n_tp):
        origin = pl.ds(pl.multiple_of(lax.rem(tp + n_tp - step, n_tp) * count, count), count)
        pltpu.make_async_remote_copy(
            src_ref=normed_ref,
            dst_ref=rows_ref.at[origin],
            send_sem=tok_sems.at[0, step - 1],
            recv_sem=tok_sems.at[1, step - 1],
            device_id=(sp, lax.rem(tp + step, n_tp)),
            device_id_type=MESH,
        ).wait_recv()

    blockwise = depth % LANES == 0

    def add(member, weights, first=False):
        columns = pl.ds(pl.multiple_of(member * depth, depth), depth)
        product = jnp.dot(rows_ref[:, columns], weights, preferred_element_type=jnp.float32)
        total[...] = product if first else total[...] + product

    if blockwise:
        add(sp, pack_ref[...], True)
    else:
        held[rows_of(sp), :] = pack_ref[...]
    for step in range(1, half + 1):
        for slot in range(3):
            for direction in range(2):
                parts = parts_of(step, direction)
                if slot < len(parts):
                    arrival(direction, step, parts[slot]).wait_recv()
                    if step < half and parts[slot] in parts_of(step + 1, direction):
                        go(send(direction, step + 1, parts[slot]))
        if blockwise:
            for direction in range(1 if step == half else 2):
                member = owner(direction, step)
                add(member, held[rows_of(member), :])
    if not blockwise:
        total[...] = jnp.dot(rows_ref[...], held[...], preferred_element_type=jnp.float32)
    out_ref[...] = total[...].astype(out_ref.dtype)
    for copy in started:
        copy.wait_send()


def project(normed, pack, logs, n, n_tp):
    depth, width = pack.shape
    count = normed.shape[0]
    features = normed.shape[1]
    vmem = pl.BlockSpec(memory_space=pltpu.VMEM)
    return pl.pallas_call(
        functools.partial(project_kernel, n, n_tp),
        out_shape=(
            jax.ShapeDtypeStruct((n_tp * count, width), jnp.bfloat16),
            jax.ShapeDtypeStruct((n,) + logs.shape, jnp.float32),
        ),
        in_specs=[vmem, vmem, vmem],
        out_specs=(vmem, vmem),
        scratch_shapes=[
            pltpu.VMEM((n_tp * count, features), jnp.bfloat16),
            pltpu.VMEM((n * depth, width), jnp.bfloat16),
            pltpu.VMEM((n_tp * count, width), jnp.float32),
            pltpu.SemaphoreType.DMA((2, 2, n // 2, 3)),
            pltpu.SemaphoreType.DMA((2, n_tp - 1)),
        ],
        compiler_params=pltpu.CompilerParams(
            collective_id=0, has_side_effects=True, vmem_limit_bytes=40 * 2**20
        ),
        cost_estimate=pl.CostEstimate(
            flops=400 * 2**30, bytes_accessed=n * depth * width * 2, transcendentals=0
        ),
        name="project_ring",
    )(normed, pack, logs)


def exchange_kernel(n, extra, rim_ref, state_ref, *refs):
    weight_refs = refs[:extra]
    before_ref, states_ref = refs[extra : extra + 2]
    whole_refs = refs[extra + 2 : 2 * extra + 2]
    sems, rim_sems = refs[2 * extra + 2 :]
    sources = [state_ref.at[0], state_ref.at[1], *weight_refs]
    sp, tp = lax.axis_index("sp"), lax.axis_index("tp")
    half = n // 2
    spot = ring_spot(sp, n)
    ahead = ring_member(lax.rem(spot + 1, n), n)
    behind = ring_member(lax.rem(spot + n - 1, n), n)
    later, earlier = lax.rem(sp + 1, n), lax.rem(sp + n - 1, n)
    barrier = pltpu.get_barrier_semaphore()
    for peer in (ahead, behind, later, earlier):
        pl.semaphore_signal(barrier, inc=1, device_id=(peer, tp), device_id_type=MESH)
    pl.semaphore_wait(barrier, 4)

    def owner(direction, distance):
        shift = n - distance if direction == 0 else distance
        return ring_member(lax.rem(spot + shift, n), n)

    def parts_of(step, direction):
        order = []
        for first in range(0, 2 + extra, 2):
            order.append(first + direction)
            if step < half:
                order.append(first + 1 - direction)
        return order

    def target(member, part):
        return states_ref.at[member, part] if part < 2 else whole_refs[part - 2].at[member]

    def hop(direction, step, part, member, source):
        return pltpu.make_async_remote_copy(
            src_ref=source,
            dst_ref=target(member, part),
            send_sem=sems.at[0, direction, step - 1, part],
            recv_sem=sems.at[1, direction, step - 1, part],
            device_id=(ahead if direction == 0 else behind, tp),
            device_id_type=MESH,
        )

    started = []
    rim = pltpu.make_async_remote_copy(
        src_ref=rim_ref,
        dst_ref=before_ref,
        send_sem=rim_sems.at[0],
        recv_sem=rim_sems.at[1],
        device_id=(later, tp),
        device_id_type=MESH,
    )
    for slot in range(2 + extra):
        for direction in range(2):
            parts = parts_of(1, direction)
            if slot < len(parts):
                copy = hop(direction, 1, parts[slot], sp, sources[parts[slot]])
                copy.start()
                started.append(copy)
    rim.start()
    states_ref[sp] = state_ref[...]
    for whole, piece in zip(whole_refs, weight_refs):
        whole[sp] = piece[...]
    for step in range(1, half + 1):
        for slot in range(2 + extra):
            for direction in range(2):
                parts = parts_of(step, direction)
                if slot < len(parts):
                    part = parts[slot]
                    member = owner(direction, step)
                    hop(direction, step, part, member, sources[part]).wait_recv()
                    if step < half and part in parts_of(step + 1, direction):
                        copy = hop(direction, step + 1, part, member, target(member, part))
                        copy.start()
                        started.append(copy)
    rim.wait()
    for copy in started:
        copy.wait_send()


def exchange(rim, state, weights, n):
    vmem = pl.BlockSpec(memory_space=pltpu.VMEM)
    return pl.pallas_call(
        functools.partial(exchange_kernel, n, len(weights)),
        out_shape=(
            jax.ShapeDtypeStruct(rim.shape, rim.dtype),
            jax.ShapeDtypeStruct((n,) + state.shape, state.dtype),
            *[jax.ShapeDtypeStruct((n,) + weight.shape, weight.dtype) for weight in weights],
        ),
        in_specs=[vmem] * (2 + len(weights)),
        out_specs=(vmem,) * (2 + len(weights)),
        scratch_shapes=[
            pltpu.SemaphoreType.DMA((2, 2, n // 2, 2 + len(weights))),
            pltpu.SemaphoreType.DMA((2,)),
        ],
        compiler_params=pltpu.CompilerParams(
            collective_id=2, has_side_effects=True, vmem_limit_bytes=40 * 2**20
        ),
        cost_estimate=pl.CostEstimate(
            flops=20 * 2**30, bytes_accessed=n * state.size * 2, transcendentals=0
        ),
        name="state_ring",
    )(rim, state, *weights)


def merge_kernel(n_tp, ret_ref, att_ref, ret_out_ref, att_out_ref, out_ref, total, outgoing, incoming, sent, landed, sems):
    sp, tp = lax.axis_index("sp"), lax.axis_index("tp")
    outer, inner = tp // 2, lax.rem(tp, 2)
    groups = n_tp // 2
    count = out_ref.shape[0]
    barrier = pltpu.get_barrier_semaphore()
    mate = outer * 2 + 1 - inner
    pl.semaphore_signal(barrier, inc=1, device_id=(sp, mate), device_id_type=MESH)
    for step in range(1, groups):
        peer = lax.rem(outer + step, groups) * 2 + inner
        pl.semaphore_signal(barrier, inc=1, device_id=(sp, peer), device_id_type=MESH)
    pl.semaphore_wait(barrier, groups)

    blocks, _, width = ret_out_ref.shape

    def partial(side, block):
        return jnp.dot(
            ret_ref[side], ret_out_ref[block], preferred_element_type=jnp.float32
        ) + jnp.dot(att_ref[side], att_out_ref[block], preferred_element_type=jnp.float32)

    for block in range(blocks):
        outgoing[:, block * width : (block + 1) * width] = partial(1 - inner, block).astype(
            jnp.bfloat16
        )
    swap = pltpu.make_async_remote_copy(
        src_ref=outgoing,
        dst_ref=incoming,
        send_sem=sems.at[0, 0],
        recv_sem=sems.at[1, 0],
        device_id=(sp, mate),
        device_id_type=MESH,
    )
    swap.start()
    for block in range(blocks):
        total[:, block * width : (block + 1) * width] = partial(inner, block)
    swap.wait_recv()
    own = total[...] + incoming[...].astype(jnp.float32)
    sent[...] = own.astype(jnp.bfloat16)
    copies = []
    for step in range(1, groups):
        other = lax.rem(outer + step, groups)
        copy = pltpu.make_async_remote_copy(
            src_ref=sent.at[pl.ds(pl.multiple_of(other * count, count), count)],
            dst_ref=landed.at[step - 1],
            send_sem=sems.at[0, step],
            recv_sem=sems.at[1, step],
            device_id=(sp, other * 2 + inner),
            device_id_type=MESH,
        )
        copy.start()
        copies.append(copy)
    mine = sent[pl.ds(pl.multiple_of(outer * count, count), count), :].astype(jnp.float32)
    for step, copy in enumerate(copies):
        copy.wait_recv()
        mine = mine + landed[step].astype(jnp.float32)
    out_ref[...] = mine.astype(out_ref.dtype)
    swap.wait_send()
    for copy in copies:
        copy.wait_send()


def merge(mixes, weights, n_tp):
    rows = mixes[0].shape[0]
    groups = n_tp // 2
    count = rows // n_tp
    width = weights[0].shape[0] * weights[0].shape[2]
    mixes = [
        mix.reshape(groups, 2, count, -1).transpose(1, 0, 2, 3).reshape(2, groups * count, -1)
        for mix in mixes
    ]
    vmem = pl.BlockSpec(memory_space=pltpu.VMEM)
    return pl.pallas_call(
        functools.partial(merge_kernel, n_tp),
        out_shape=jax.ShapeDtypeStruct((count, width), jnp.bfloat16),
        in_specs=[vmem] * 4,
        out_specs=vmem,
        scratch_shapes=[
            pltpu.VMEM((groups * count, width), jnp.float32),
            pltpu.VMEM((groups * count, width), jnp.bfloat16),
            pltpu.VMEM((groups * count, width), jnp.bfloat16),
            pltpu.VMEM((groups * count, width), jnp.bfloat16),
            pltpu.VMEM((max(1, groups - 1), count, width), jnp.bfloat16),
            pltpu.SemaphoreType.DMA((2, groups)),
        ],
        compiler_params=pltpu.CompilerParams(
            collective_id=1, has_side_effects=True, vmem_limit_bytes=40 * 2**20
        ),
        cost_estimate=pl.CostEstimate(
            flops=4 * rows * weights[0].size // 1, bytes_accessed=4 * weights[0].size, transcendentals=0
        ),
        name="merge_scatter",
    )(*mixes, *weights)


SIDES = 2
CORES = 2
PAIR = 2
PIECES = 2


def layer_fits(n, n_tp, shapes):
    count, heads_here, att_here, kv_here, length = shapes
    nz, nx = n // SIDES, n_tp // CORES
    return (
        n == nz * SIDES
        and nx == 2
        and n_tp == nx * CORES
        and nz == 2 * PAIR
        and nz == heads_here * CORES
        and kv_here == 1
        and att_here * HEAD_DIM == heads_here * V_DIM
        and count % 16 == 0
        and n_tp * count == length
        and length == 2 * WINDOW
        and length == 2 * BLOCK
        and nx * WINDOW == length
    )


def layer_scratch(n, n_tp, count, features, depth, width):
    nz = n // SIDES
    length = n_tp * count
    rows = nz * length
    slab = n * width // PIECES
    att_width = V_DIM + 2 * HEAD_DIM
    ret_width = 2 * RETAIN_KEY_SIZE + V_DIM
    parts = nz // CORES
    bf, f32 = jnp.bfloat16, jnp.float32
    dma = pltpu.SemaphoreType.DMA
    return dict(
        tok=pltpu.VMEM((rows, features), bf),
        ret_pack=pltpu.VMEM((parts, depth, ret_width), bf),
        att_pack=pltpu.VMEM((parts, depth, att_width), bf),
        ret_w=pltpu.VMEM((n * depth, ret_width), bf),
        att_w=pltpu.VMEM((n * depth, att_width), bf),
        out_pack=pltpu.VMEM((2, parts * V_DIM, width), bf),
        out_w=pltpu.VMEM((V_DIM, n * width), bf),
        tokens=pltpu.VMEM((count, features), bf),
        gain=pltpu.VMEM((1, features), f32),
        aux_here=pltpu.VMEM((8, length), f32),
        kv_pack=pltpu.VMEM((2 * HEAD_DIM, depth), bf),
        bias=pltpu.VMEM((2, WINDOW, 2 * WINDOW), f32),
        aux=pltpu.VMEM((n, 8, length), f32),
        cosine=pltpu.VMEM((rows, RETAIN_KEY_SIZE), f32),
        sine=pltpu.VMEM((rows, RETAIN_KEY_SIZE), f32),
        fade_q=pltpu.VMEM((rows, RETAIN_KEY_SIZE), f32),
        fade_k=pltpu.VMEM((rows, RETAIN_KEY_SIZE), f32),
        decay=pltpu.VMEM((rows, length), f32),
        queries=pltpu.VMEM((rows, V_DIM), bf),
        keys=pltpu.VMEM((rows, RETAIN_KEY_SIZE), bf),
        values=pltpu.VMEM((rows, V_DIM), bf),
        inner=pltpu.VMEM((rows, V_DIM), f32),
        states=pltpu.VMEM((nz, SIDES, RETAIN_KEY_SIZE, V_DIM), bf),
        before=pltpu.VMEM((nz, SIDES, RETAIN_KEY_SIZE, V_DIM), f32),
        kv=pltpu.VMEM((4, nz, length + WINDOW, 2 * HEAD_DIM), bf),
        rim=pltpu.VMEM((nz, WINDOW, 2 * HEAD_DIM), bf),
        halo=pltpu.VMEM((nz, WINDOW, 2 * HEAD_DIM), bf),
        mix=pltpu.VMEM((length, V_DIM), bf),
        part=pltpu.VMEM((length, slab), f32),
        keep=pltpu.VMEM((2, nz, PIECES, count, slab), f32),
        core_out=pltpu.VMEM((2, nz, PIECES, count, slab), bf),
        core_in=pltpu.VMEM((2, nz, PIECES, count, slab), bf),
        x_out=pltpu.VMEM((nz, PIECES, count, slab), bf),
        x_in=pltpu.VMEM((nz, PIECES, count, slab), bf),
        z_out=pltpu.VMEM((nz, PIECES, count, slab), bf),
        z_in=pltpu.VMEM((nz, PIECES, count, slab), bf),
        tz_s=dma((2, nz)),
        tz_r=dma((nz,)),
        tx_s=dma((nz,)),
        tx_r=dma((nz,)),
        tc_s=dma((nz, 2)),
        tc_r=dma((nz, 2)),
        w_s=dma((3, nz, CORES)),
        w_r=dma((3, nz)),
        f_s=dma((3, nz)),
        f_r=dma((3, nz)),
        s_s=dma((nz,)),
        s_r=dma((nz,)),
        h_s=dma((1,)),
        h_r=dma((1,)),
        rc_s=dma((2, nz, PIECES)),
        rc_r=dma((2, nz, PIECES)),
        rx_s=dma((nz, PIECES)),
        rx_r=dma((nz, PIECES)),
        rz_s=dma((nz, PIECES)),
        rz_r=dma((nz, PIECES)),
        load=dma((16,)),
    )


class Named:
    def __init__(self, names, refs):
        for name, ref in zip(names, refs):
            setattr(self, name, ref)


def dot_nt(a, b, **kw):
    return lax.dot_general(a, b, (((1,), (1,)), ((), ())), preferred_element_type=jnp.float32, **kw)


def dot_tn(a, b):
    return lax.dot_general(a, b, (((0,), (0,)), ((), ())), preferred_element_type=jnp.float32)


def dot_nn(a, b):
    return jnp.dot(a, b, preferred_element_type=jnp.float32)


def layer_kernel(n, n_tp, names, *refs):
    (tokens_ref, gain_ref, aux_ref, rq_ref, rk_ref, rv_ref, aq_ref, ak_ref, av_ref, ro_ref, ao_ref) = refs[:11]
    out_ref = refs[11]
    m = Named(names, refs[12:])
    nz = n // SIDES
    parts = nz // CORES
    count, features = tokens_ref.shape
    depth = rq_ref.shape[0]
    width = out_ref.shape[1] // n
    length = n_tp * count
    slab = out_ref.shape[1] // PIECES
    key_size = RETAIN_KEY_SIZE
    bf, f32 = jnp.bfloat16, jnp.float32

    sp, tp = lax.axis_index("sp"), lax.axis_index("tp")
    z, y = sp // SIDES, lax.rem(sp, SIDES)
    x, c = tp // CORES, lax.rem(tp, CORES)
    ny, nx, nc = 1 - y, 1 - x, 1 - c
    is_ret, is_att = c == 0, c == 1
    source_core = z // parts
    mate = z + 1 - 2 * lax.rem(z, PAIR)
    part_here = lax.rem(z, parts)

    def device(zz, yy, xx, cc):
        return (zz * SIDES + yy, xx * CORES + cc)

    def remote(src, dst, send_sem, recv_sem, target):
        return pltpu.make_async_remote_copy(
            src_ref=src,
            dst_ref=dst,
            send_sem=send_sem,
            recv_sem=recv_sem,
            device_id=target,
            device_id_type=MESH,
        )

    started = []

    def go(copy, condition=None):
        started.append((copy, condition))
        if condition is None:
            copy.start()
        else:
            pl.when(condition)(copy.start)

    def both(*conditions):
        conditions = [cond for cond in conditions if cond is not None]
        if not conditions:
            return None
        result = conditions[0]
        for cond in conditions[1:]:
            result = result & cond
        return result

    def await_recv(copy, condition=None):
        if condition is None:
            copy.wait_recv()
        else:
            pl.when(condition)(copy.wait_recv)

    moves = [(tokens_ref, m.tokens), (gain_ref, m.gain), (aux_ref, m.aux_here)]
    moves += [(ak_ref, m.kv_pack.at[0:HEAD_DIM]), (av_ref, m.kv_pack.at[HEAD_DIM:])]
    for part in range(parts):
        wide = slice(part * V_DIM, (part + 1) * V_DIM)
        thin = slice(part * key_size, (part + 1) * key_size)
        moves += [
            (rq_ref.at[:, thin], m.ret_pack.at[part, :, 0:key_size]),
            (rk_ref.at[:, thin], m.ret_pack.at[part, :, key_size : 2 * key_size]),
            (rv_ref.at[:, wide], m.ret_pack.at[part, :, 2 * key_size :]),
            (aq_ref.at[:, wide], m.att_pack.at[part, :, 0:V_DIM]),
        ]
    moves += [(ro_ref, m.out_pack.at[0]), (ao_ref, m.out_pack.at[1])]
    loads = []
    for index, (src, dst) in enumerate(moves):
        loads.append(pltpu.make_async_copy(src, dst, m.load.at[index]))
        loads[-1].start()

    barrier = pltpu.get_barrier_semaphore()
    peers = [device(z, ny, x, c), device(z, y, nx, c), device(z, y, x, nc)]
    for step in range(1, nz):
        for cc in range(CORES):
            peers.append(device(lax.rem(z + step, nz), y, x, cc))
    for peer in peers:
        pl.semaphore_signal(barrier, inc=1, device_id=peer, device_id_type=MESH)

    def token_rows(zz, xx, cc):
        return pl.ds(pl.multiple_of(zz * length + xx * (CORES * count) + cc * count, count), count)

    loads[0].wait()
    loads[1].wait()
    tok_float = m.tokens[...].astype(f32)
    scale = lax.rsqrt(jnp.mean(tok_float * tok_float, axis=-1, keepdims=True) + epsilon)
    m.tok[token_rows(z, x, c), :] = (tok_float * scale * m.gain[...]).astype(bf)
    for copy in loads[2:]:
        copy.wait()
    pair = jnp.transpose(m.kv_pack[...].astype(f32)).astype(bf)
    for part in range(parts):
        m.att_pack[part, :, V_DIM:] = pair
    pl.semaphore_wait(barrier, len(peers))

    def token_at(zz, xx, cc):
        return m.tok.at[token_rows(zz, xx, cc)]

    def token_z(origin, way):
        piece = token_at(origin, x, c)
        return remote(piece, piece, m.tz_s.at[way, origin], m.tz_r.at[origin], device(z + 1 - 2 * way, y, x, c))

    def token_x(origin, side):
        piece = token_at(origin, side, c)
        return remote(piece, piece, m.tx_s.at[origin], m.tx_r.at[origin], device(z, y, nx, c))

    def token_core(origin, side, core):
        piece = token_at(origin, side, core)
        return remote(piece, piece, m.tc_s.at[origin, side], m.tc_r.at[origin, side], device(z, y, x, nc))

    can_go = (z < nz - 1, z > 0)

    def spread(origin, way, condition):
        go(token_z(origin, way), both(condition, can_go[way]))

    def weight_rows(zz, yy):
        return pl.ds(pl.multiple_of((zz * SIDES + yy) * depth, depth), depth)

    near, distant = c == z // parts, c != z // parts

    def toward(step):
        return (z, mate, lax.rem(z + PAIR, nz), nz - 1 - z)[step]

    def send_weights(step, kind):
        target_z = toward(step)
        part = lax.rem(target_z, parts)
        valid = near if step < PAIR else distant
        first = len(started)
        for core in range(CORES):
            target = device(target_z, y, x, core)
            pack, dest = (m.ret_pack, m.ret_w) if core == 0 else (m.att_pack, m.att_w)
            rows = pl.ds(pl.multiple_of(part * V_DIM, V_DIM), V_DIM)
            if kind == 0:
                src = pack.at[part]
            elif kind == 1:
                src = m.out_pack.at[core, rows]
            else:
                src = m.aux_here
            dst = weight_piece(kind, z, y, core)
            away = valid if step else valid & (c != core)
            go(remote(src, dst, m.w_s.at[kind, step, core], m.w_r.at[kind, z], target), away)
            if step == 0:

                @pl.when(valid & (c == core))
                def _():
                    if kind == 0:
                        dest[weight_rows(z, y), :] = pack[part]
                    elif kind == 1:
                        m.out_w[:, out_columns(z, y)] = m.out_pack[core, rows, :]
                    else:
                        m.aux[sp] = m.aux_here[...]

        return started[first:]

    def finish(copies):
        for entry in copies:
            started[:] = [kept for kept in started if kept is not entry]
            pl.when(entry[1])(entry[0].wait_send)

    def out_columns(zz, yy):
        return pl.ds(pl.multiple_of((zz * SIDES + yy) * width, width), width)

    def weight_piece(kind, zz, yy, core):
        if kind == 0:
            return (m.ret_w if core == 0 else m.att_w).at[weight_rows(zz, yy)]
        if kind == 1:
            return m.out_w.at[:, out_columns(zz, yy)]
        return m.aux.at[zz * SIDES + yy]

    def per_core(kind):
        return ((0, is_ret), (1, is_att)) if kind == 0 else ((0, None),)

    def pass_weights(kind, step):
        zz = toward(step)
        other = jnp.logical_not((zz == z) & (c == source_core))
        for core, condition in per_core(kind):
            piece = weight_piece(kind, zz, y, core)
            await_recv(
                remote(piece, piece, m.f_s.at[kind, zz], m.w_r.at[kind, zz], device(z, ny, x, c)),
                both(condition, other),
            )
            go(
                remote(piece, piece, m.f_s.at[kind, zz], m.f_r.at[kind, zz], device(z, ny, x, c)),
                condition,
            )

    def take_weights(kind, zz):
        for core, condition in per_core(kind):
            piece = weight_piece(kind, zz, ny, core)
            await_recv(
                remote(piece, piece, m.f_s.at[kind, zz], m.f_r.at[kind, zz], device(z, ny, x, c)), condition
            )

    for step in range(nz):
        send_weights(step, 2)
    for way in range(2):
        spread(z, way, None)
    go(token_x(z, x))
    go(token_core(z, x, c))
    for kind in range(2):
        for step in range(PAIR):
            send_weights(step, kind)

    def pass_tokens(step):
        for way in range(2):
            origin = z - step if way == 0 else z + step
            valid = origin >= 0 if way == 0 else origin < nz
            await_recv(token_z(origin, way), valid)
            spread(origin, way, valid)
            go(token_x(origin, x), valid)
            go(token_core(origin, x, c), valid)

    def across_tokens(step):
        origin = toward(step)
        await_recv(token_x(origin, nx))
        go(token_core(origin, nx, c))

    @pl.when(is_ret)
    def _():
        lane = lax.broadcasted_iota(jnp.int32, (length, key_size), 1)
        row = lax.broadcasted_iota(jnp.int32, (length, key_size), 0)
        half = key_size // 2
        inverse = jnp.exp(
            lax.rem(lane, half).astype(f32) * (-math.log(rope_base) / half)
        )
        sign = jnp.where(lane < half, -1.0, 1.0)

        def table(zz, carry):
            where = pl.ds(pl.multiple_of(zz * length, length), length)
            angles = (row + (zz * SIDES + y) * length).astype(f32) * inverse
            m.cosine[where, :] = jnp.cos(angles)
            m.sine[where, :] = jnp.sin(angles) * sign
            return carry

        lax.fori_loop(0, nz, table, 0)

    pass_weights(0, 0)
    pass_tokens(1)
    second = send_weights(2, 0)
    for step in range(nz):
        pass_weights(2, step)
    pass_weights(0, 1)
    pass_weights(1, 0)
    pass_tokens(2)
    across_tokens(0)
    pass_weights(1, 1)
    finish(second)
    third = send_weights(3, 0)
    pass_tokens(3)
    pass_weights(0, 2)
    across_tokens(1)
    finish(third)
    send_weights(2, 1)
    send_weights(3, 1)
    pass_weights(0, 3)
    across_tokens(3)
    across_tokens(2)
    for zz in range(nz):
        take_weights(2, zz)

    @pl.when(is_ret)
    def _():
        lower = (
            lax.broadcasted_iota(jnp.int32, (length, length), 0)
            >= lax.broadcasted_iota(jnp.int32, (length, length), 1)
        )
        lower_float = lower.astype(f32)
        mine = [m.aux[zz * SIDES + y, pl.ds(part_here, 1), :] for zz in range(nz)]
        logs = jnp.concatenate(mine * (8 // nz), axis=0)
        by_row = dot_nt(logs, lower_float, precision=lax.Precision.HIGHEST)
        by_column = dot_nt(lower_float, logs, precision=lax.Precision.HIGHEST)
        for zz in range(nz):
            rows = slice(zz * length, (zz + 1) * length)
            column = by_column[:, zz : zz + 1]
            closing = by_column[length - 1 : length, zz : zz + 1]
            within = jnp.minimum(column - by_row[zz : zz + 1, :], 0.0)
            m.decay[rows, :] = jnp.where(lower, jnp.exp(within), 0.0)
            m.fade_q[rows, :] = jnp.broadcast_to(jnp.exp(column), (length, key_size))
            m.fade_k[rows, :] = jnp.broadcast_to(jnp.exp(closing - column), (length, key_size))

    for step in range(nz):
        take_weights(0, toward(step))
    for step in range(nz):
        origin = toward(step)
        for side in (x, nx):
            await_recv(token_core(origin, side, nc))

    def run_rows(zz):
        return pl.ds(pl.multiple_of(zz * length, length), length)

    def state_copy(zz):
        piece = m.states.at[zz, y]
        return remote(piece, piece, m.s_s.at[zz], m.s_r.at[zz], device(z, ny, x, c))

    def state_arrival(zz):
        piece = m.states.at[zz, ny]
        return remote(piece, piece, m.s_s.at[zz], m.s_r.at[zz], device(z, ny, x, c))

    halo_copy = remote(m.rim, m.halo, m.h_s.at[0], m.h_r.at[0], device(z, ny, x, c))

    @pl.when(is_ret)
    def _():
        def project_run(zz, carry):
            rows = run_rows(zz)
            product = dot_nn(m.tok[rows, :], m.ret_w[...]).astype(bf)
            cosine, sine = m.cosine[rows, :], m.sine[rows, :]

            def turn(values):
                values = values.astype(f32)
                return values * cosine + pltpu.roll(values, key_size // 2, 1) * sine

            m.queries[rows, 0:key_size] = turn(product[:, 0:key_size]).astype(bf)
            key = (turn(product[:, key_size : 2 * key_size]) * key_size ** (-0.5)).astype(bf)
            m.keys[rows, :] = key
            value = product[:, 2 * key_size :]
            m.values[rows, :] = value
            faded = (key.astype(f32) * m.fade_k[rows, :]).astype(bf)
            m.states[zz, y] = dot_tn(faded, value).astype(bf)
            state_copy(zz).start()
            return carry

        lax.fori_loop(0, nz, project_run, 0)

    lane_kv = lax.broadcasted_iota(jnp.int32, (WINDOW, 2 * HEAD_DIM), 1)

    def place(zz, spot, packed):
        where = pl.ds(spot * WINDOW, WINDOW)
        packed = packed.astype(f32)
        low = jnp.where(lane_kv < HEAD_DIM, packed, 0.0)
        turned = pltpu.roll(packed, HEAD_DIM, 1)
        m.kv[0, zz, where, :] = low.astype(bf)
        m.kv[1, zz, where, :] = pltpu.roll(low, HEAD_DIM, 1).astype(bf)
        m.kv[2, zz, where, :] = jnp.where(lane_kv < HEAD_DIM, turned, 1.0).astype(bf)
        m.kv[3, zz, where, :] = jnp.where(lane_kv < HEAD_DIM, 1.0, packed).astype(bf)

    @pl.when(is_att)
    def _():
        def project_run(zz, carry):
            rows = run_rows(zz)
            product = dot_nn(m.tok[rows, :], m.att_w[...]).astype(bf)
            m.queries[rows, :] = (product[:, 0:V_DIM].astype(f32) * HEAD_DIM ** (-0.5)).astype(bf)
            for spot in range(2):
                place(zz, spot + 1, product[spot * WINDOW : (spot + 1) * WINDOW, V_DIM:])
            m.rim[zz] = product[length - WINDOW :, V_DIM:]
            return carry

        lax.fori_loop(0, nz, project_run, 0)
        halo_copy.start()

    far = jnp.where(z < PAIR, nz - 1, 0)

    def home(turn):
        near = far + jnp.where(z < PAIR, -1, 1)
        if isinstance(turn, int):
            return (far, near, mate, z)[turn]
        return jnp.where(turn == 0, far, jnp.where(turn == 1, near, jnp.where(turn == 2, mate, z)))

    def core_copy(slot, turn, piece):
        return remote(
            m.core_out.at[slot, turn, piece],
            m.core_in.at[slot, turn, piece],
            m.rc_s.at[slot, turn, piece],
            m.rc_r.at[slot, turn, piece],
            device(z, y, x, nc),
        )

    def x_copy(turn, piece):
        return remote(
            m.x_out.at[turn, piece],
            m.x_in.at[turn, piece],
            m.rx_s.at[turn, piece],
            m.rx_r.at[turn, piece],
            device(z, y, nx, c),
        )

    def z_copy(turn, piece, target_z, slot):
        return remote(
            m.z_out.at[turn, piece],
            m.z_in.at[slot, piece],
            m.rz_s.at[turn, piece],
            m.rz_r.at[slot, piece],
            device(target_z, y, x, c),
        )

    def take_out_weights():
        for step in range(nz):
            take_weights(1, toward(step))

    def mix_rows(xx, cc):
        return pl.ds(pl.multiple_of((xx * CORES + cc) * count, count), count)

    def emit(turn):
        for piece in range(PIECES):
            m.part[...] = dot_nn(m.mix[...], m.out_w[:, piece * slab : (piece + 1) * slab])
            for slot, side in enumerate((nx, x)):
                m.core_out[slot, turn, piece] = m.part[mix_rows(side, nc), :].astype(bf)
                core_copy(slot, turn, piece).start()
            for slot, side in enumerate((nx, x)):
                m.keep[slot, turn, piece] = m.part[mix_rows(side, c), :]

    def to_x(turn, carry):
        for piece in range(PIECES):
            core_copy(0, turn, piece).wait_recv()
            total = m.keep[0, turn, piece] + m.core_in[0, turn, piece].astype(f32)
            m.x_out[turn, piece] = total.astype(bf)
            x_copy(turn, piece).start()
        return carry

    for step in range(PAIR, nz):
        pass_weights(1, step)

    @pl.when(is_ret)
    def _():
        def inner_run(zz, carry):
            rows = run_rows(zz)
            scores = dot_nt(m.queries[rows, 0:key_size], m.keys[rows, :]) * m.decay[rows, :]
            m.inner[rows, :] = dot_nn(scores.astype(bf), m.values[rows, :])
            return carry

        lax.fori_loop(0, nz, inner_run, 0)
        totals = [
            jnp.sum(m.aux[spot, pl.ds(part_here, 1), :], axis=1, keepdims=True) for spot in range(n)
        ]
        for zz in range(nz):
            state_arrival(zz).wait_recv()
        running = jnp.zeros((key_size, V_DIM), f32)
        for zz in range(nz):
            for yy in range(SIDES):
                m.before[zz, yy] = running
                running = running * jnp.exp(totals[zz * SIDES + yy]) + m.states[zz, yy].astype(f32)

        def finish_run(turn, carry):
            zz = home(turn)
            rows = run_rows(zz)
            query = (m.queries[rows, 0:key_size].astype(f32) * m.fade_q[rows, :]).astype(bf)
            state = m.before[zz, y]
            high = state.astype(bf)
            low = (state - high.astype(f32)).astype(bf)
            total = m.inner[rows, :] + (dot_nn(query, high) + dot_nn(query, low))
            total = total * lax.rsqrt(jnp.mean(total * total, axis=-1, keepdims=True) + epsilon)
            m.mix[...] = total.astype(bf)
            emit(turn)
            return carry

        take_out_weights()
        lax.fori_loop(0, nz, finish_run, 0)
        lax.fori_loop(0, nz, to_x, 0)
        for zz in range(nz):
            state_copy(zz).wait_send()

    @pl.when(is_att)
    def _():
        row = lax.broadcasted_iota(jnp.int32, (WINDOW, 2 * WINDOW), 0)
        column = lax.broadcasted_iota(jnp.int32, (WINDOW, 2 * WINDOW), 1)
        band = (column > row) & (column <= row + WINDOW)
        m.bias[0] = jnp.where(band & (column >= WINDOW), 0.0, masked_out)
        m.bias[1] = jnp.where(band, 0.0, masked_out)
        sink_row = m.aux[sp, parts : parts + 1, 0:LANES]
        sink_lane = lax.broadcasted_iota(jnp.int32, (1, LANES), 1)
        heads = V_DIM // HEAD_DIM
        sinks = [
            jnp.sum(
                jnp.where(sink_lane == part_here * heads + head, sink_row, 0.0), axis=1, keepdims=True
            )
            for head in range(heads)
        ]
        halo_copy.wait_recv()
        for zz in range(nz):
            place(zz, 0, m.halo[jnp.maximum(zz - 1 + y, 0)])
        take_out_weights()

        def attend_run(turn, carry):
            zz = home(turn)
            for xx in range(2):
                bias = m.bias[jnp.minimum(zz + y + xx, 1)]
                where = pl.ds(xx * WINDOW, 2 * WINDOW)
                rows = pl.ds(pl.multiple_of(zz * length + xx * WINDOW, WINDOW), WINDOW)
                for pair in range(heads // 2):
                    lanes = slice(pair * LANES, (pair + 1) * LANES)
                    query = m.queries[rows, lanes]
                    terms, ends = [], []
                    for side in range(2):
                        sink = sinks[pair * 2 + side]
                        scores = dot_nt(query, m.kv[side, zz, where, :]) + bias
                        highest = jnp.maximum(jnp.max(scores, axis=-1, keepdims=True), sink)
                        lifted = jnp.exp(scores - highest).astype(bf)
                        ends.append(jnp.exp(sink - highest))
                        terms.append(dot_nn(lifted, m.kv[2 + side, zz, where, :]))
                    first = lane_kv < HEAD_DIM
                    below = pltpu.roll(jnp.where(first, terms[1], terms[0]), HEAD_DIM, 1)
                    below = below + jnp.where(first, ends[0], ends[1])
                    mixed = jnp.where(first, terms[0], terms[1]) / below
                    m.mix[xx * WINDOW : (xx + 1) * WINDOW, lanes] = mixed.astype(bf)
            emit(turn)
            to_x(turn, carry)
            return carry

        lax.fori_loop(0, nz, attend_run, 0)
        halo_copy.wait_send()

    outer = (z == 0) | (z == nz - 1)

    def to_z(turn):
        for piece in range(PIECES):
            core_copy(1, turn, piece).wait_recv()
            x_copy(turn, piece).wait_recv()
            total = m.keep[1, turn, piece] + m.core_in[1, turn, piece].astype(f32)
            total = total + m.x_in[turn, piece].astype(f32)
            if turn < PAIR:

                @pl.when(outer)
                def _():
                    m.z_out[turn, piece] = total.astype(bf)
                    z_copy(turn, piece, mate, turn).start()

                @pl.when(jnp.logical_not(outer))
                def _():
                    z_copy(turn, piece, mate, turn).wait_recv()
                    merged = total + m.z_in[turn, piece].astype(f32)
                    m.z_out[turn, piece] = merged.astype(bf)
                    z_copy(turn, piece, home(turn), nz - 1).start()
            elif turn < nz - 1:
                m.z_out[turn, piece] = total.astype(bf)
                z_copy(turn, piece, mate, turn).start()
            else:
                z_copy(nz - 2, piece, mate, nz - 2).wait_recv()
                total = total + m.z_in[nz - 2, piece].astype(f32)
                z_copy(0, piece, mate, nz - 1).wait_recv()
                total = total + m.z_in[nz - 1, piece].astype(f32)
                out_ref[:, piece * slab : (piece + 1) * slab] = total.astype(bf)

    for turn in range(nz):
        to_z(turn)

    for copy, condition in started:
        if condition is None:
            copy.wait_send()
        else:
            pl.when(condition)(copy.wait_send)
    for turn in range(nz):
        for piece in range(PIECES):
            for slot in range(2):
                core_copy(slot, turn, piece).wait_send()
            x_copy(turn, piece).wait_send()
            if turn < nz - 1:
                z_copy(turn, piece, mate, turn).wait_send()


def layer(n, n_tp, tokens, norm_gain, aux, *weights):
    count, features = tokens.shape
    depth = weights[0].shape[0]
    width = weights[-1].shape[1]
    scratch = layer_scratch(n, n_tp, count, features, depth, width)
    vmem = pl.BlockSpec(memory_space=pltpu.VMEM)
    return pl.pallas_call(
        functools.partial(layer_kernel, n, n_tp, tuple(scratch)),
        out_shape=jax.ShapeDtypeStruct((count, n * width), jnp.bfloat16),
        in_specs=[pl.BlockSpec(memory_space=pltpu.HBM)] * (3 + len(weights)),
        out_specs=vmem,
        scratch_shapes=list(scratch.values()),
        compiler_params=pltpu.CompilerParams(
            collective_id=3, has_side_effects=True, vmem_limit_bytes=60 * 2**20
        ),
        cost_estimate=pl.CostEstimate(flops=4 * 2**30, bytes_accessed=16 * 2**20, transcendentals=0),
        name="layer",
    )(tokens, norm_gain.reshape(1, -1), aux, *weights)


def on_device(
    tokens,
    norm_gain,
    ret_query,
    ret_key,
    ret_value,
    log_decay,
    att_query,
    att_key,
    att_value,
    sink_logits,
    ret_out,
    att_out,
):
    n, n_tp = lax.axis_size("sp"), lax.axis_size("tp")
    length = log_decay.shape[1]
    shapes = (
        tokens.shape[0],
        log_decay.shape[0],
        sink_logits.shape[0],
        att_key.shape[1] // HEAD_DIM,
        length,
    )
    if layer_fits(n, n_tp, shapes):
        aux = jnp.concatenate(
            [log_decay, jnp.pad(sink_logits[None], ((0, 7 - log_decay.shape[0]), (0, length - sink_logits.shape[0])))], axis=0
        )
        return layer(
            n, n_tp, tokens, norm_gain, aux,
            ret_query, ret_key, ret_value, att_query, att_key.T, att_value.T, ret_out, att_out,
        )
    tok_float = tokens.astype(jnp.float32)
    normed = (
        tok_float
        * lax.rsqrt(jnp.mean(tok_float * tok_float, axis=-1, keepdims=True) + epsilon)
        * norm_gain
    ).astype(jnp.bfloat16)
    weights = (ret_query, ret_key, ret_value, att_query, att_key, att_value)
    widths = [weight.shape[1] for weight in weights]
    points = [sum(widths[:index]) for index in range(1, len(widths))]
    aligned = ret_out.shape[1] % LANES == 0
    local_logs = jnp.sum(log_decay, axis=1)
    log_tile = jnp.broadcast_to(
        jnp.pad(local_logs, (0, -local_logs.shape[0] % 8))[:, None], (-(-local_logs.shape[0] // 8) * 8, LANES)
    )
    projected, logs = project(normed, jnp.concatenate(weights, axis=1), log_tile, n, n_tp)
    logs = logs[:, : local_logs.shape[0], 0]
    sections = jnp.split(projected, points, axis=1)
    tok_count = sections[0].shape[0]
    anchor = lax.axis_index("sp") * tok_count
    positions = anchor + jnp.arange(tok_count, dtype=jnp.int32)
    query_ret = rotate(sections[0].reshape(tok_count, -1, RETAIN_KEY_SIZE), positions).astype(
        jnp.bfloat16
    )
    key_ret = (
        rotate(sections[1].reshape(tok_count, -1, RETAIN_KEY_SIZE), positions)
        * RETAIN_KEY_SIZE ** (-0.5)
    ).astype(jnp.bfloat16)
    value_ret = sections[2].reshape(tok_count, -1, V_DIM)
    stacked = projected[:, points[3] :]
    ret_mix, rim, wholes = retention_path(
        query_ret,
        key_ret,
        value_ret,
        log_decay,
        stacked[tok_count - WINDOW :],
        logs,
        (ret_out, att_out) if aligned else (),
    )
    if not aligned:
        wholes = [
            lax.all_gather(weight, "sp", axis=1, tiled=True)[None] for weight in (ret_out, att_out)
        ]
    att_mix = attention_path(sections[3], stacked, rim, sink_logits, anchor)
    return merge((ret_mix, att_mix), wholes, n_tp)


def solution(mesh):
    in_specs = (
        P(("sp", "tp"), None),
        P(),
        P("sp", "tp"),
        P("sp", "tp"),
        P("sp", "tp"),
        P("tp", "sp"),
        P("sp", "tp"),
        P("sp", "tp"),
        P("sp", "tp"),
        P("tp"),
        P("tp", "sp"),
        P("tp", "sp"),
    )
    out_specs = P(("sp", "tp"), None)
    return jax.shard_map(
        on_device, mesh=mesh, in_specs=in_specs, out_specs=out_specs, check_vma=False
    )
```

```python
import functools
import math

import jax
import jax.numpy as jnp
from jax import lax
from jax.experimental import pallas as pl
from jax.experimental.pallas import tpu as pltpu
from jax.sharding import PartitionSpec as P

MESH = pl.DeviceIdType.MESH
LANES = 128

RETAIN_KEY_SIZE = 128
V_DIM = 256
HEAD_DIM = 64
WINDOW = 128
BLOCK = 128


epsilon = 1e-05
rope_base = 10000.0
masked_out = -1e30


def rotate(values, positions):
    half_dim = values.shape[-1] // 2
    inverse = rope_base ** (-jnp.arange(half_dim, dtype=jnp.float32) / half_dim)
    angles = positions.astype(jnp.float32)[:, None] * inverse[None, :]
    cosine = jnp.cos(angles)[:, None, :]
    sine_part = jnp.sin(angles)[:, None, :]
    first_half = values[..., :half_dim].astype(jnp.float32)
    second_half = values[..., half_dim:].astype(jnp.float32)
    return jnp.concatenate(
        [
            first_half * cosine - second_half * sine_part,
            second_half * cosine + first_half * sine_part,
        ],
        axis=-1,
    )


def retention_path(query_ret, key_ret, value_ret, log_decay, rim, logs, weights):
    tok_count, heads_here = (query_ret.shape[0], query_ret.shape[1])
    blocks = tok_count // BLOCK
    q_blocks = query_ret.reshape(blocks, BLOCK, heads_here, RETAIN_KEY_SIZE)
    k_blocks = key_ret.reshape(blocks, BLOCK, heads_here, RETAIN_KEY_SIZE)
    v_blocks = value_ret.reshape(blocks, BLOCK, heads_here, V_DIM)
    running = jnp.cumsum(log_decay.reshape(heads_here, blocks, BLOCK), axis=-1)
    closing = running[:, :, -1:]
    within = running[:, :, :, None] - running[:, :, None, :]
    causal_mask = jnp.arange(BLOCK)[:, None] >= jnp.arange(BLOCK)[None, :]
    weighting = jnp.where(causal_mask, jnp.exp(jnp.minimum(within, 0.0)), 0.0)
    scores = (
        jnp.einsum("nihd,njhd->hnij", q_blocks, k_blocks, preferred_element_type=jnp.float32)
        * weighting
    )
    in_block = jnp.einsum(
        "hnij,njhv->nihv", scores.astype(jnp.bfloat16), v_blocks, preferred_element_type=jnp.float32
    )
    key_fade = (
        k_blocks.astype(jnp.float32) * jnp.exp(closing - running).transpose(1, 2, 0)[..., None]
    ).astype(jnp.bfloat16)
    contrib = jnp.einsum("njhd,njhv->nhdv", key_fade, v_blocks, preferred_element_type=jnp.float32)
    block_fade = jnp.exp(closing[:, :, 0]).T

    def advance(carried, entry_pair):
        addend, factor = entry_pair
        return (carried * factor[:, None, None] + addend, carried)

    final_state, before = lax.scan(
        advance, jnp.zeros((heads_here, RETAIN_KEY_SIZE, V_DIM), jnp.float32), (contrib, block_fade)
    )
    n = lax.axis_size("sp")
    place = lax.axis_index("sp")
    before_rim, states, *wholes = exchange(
        rim, final_state.astype(jnp.bfloat16).reshape(2, -1, V_DIM), weights, n
    )
    states = states.reshape(n, heads_here, RETAIN_KEY_SIZE, V_DIM)
    spots = jnp.arange(n)
    between = (spots[None, :] > spots[:, None]) & (spots[None, :] < place)
    spans = jnp.sum(jnp.where(between[:, :, None], logs[None], 0.0), axis=1)
    shares = jnp.where((spots < place)[:, None], jnp.exp(spans), 0.0)
    arrived = jnp.sum(shares[:, :, None, None] * states.astype(jnp.float32), axis=0)
    leading = jnp.cumsum(closing[:, :, 0], axis=1) - closing[:, :, 0]
    before = before + arrived[None] * jnp.exp(leading).T[:, :, None, None]
    query_fade = (
        q_blocks.astype(jnp.float32) * jnp.exp(running).transpose(1, 2, 0)[..., None]
    ).astype(jnp.bfloat16)
    carried_term = jnp.einsum(
        "nihd,nhdv->nihv", query_fade.astype(jnp.float32), before, precision=lax.Precision.HIGHEST
    )
    final_product = in_block + carried_term
    final_product = final_product * lax.rsqrt(
        jnp.mean(final_product * final_product, axis=-1, keepdims=True) + epsilon
    )
    return final_product.reshape(tok_count, heads_here * V_DIM).astype(jnp.bfloat16), before_rim, wholes


def attention_path(query_att, stacked, window_rim, sink_logits, anchor):
    tok_count = query_att.shape[0]
    kv_here = stacked.shape[1] // (2 * HEAD_DIM)
    group_size = query_att.shape[1] // (kv_here * HEAD_DIM)
    blocks = tok_count // WINDOW
    extended = jnp.concatenate([window_rim, stacked], axis=0).reshape(
        blocks + 1, WINDOW, 2, kv_here, HEAD_DIM
    )
    paired = jnp.concatenate([extended[:-1], extended[1:]], axis=1)
    keys_pair = paired[:, :, 0]
    values_pair = paired[:, :, 1]
    q_blocks = query_att.reshape(blocks, WINDOW, kv_here, group_size, HEAD_DIM)
    scores = jnp.einsum(
        "nihgd,njhd->nhgij", q_blocks, keys_pair, preferred_element_type=jnp.float32
    ) * HEAD_DIM ** (-0.5)
    query_pos = anchor + (jnp.arange(blocks) * WINDOW)[:, None] + jnp.arange(WINDOW)[None, :]
    key_pos = (
        anchor + (jnp.arange(blocks) * WINDOW - WINDOW)[:, None] + jnp.arange(2 * WINDOW)[None, :]
    )
    allowed = (
        (key_pos[:, None, :] >= 0)
        & (key_pos[:, None, :] <= query_pos[:, :, None])
        & (query_pos[:, :, None] - key_pos[:, None, :] < WINDOW)
    )
    scores = jnp.where(allowed[:, None, None], scores, masked_out)
    sink_logit = sink_logits.reshape(kv_here, group_size)[None, :, :, None]
    highest = jnp.maximum(jnp.max(scores, axis=-1), sink_logit)
    lifted = jnp.exp(scores - highest[..., None])
    denominator = jnp.sum(lifted, axis=-1) + jnp.exp(sink_logit - highest)
    attn_weights = (lifted / denominator[..., None]).astype(jnp.bfloat16)
    final_product = jnp.einsum(
        "nhgij,njhd->nihgd", attn_weights, values_pair, preferred_element_type=jnp.float32
    )
    return final_product.reshape(tok_count, kv_here * group_size * HEAD_DIM).astype(jnp.bfloat16)


def ring_spot(index, count):
    half = count // 2
    return jnp.where(lax.rem(index, 2) == 0, index // 2, count - 1 - index // 2)


def ring_member(spot, count):
    half = count // 2
    return jnp.where(spot < half, 2 * spot, 2 * (count - 1 - spot) + 1)


def project_kernel(n, n_tp, normed_ref, pack_ref, log_ref, out_ref, logs_ref, rows_ref, held, total, sems, tok_sems):
    sp, tp = lax.axis_index("sp"), lax.axis_index("tp")
    depth, width = pack_ref.shape
    count = normed_ref.shape[0]
    half = n // 2
    spot = ring_spot(sp, n)
    ahead = ring_member(lax.rem(spot + 1, n), n)
    behind = ring_member(lax.rem(spot + n - 1, n), n)

    barrier = pltpu.get_barrier_semaphore()
    for peer in (ahead, behind):
        pl.semaphore_signal(barrier, inc=1, device_id=(peer, tp), device_id_type=MESH)
    for step in range(1, n_tp):
        pl.semaphore_signal(
            barrier, inc=1, device_id=(sp, lax.rem(tp + step, n_tp)), device_id_type=MESH
        )
    pl.semaphore_wait(barrier, 2 + n_tp - 1)

    def rows_of(member):
        return pl.ds(pl.multiple_of(member * depth, depth), depth)

    middle = (width // LANES + 1) // 2 * LANES
    spans = (pl.ds(0, middle), pl.ds(middle, width - middle))

    def owner(direction, distance):
        shift = n - distance if direction == 0 else distance
        return ring_member(lax.rem(spot + shift, n), n)

    def send(direction, step, part):
        member = owner(direction, step - 1)
        if part == 2:
            return pltpu.make_async_remote_copy(
                src_ref=log_ref if step == 1 else logs_ref.at[member],
                dst_ref=logs_ref.at[member],
                send_sem=sems.at[0, direction, step - 1, part],
                recv_sem=sems.at[1, direction, step - 1, part],
                device_id=(ahead if direction == 0 else behind, tp),
                device_id_type=MESH,
            )
        source = pack_ref.at[:, spans[part]] if step == 1 else held.at[rows_of(member), spans[part]]
        return pltpu.make_async_remote_copy(
            src_ref=source,
            dst_ref=held.at[rows_of(member), spans[part]],
            send_sem=sems.at[0, direction, step - 1, part],
            recv_sem=sems.at[1, direction, step - 1, part],
            device_id=(ahead if direction == 0 else behind, tp),
            device_id_type=MESH,
        )

    def arrival(direction, step, part):
        member = owner(direction, step)
        if part == 2:
            return pltpu.make_async_remote_copy(
                src_ref=log_ref,
                dst_ref=logs_ref.at[member],
                send_sem=sems.at[0, direction, step - 1, part],
                recv_sem=sems.at[1, direction, step - 1, part],
                device_id=(ahead if direction == 0 else behind, tp),
                device_id_type=MESH,
            )
        return pltpu.make_async_remote_copy(
            src_ref=held.at[rows_of(member), spans[part]],
            dst_ref=held.at[rows_of(member), spans[part]],
            send_sem=sems.at[0, direction, step - 1, part],
            recv_sem=sems.at[1, direction, step - 1, part],
            device_id=(ahead if direction == 0 else behind, tp),
            device_id_type=MESH,
        )

    started = []

    def go(copy):
        copy.start()
        started.append(copy)

    def parts_of(step, direction):
        first = direction
        if step == half:
            return (2, first) if direction == 0 else (first,)
        return (2, first, 1 - first)

    for slot in range(3):
        for direction in range(2):
            parts = parts_of(1, direction)
            if slot < len(parts):
                go(send(direction, 1, parts[slot]))
    tok_here = pl.ds(pl.multiple_of(tp * count, count), count)
    for step in range(1, n_tp):
        go(
            pltpu.make_async_remote_copy(
                src_ref=normed_ref,
                dst_ref=rows_ref.at[tok_here],
                send_sem=tok_sems.at[0, step - 1],
                recv_sem=tok_sems.at[1, step - 1],
                device_id=(sp, lax.rem(tp + step, n_tp)),
                device_id_type=MESH,
            )
        )
    rows_ref[tok_here, :] = normed_ref[...]
    logs_ref[sp] = log_ref[...]
    for step in range(1, n_tp):
        origin = pl.ds(pl.multiple_of(lax.rem(tp + n_tp - step, n_tp) * count, count), count)
        pltpu.make_async_remote_copy(
            src_ref=normed_ref,
            dst_ref=rows_ref.at[origin],
            send_sem=tok_sems.at[0, step - 1],
            recv_sem=tok_sems.at[1, step - 1],
            device_id=(sp, lax.rem(tp + step, n_tp)),
            device_id_type=MESH,
        ).wait_recv()

    blockwise = depth % LANES == 0

    def add(member, weights, first=False):
        columns = pl.ds(pl.multiple_of(member * depth, depth), depth)
        product = jnp.dot(rows_ref[:, columns], weights, preferred_element_type=jnp.float32)
        total[...] = product if first else total[...] + product

    if blockwise:
        add(sp, pack_ref[...], True)
    else:
        held[rows_of(sp), :] = pack_ref[...]
    for step in range(1, half + 1):
        for slot in range(3):
            for direction in range(2):
                parts = parts_of(step, direction)
                if slot < len(parts):
                    arrival(direction, step, parts[slot]).wait_recv()
                    if step < half and parts[slot] in parts_of(step + 1, direction):
                        go(send(direction, step + 1, parts[slot]))
        if blockwise:
            for direction in range(1 if step == half else 2):
                member = owner(direction, step)
                add(member, held[rows_of(member), :])
    if not blockwise:
        total[...] = jnp.dot(rows_ref[...], held[...], preferred_element_type=jnp.float32)
    out_ref[...] = total[...].astype(out_ref.dtype)
    for copy in started:
        copy.wait_send()


def project(normed, pack, logs, n, n_tp):
    depth, width = pack.shape
    count = normed.shape[0]
    features = normed.shape[1]
    vmem = pl.BlockSpec(memory_space=pltpu.VMEM)
    return pl.pallas_call(
        functools.partial(project_kernel, n, n_tp),
        out_shape=(
            jax.ShapeDtypeStruct((n_tp * count, width), jnp.bfloat16),
            jax.ShapeDtypeStruct((n,) + logs.shape, jnp.float32),
        ),
        in_specs=[vmem, vmem, vmem],
        out_specs=(vmem, vmem),
        scratch_shapes=[
            pltpu.VMEM((n_tp * count, features), jnp.bfloat16),
            pltpu.VMEM((n * depth, width), jnp.bfloat16),
            pltpu.VMEM((n_tp * count, width), jnp.float32),
            pltpu.SemaphoreType.DMA((2, 2, n // 2, 3)),
            pltpu.SemaphoreType.DMA((2, n_tp - 1)),
        ],
        compiler_params=pltpu.CompilerParams(
            collective_id=0, has_side_effects=True, vmem_limit_bytes=40 * 2**20
        ),
        cost_estimate=pl.CostEstimate(
            flops=400 * 2**30, bytes_accessed=n * depth * width * 2, transcendentals=0
        ),
        name="project_ring",
    )(normed, pack, logs)


def exchange_kernel(n, extra, rim_ref, state_ref, *refs):
    weight_refs = refs[:extra]
    before_ref, states_ref = refs[extra : extra + 2]
    whole_refs = refs[extra + 2 : 2 * extra + 2]
    sems, rim_sems = refs[2 * extra + 2 :]
    sources = [state_ref.at[0], state_ref.at[1], *weight_refs]
    sp, tp = lax.axis_index("sp"), lax.axis_index("tp")
    half = n // 2
    spot = ring_spot(sp, n)
    ahead = ring_member(lax.rem(spot + 1, n), n)
    behind = ring_member(lax.rem(spot + n - 1, n), n)
    later, earlier = lax.rem(sp + 1, n), lax.rem(sp + n - 1, n)
    barrier = pltpu.get_barrier_semaphore()
    for peer in (ahead, behind, later, earlier):
        pl.semaphore_signal(barrier, inc=1, device_id=(peer, tp), device_id_type=MESH)
    pl.semaphore_wait(barrier, 4)

    def owner(direction, distance):
        shift = n - distance if direction == 0 else distance
        return ring_member(lax.rem(spot + shift, n), n)

    def parts_of(step, direction):
        order = []
        for first in range(0, 2 + extra, 2):
            order.append(first + direction)
            if step < half:
                order.append(first + 1 - direction)
        return order

    def target(member, part):
        return states_ref.at[member, part] if part < 2 else whole_refs[part - 2].at[member]

    def hop(direction, step, part, member, source):
        return pltpu.make_async_remote_copy(
            src_ref=source,
            dst_ref=target(member, part),
            send_sem=sems.at[0, direction, step - 1, part],
            recv_sem=sems.at[1, direction, step - 1, part],
            device_id=(ahead if direction == 0 else behind, tp),
            device_id_type=MESH,
        )

    started = []
    rim = pltpu.make_async_remote_copy(
        src_ref=rim_ref,
        dst_ref=before_ref,
        send_sem=rim_sems.at[0],
        recv_sem=rim_sems.at[1],
        device_id=(later, tp),
        device_id_type=MESH,
    )
    for slot in range(2 + extra):
        for direction in range(2):
            parts = parts_of(1, direction)
            if slot < len(parts):
                copy = hop(direction, 1, parts[slot], sp, sources[parts[slot]])
                copy.start()
                started.append(copy)
    rim.start()
    states_ref[sp] = state_ref[...]
    for whole, piece in zip(whole_refs, weight_refs):
        whole[sp] = piece[...]
    for step in range(1, half + 1):
        for slot in range(2 + extra):
            for direction in range(2):
                parts = parts_of(step, direction)
                if slot < len(parts):
                    part = parts[slot]
                    member = owner(direction, step)
                    hop(direction, step, part, member, sources[part]).wait_recv()
                    if step < half and part in parts_of(step + 1, direction):
                        copy = hop(direction, step + 1, part, member, target(member, part))
                        copy.start()
                        started.append(copy)
    rim.wait()
    for copy in started:
        copy.wait_send()


def exchange(rim, state, weights, n):
    vmem = pl.BlockSpec(memory_space=pltpu.VMEM)
    return pl.pallas_call(
        functools.partial(exchange_kernel, n, len(weights)),
        out_shape=(
            jax.ShapeDtypeStruct(rim.shape, rim.dtype),
            jax.ShapeDtypeStruct((n,) + state.shape, state.dtype),
            *[jax.ShapeDtypeStruct((n,) + weight.shape, weight.dtype) for weight in weights],
        ),
        in_specs=[vmem] * (2 + len(weights)),
        out_specs=(vmem,) * (2 + len(weights)),
        scratch_shapes=[
            pltpu.SemaphoreType.DMA((2, 2, n // 2, 2 + len(weights))),
            pltpu.SemaphoreType.DMA((2,)),
        ],
        compiler_params=pltpu.CompilerParams(
            collective_id=2, has_side_effects=True, vmem_limit_bytes=40 * 2**20
        ),
        cost_estimate=pl.CostEstimate(
            flops=20 * 2**30, bytes_accessed=n * state.size * 2, transcendentals=0
        ),
        name="state_ring",
    )(rim, state, *weights)


def merge_kernel(n_tp, ret_ref, att_ref, ret_out_ref, att_out_ref, out_ref, total, outgoing, incoming, sent, landed, sems):
    sp, tp = lax.axis_index("sp"), lax.axis_index("tp")
    outer, inner = tp // 2, lax.rem(tp, 2)
    groups = n_tp // 2
    count = out_ref.shape[0]
    barrier = pltpu.get_barrier_semaphore()
    mate = outer * 2 + 1 - inner
    pl.semaphore_signal(barrier, inc=1, device_id=(sp, mate), device_id_type=MESH)
    for step in range(1, groups):
        peer = lax.rem(outer + step, groups) * 2 + inner
        pl.semaphore_signal(barrier, inc=1, device_id=(sp, peer), device_id_type=MESH)
    pl.semaphore_wait(barrier, groups)

    blocks, _, width = ret_out_ref.shape

    def partial(side, block):
        return jnp.dot(
            ret_ref[side], ret_out_ref[block], preferred_element_type=jnp.float32
        ) + jnp.dot(att_ref[side], att_out_ref[block], preferred_element_type=jnp.float32)

    for block in range(blocks):
        outgoing[:, block * width : (block + 1) * width] = partial(1 - inner, block).astype(
            jnp.bfloat16
        )
    swap = pltpu.make_async_remote_copy(
        src_ref=outgoing,
        dst_ref=incoming,
        send_sem=sems.at[0, 0],
        recv_sem=sems.at[1, 0],
        device_id=(sp, mate),
        device_id_type=MESH,
    )
    swap.start()
    for block in range(blocks):
        total[:, block * width : (block + 1) * width] = partial(inner, block)
    swap.wait_recv()
    own = total[...] + incoming[...].astype(jnp.float32)
    sent[...] = own.astype(jnp.bfloat16)
    copies = []
    for step in range(1, groups):
        other = lax.rem(outer + step, groups)
        copy = pltpu.make_async_remote_copy(
            src_ref=sent.at[pl.ds(pl.multiple_of(other * count, count), count)],
            dst_ref=landed.at[step - 1],
            send_sem=sems.at[0, step],
            recv_sem=sems.at[1, step],
            device_id=(sp, other * 2 + inner),
            device_id_type=MESH,
        )
        copy.start()
        copies.append(copy)
    mine = sent[pl.ds(pl.multiple_of(outer * count, count), count), :].astype(jnp.float32)
    for step, copy in enumerate(copies):
        copy.wait_recv()
        mine = mine + landed[step].astype(jnp.float32)
    out_ref[...] = mine.astype(out_ref.dtype)
    swap.wait_send()
    for copy in copies:
        copy.wait_send()


def merge(mixes, weights, n_tp):
    rows = mixes[0].shape[0]
    groups = n_tp // 2
    count = rows // n_tp
    width = weights[0].shape[0] * weights[0].shape[2]
    mixes = [
        mix.reshape(groups, 2, count, -1).transpose(1, 0, 2, 3).reshape(2, groups * count, -1)
        for mix in mixes
    ]
    vmem = pl.BlockSpec(memory_space=pltpu.VMEM)
    return pl.pallas_call(
        functools.partial(merge_kernel, n_tp),
        out_shape=jax.ShapeDtypeStruct((count, width), jnp.bfloat16),
        in_specs=[vmem] * 4,
        out_specs=vmem,
        scratch_shapes=[
            pltpu.VMEM((groups * count, width), jnp.float32),
            pltpu.VMEM((groups * count, width), jnp.bfloat16),
            pltpu.VMEM((groups * count, width), jnp.bfloat16),
            pltpu.VMEM((groups * count, width), jnp.bfloat16),
            pltpu.VMEM((max(1, groups - 1), count, width), jnp.bfloat16),
            pltpu.SemaphoreType.DMA((2, groups)),
        ],
        compiler_params=pltpu.CompilerParams(
            collective_id=1, has_side_effects=True, vmem_limit_bytes=40 * 2**20
        ),
        cost_estimate=pl.CostEstimate(
            flops=4 * rows * weights[0].size // 1, bytes_accessed=4 * weights[0].size, transcendentals=0
        ),
        name="merge_scatter",
    )(*mixes, *weights)


ORDER = (
    "s0a", "S0a", "s1a", "T", "p0", "t1", "s2a", "a", "p1", "D", "P0", "t2", "x0", "f2a", "s3a", "c0",
    "k0", "m00", "x1", "p2", "t3", "p3", "f3a", "S1a", "S2a", "S3a", "c1", "k1", "m01", "m10", "m11",
    "x2", "x3", "u0", "v0", "c2", "m02", "m12", "c3", "m03", "m13", "P1", "u1", "k2", "m20", "m21",
    "m22", "m23", "k3", "m30", "m31", "m32", "m33",
)
AFTER = (
    "P2", "u2", "P3", "u3", "v1",
)
SIDES = 2
CORES = 2
PAIR = 2
SLICES = 4
SHARES = 1
OUT = SHARES
SMALL = SHARES + 1


def layer_fits(n, n_tp, shapes):
    count, heads_here, att_here, kv_here, length = shapes
    nz, nx = n // SIDES, n_tp // CORES
    return (
        n == nz * SIDES
        and nx == 2
        and n_tp == nx * CORES
        and nz == 2 * PAIR
        and nz == heads_here * CORES
        and kv_here == 1
        and att_here * HEAD_DIM == heads_here * V_DIM
        and count % 16 == 0
        and n_tp * count == length
        and length == 2 * WINDOW
        and length == 2 * BLOCK
        and nx * WINDOW == length
    )


def layer_scratch(n, n_tp, count, features, depth, width):
    nz = n // SIDES
    length = n_tp * count
    rows = nz * length
    slab = SIDES * width
    att_width = V_DIM + 2 * HEAD_DIM
    ret_width = 2 * RETAIN_KEY_SIZE + V_DIM
    parts = nz // CORES
    bf, f32 = jnp.bfloat16, jnp.float32
    dma = pltpu.SemaphoreType.DMA
    return dict(
        tok=pltpu.VMEM((rows, features), bf),
        ret_pack=pltpu.VMEM((parts, depth, ret_width), bf),
        att_pack=pltpu.VMEM((parts, depth, att_width), bf),
        ret_w=pltpu.VMEM((n * depth, ret_width), bf),
        att_w=pltpu.VMEM((n * depth, att_width), bf),
        out_pack=pltpu.VMEM((2, parts * V_DIM, width), bf),
        out_w=pltpu.VMEM((V_DIM, n * width), bf),
        tokens=pltpu.VMEM((count, features), bf),
        gain=pltpu.VMEM((1, features), f32),
        logs=pltpu.VMEM((parts, length), f32),
        sinks=pltpu.VMEM((1, parts * V_DIM // HEAD_DIM), f32),
        aux_here=pltpu.VMEM((8, length), f32),
        kv_pack=pltpu.VMEM((2 * HEAD_DIM, depth), bf),
        bias=pltpu.VMEM((2, WINDOW, 2 * WINDOW), f32),
        aux=pltpu.VMEM((n, 8, length), f32),
        total=pltpu.VMEM((rows, ret_width), f32),
        cosine=pltpu.VMEM((rows, RETAIN_KEY_SIZE), f32),
        sine=pltpu.VMEM((rows, RETAIN_KEY_SIZE), f32),
        fade_q=pltpu.VMEM((rows, RETAIN_KEY_SIZE), f32),
        fade_k=pltpu.VMEM((rows, RETAIN_KEY_SIZE), f32),
        decay=pltpu.VMEM((rows, length), f32),
        queries=pltpu.VMEM((rows, V_DIM), bf),
        keys=pltpu.VMEM((rows, RETAIN_KEY_SIZE), bf),
        values=pltpu.VMEM((rows, V_DIM), bf),
        inner=pltpu.VMEM((rows, V_DIM), f32),
        states=pltpu.VMEM((nz, SIDES, RETAIN_KEY_SIZE, V_DIM), bf),
        before=pltpu.VMEM((nz, SIDES, RETAIN_KEY_SIZE, V_DIM), f32),
        kv=pltpu.VMEM((4, nz, length + WINDOW, 2 * HEAD_DIM), bf),
        rim=pltpu.VMEM((nz, WINDOW, 2 * HEAD_DIM), bf),
        halo=pltpu.VMEM((nz, WINDOW, 2 * HEAD_DIM), bf),
        mix_far=pltpu.VMEM((nz, WINDOW, V_DIM), bf),
        mix_near=pltpu.VMEM((nz, WINDOW, V_DIM), bf),
        mix_in=pltpu.VMEM((nz, WINDOW, V_DIM), bf),
        out_wx=pltpu.VMEM((V_DIM, n * width), bf),
        part=pltpu.VMEM((WINDOW, slab), f32),
        result=pltpu.VMEM((count, n * width), bf),
        keep=pltpu.VMEM((nz, nz, count, slab), f32),
        core_out=pltpu.VMEM((nz, nz, count, slab), bf),
        core_in=pltpu.VMEM((nz, nz, count, slab), bf),
        z_out=pltpu.VMEM((nz, nz, count, slab), bf),
        z_in=pltpu.VMEM((nz, nz, count, slab), bf),
        tz_s=dma((2, nz)),
        tz_r=dma((nz, SLICES)),
        tx_s=dma((nz,)),
        tx_r=dma((nz, SLICES)),
        tc_s=dma((nz, 2)),
        tc_r=dma((nz, 2)),
        w_s=dma((SHARES + 2, nz, CORES)),
        w_r=dma((SHARES + 2, nz)),
        f_s=dma((SHARES + 2, nz)),
        f_r=dma((SHARES + 2, nz)),
        s_s=dma((nz,)),
        s_r=dma((nz,)),
        h_s=dma((1,)),
        h_r=dma((1,)),
        ox_s=dma((1,)),
        ox_r=dma((nz, SIDES)),
        rc_s=dma((1,)),
        rc_r=dma((nz, nz)),
        rx_s=dma((1,)),
        rx_r=dma((nz,)),
        rz_s=dma((1,)),
        rz_r=dma((nz, nz)),
        load=dma((8,)),
        store=dma((1,)),
    )


class Named:
    def __init__(self, names, refs):
        for name, ref in zip(names, refs):
            setattr(self, name, ref)


def dot_nt(a, b, **kw):
    return lax.dot_general(a, b, (((1,), (1,)), ((), ())), preferred_element_type=jnp.float32, **kw)


def dot_tn(a, b):
    return lax.dot_general(a, b, (((0,), (0,)), ((), ())), preferred_element_type=jnp.float32)


def dot_nn(a, b):
    return jnp.dot(a, b, preferred_element_type=jnp.float32)


def layer_kernel(n, n_tp, names, *refs):
    (tokens_ref, gain_ref, logs_ref, sinks_ref, rq_ref, rk_ref, rv_ref, aq_ref, ak_ref, av_ref, ro_ref, ao_ref) = refs[:12]
    out_ref = refs[12]
    m = Named(names, refs[13:])
    nz = n // SIDES
    parts = nz // CORES
    count, features = tokens_ref.shape
    depth = rq_ref.shape[0]
    width = out_ref.shape[1] // n
    length = n_tp * count
    slab = SIDES * width
    key_size = RETAIN_KEY_SIZE
    bf, f32 = jnp.bfloat16, jnp.float32

    sp, tp = lax.axis_index("sp"), lax.axis_index("tp")
    z, y = sp // SIDES, lax.rem(sp, SIDES)
    x, c = tp // CORES, lax.rem(tp, CORES)
    ny, nx, nc = 1 - y, 1 - x, 1 - c
    is_ret, is_att = c == 0, c == 1
    source_core = z // parts
    mate = z + 1 - 2 * lax.rem(z, PAIR)
    part_here = lax.rem(z, parts)

    def device(zz, yy, xx, cc):
        return (zz * SIDES + yy, xx * CORES + cc)

    def remote(src, dst, send_sem, recv_sem, target):
        return pltpu.make_async_remote_copy(
            src_ref=src,
            dst_ref=dst,
            send_sem=send_sem,
            recv_sem=recv_sem,
            device_id=target,
            device_id_type=MESH,
        )

    started = []

    def go(copy, condition=None):
        started.append((copy, condition))
        if condition is None:
            copy.start()
        else:
            pl.when(condition)(copy.start)

    def both(*conditions):
        conditions = [cond for cond in conditions if cond is not None]
        if not conditions:
            return None
        result = conditions[0]
        for cond in conditions[1:]:
            result = result & cond
        return result

    def await_recv(copy, condition=None):
        if condition is None:
            copy.wait_recv()
        else:
            pl.when(condition)(copy.wait_recv)

    moves = [
        (tokens_ref, m.tokens, 0),
        (gain_ref, m.gain, 1),
        (logs_ref, m.logs, 2),
        (sinks_ref, m.sinks, 3),
        (ak_ref, m.kv_pack.at[0:HEAD_DIM], 4),
        (av_ref, m.kv_pack.at[HEAD_DIM:], 4),
    ]
    for part in range(parts):
        wide = slice(part * V_DIM, (part + 1) * V_DIM)
        thin = slice(part * key_size, (part + 1) * key_size)
        moves += [
            (rq_ref.at[:, thin], m.ret_pack.at[part, :, 0:key_size], 5),
            (rk_ref.at[:, thin], m.ret_pack.at[part, :, key_size : 2 * key_size], 5),
            (rv_ref.at[:, wide], m.ret_pack.at[part, :, 2 * key_size :], 5),
            (aq_ref.at[:, wide], m.att_pack.at[part, :, 0:V_DIM], 6),
        ]
    moves += [(ro_ref, m.out_pack.at[0], 7), (ao_ref, m.out_pack.at[1], 7)]
    for src, dst, index in moves:
        pltpu.make_async_copy(src, dst, m.load.at[index]).start()

    def loaded(piece, index):
        pltpu.make_async_copy(piece, piece, m.load.at[index]).wait()

    barrier = pltpu.get_barrier_semaphore()
    peers = [device(z, ny, x, c), device(z, y, nx, c), device(z, y, x, nc)]
    for step in range(1, nz):
        for cc in range(CORES):
            peers.append(device(lax.rem(z + step, nz), y, x, cc))
    for peer in peers:
        pl.semaphore_signal(barrier, inc=1, device_id=peer, device_id_type=MESH)

    def token_rows(zz, xx, cc):
        return pl.ds(pl.multiple_of(zz * length + xx * (CORES * count) + cc * count, count), count)

    loaded(m.tokens, 0)
    loaded(m.gain, 1)
    tok_float = m.tokens[...].astype(f32)
    scale = lax.rsqrt(jnp.mean(tok_float * tok_float, axis=-1, keepdims=True) + epsilon)
    m.tok[token_rows(z, x, c), :] = (tok_float * scale * m.gain[...]).astype(bf)
    loaded(m.logs, 2)
    loaded(m.sinks, 3)
    loaded(m.kv_pack, 4)
    loaded(m.ret_pack, 5)
    loaded(m.att_pack.at[:, :, 0:V_DIM], 6)
    loaded(m.out_pack, 7)
    many = m.sinks.shape[1]
    m.aux_here[...] = jnp.zeros_like(m.aux_here)
    m.aux_here[0:parts, :] = m.logs[...]
    m.aux_here[parts : parts + 1, 0:many] = m.sinks[...]
    pair = jnp.transpose(m.kv_pack[...].astype(f32)).astype(bf)
    for part in range(parts):
        m.att_pack[part, :, V_DIM:] = pair
    pl.semaphore_wait(barrier, len(peers))

    def token_at(zz, xx, cc, cut):
        if cut is None:
            return m.tok.at[token_rows(zz, xx, cc)]
        wide = features // SLICES
        return m.tok.at[token_rows(zz, xx, cc), cut * wide : (cut + 1) * wide]

    def token_z(origin, way, cut=None):
        piece = token_at(origin, x, c, cut)
        return remote(
            piece,
            piece,
            m.tz_s.at[way, origin],
            m.tz_r.at[origin, 0 if cut is None else cut],
            device(z + 1 - 2 * way, y, x, c),
        )

    def token_x(origin, side, cut=None):
        piece = token_at(origin, side, c, cut)
        return remote(
            piece, piece, m.tx_s.at[origin], m.tx_r.at[origin, 0 if cut is None else cut], device(z, y, nx, c)
        )

    def token_core(origin, side, core, cut=None):
        piece = token_at(origin, side, core, cut)
        return remote(piece, piece, m.tc_s.at[origin, side], m.tc_r.at[origin, side], device(z, y, x, nc))

    def send_rows(maker, cut, condition, *place):
        copy = maker(*place, cut)
        if condition is None:
            copy.start()
        else:
            pl.when(condition)(copy.start)
        if cut == 0:
            started.append((maker(*place), condition))

    can_go = (z < nz - 1, z > 0)

    def spread(origin, cut, condition, ways):
        for way in ways:
            send_rows(token_z, cut, both(condition, can_go[way]), origin, way)
        send_rows(token_x, cut, condition, origin, x)
        send_rows(token_core, cut, condition, origin, x, c)

    def weight_rows(zz, yy, share):
        start = (zz * SIDES + yy) * depth + share * (depth // SHARES)
        return pl.ds(pl.multiple_of(start, depth // SHARES), depth // SHARES)

    near, distant = c == z // parts, c != z // parts
    outer = (z == 0) | (z == nz - 1)
    inside = jnp.logical_not(outer)

    def toward(step):
        return (z, mate, lax.rem(z + PAIR, nz), nz - 1 - z)[step]

    def send_weights(step, kind, where=None):
        target_z = toward(step)
        part = lax.rem(target_z, parts)
        valid = both(near if step < PAIR else distant, where)
        first = len(started)
        for core in range(CORES):
            target = device(target_z, y, x, core)
            pack = m.ret_pack if core == 0 else m.att_pack
            if kind < SHARES:
                high = depth // SHARES
                src = pack.at[part, kind * high : (kind + 1) * high]
            elif kind == OUT:
                src = m.out_pack.at[core, pl.ds(pl.multiple_of(part * V_DIM, V_DIM), V_DIM)]
            else:
                src = m.aux_here
            dst = weight_piece(kind, z, y, core)
            away = valid if step else valid & (c != core)
            go(remote(src, dst, m.w_s.at[kind, step, core], m.w_r.at[kind, z], target), away)
            if step == 0:

                @pl.when(valid & (c == core))
                def _():
                    dst[...] = src[...]

        return started[first:]

    def finish(copies):
        for entry in copies:
            started[:] = [kept for kept in started if kept is not entry]
            pl.when(entry[1])(entry[0].wait_send)

    def out_columns(zz, yy):
        return pl.ds(pl.multiple_of((zz * SIDES + yy) * width, width), width)

    def weight_piece(kind, zz, yy, core):
        if kind < SHARES:
            return (m.ret_w if core == 0 else m.att_w).at[weight_rows(zz, yy, kind)]
        if kind == OUT:
            return m.out_w.at[:, out_columns(zz, yy)]
        return m.aux.at[zz * SIDES + yy]

    def per_core(kind):
        return ((0, is_ret), (1, is_att)) if kind < SHARES else ((0, None),)

    def pass_weights(kind, step):
        zz = toward(step)
        other = jnp.logical_not((zz == z) & (c == source_core))
        for core, condition in per_core(kind):
            piece = weight_piece(kind, zz, y, core)
            await_recv(
                remote(piece, piece, m.f_s.at[kind, zz], m.w_r.at[kind, zz], device(z, ny, x, c)),
                both(condition, other),
            )
            go(
                remote(piece, piece, m.f_s.at[kind, zz], m.f_r.at[kind, zz], device(z, ny, x, c)),
                condition,
            )

    def take_weights(kind, zz):
        for core, condition in per_core(kind):
            piece = weight_piece(kind, zz, ny, core)
            await_recv(
                remote(piece, piece, m.f_s.at[kind, zz], m.f_r.at[kind, zz], device(z, ny, x, c)), condition
            )

    for step in range(nz):
        send_weights(step, SMALL)
    for cut in range(SLICES):
        spread(z, cut, None, (0, 1))

    def pass_tokens(step):
        for cut in range(SLICES):
            for way in range(2):
                origin = z - step if way == 0 else z + step
                valid = origin >= 0 if way == 0 else origin < nz
                await_recv(token_z(origin, way, cut), valid)
                spread(origin, cut, valid, (way,))

    def across_tokens(step):
        origin = toward(step)
        for cut in range(SLICES):
            await_recv(token_x(origin, nx, cut))
            send_rows(token_core, cut, None, origin, nx, c)

    def tables():
        @pl.when(is_ret)
        def make_tables():
            lane = lax.broadcasted_iota(jnp.int32, (length, key_size), 1)
            row = lax.broadcasted_iota(jnp.int32, (length, key_size), 0)
            half = key_size // 2
            inverse = jnp.exp(
                lax.rem(lane, half).astype(f32) * (-math.log(rope_base) / half)
            )
            sign = jnp.where(lane < half, -1.0, 1.0)

            def table(zz, carry):
                where = pl.ds(pl.multiple_of(zz * length, length), length)
                angles = (row + (zz * SIDES + y) * length).astype(f32) * inverse
                m.cosine[where, :] = jnp.cos(angles)
                m.sine[where, :] = jnp.sin(angles) * sign
                return carry

            lax.fori_loop(0, nz, table, 0)

    def decays():
        for zz in range(nz):
            take_weights(SMALL, zz)

        @pl.when(is_ret)
        def _():
            lower = (
                lax.broadcasted_iota(jnp.int32, (length, length), 0)
                >= lax.broadcasted_iota(jnp.int32, (length, length), 1)
            )
            lower_float = lower.astype(f32)
            mine = [m.aux[zz * SIDES + y, pl.ds(part_here, 1), :] for zz in range(nz)]
            logs = jnp.concatenate(mine * (8 // nz), axis=0)
            by_row = dot_nt(logs, lower_float, precision=lax.Precision.HIGHEST)
            by_column = dot_nt(lower_float, logs, precision=lax.Precision.HIGHEST)
            for zz in range(nz):
                rows = slice(zz * length, (zz + 1) * length)
                column = by_column[:, zz : zz + 1]
                closing = by_column[length - 1 : length, zz : zz + 1]
                within = jnp.minimum(column - by_row[zz : zz + 1, :], 0.0)
                m.decay[rows, :] = jnp.where(lower, jnp.exp(within), 0.0)
                m.fade_q[rows, :] = jnp.broadcast_to(jnp.exp(column), (length, key_size))
                m.fade_k[rows, :] = jnp.broadcast_to(jnp.exp(closing - column), (length, key_size))

    def run_rows(zz):
        return pl.ds(pl.multiple_of(zz * length, length), length)

    def take_tokens(step):
        origin = toward(step)
        for side in (x, nx):
            await_recv(token_core(origin, side, nc))

    def out_x(step, side):
        columns = out_columns(toward(step), side)
        return remote(
            m.out_w.at[:, columns],
            m.out_wx.at[:, columns],
            m.ox_s.at[0],
            m.ox_r.at[step, side],
            device(z, y, nx, c),
        )

    fresh = set()

    def project(step, run):
        columns = pl.ds(pl.multiple_of(toward(step) * SIDES * depth, SIDES * depth), SIDES * depth)
        rows = run_rows(toward(run))
        first = run not in fresh
        fresh.add(run)

        def accumulate(held):
            lanes = slice(0, held.shape[1])
            product = dot_nn(m.tok[rows, columns], held[columns, :])
            m.total[rows, lanes] = product if first else m.total[rows, lanes] + product

        pl.when(is_ret)(lambda: accumulate(m.ret_w))
        pl.when(is_att)(lambda: accumulate(m.att_w))

    everyone = dict(a=None, o=outer, i=inside)
    sent = {}
    def perform(word):
        step = int(word[1]) if len(word) > 1 else 0
        if word[0] == "s":
            for kind in range(SHARES):
                sent[word, kind] = send_weights(step, kind, everyone[word[2]])
        elif word[0] == "f":
            for kind in range(SHARES):
                finish(sent["s" + word[1:], kind])
        elif word[0] == "p":
            for kind in range(SHARES):
                pass_weights(kind, step)
        elif word[0] == "S":
            sent[word] = send_weights(step, OUT, everyone[word[2]])
        elif word[0] == "P":
            pass_weights(OUT, step)
        elif word[0] == "t":
            pass_tokens(step)
        elif word[0] == "x":
            across_tokens(step)
        elif word[0] == "u":
            out_x(step, y).start()
        elif word[0] == "v":
            take_weights(OUT, toward(step))
            out_x(step, ny).start()
        elif word[0] == "c":
            take_tokens(step)
        elif word[0] == "k":
            for kind in range(SHARES):
                take_weights(kind, toward(step))
        elif word[0] == "m":
            project(step, int(word[2]))
        elif word[0] == "T":
            tables()
        elif word[0] == "D":
            decays()
        elif word[0] == "a":
            for aux_step in range(nz):
                pass_weights(SMALL, aux_step)

    for word in ORDER:
        perform(word)

    def state_copy(zz):
        piece = m.states.at[zz, y]
        return remote(piece, piece, m.s_s.at[zz], m.s_r.at[zz], device(z, ny, x, c))

    def state_arrival(zz):
        piece = m.states.at[zz, ny]
        return remote(piece, piece, m.s_s.at[zz], m.s_r.at[zz], device(z, ny, x, c))

    halo_copy = remote(m.rim, m.halo, m.h_s.at[0], m.h_r.at[0], device(z, ny, x, c))

    @pl.when(is_ret)
    def _():
        def project_run(zz, carry):
            rows = run_rows(zz)
            product = m.total[rows, :].astype(bf)
            cosine, sine = m.cosine[rows, :], m.sine[rows, :]

            def turn(values):
                values = values.astype(f32)
                return values * cosine + pltpu.roll(values, key_size // 2, 1) * sine

            m.queries[rows, 0:key_size] = turn(product[:, 0:key_size]).astype(bf)
            key = (turn(product[:, key_size : 2 * key_size]) * key_size ** (-0.5)).astype(bf)
            m.keys[rows, :] = key
            value = product[:, 2 * key_size :]
            m.values[rows, :] = value
            faded = (key.astype(f32) * m.fade_k[rows, :]).astype(bf)
            m.states[zz, y] = dot_tn(faded, value).astype(bf)
            state_copy(zz).start()
            return carry

        lax.fori_loop(0, nz, project_run, 0)

    lane_kv = lax.broadcasted_iota(jnp.int32, (WINDOW, 2 * HEAD_DIM), 1)

    def place(zz, spot, packed):
        where = pl.ds(spot * WINDOW, WINDOW)
        packed = packed.astype(f32)
        low = jnp.where(lane_kv < HEAD_DIM, packed, 0.0)
        turned = pltpu.roll(packed, HEAD_DIM, 1)
        m.kv[0, zz, where, :] = low.astype(bf)
        m.kv[1, zz, where, :] = pltpu.roll(low, HEAD_DIM, 1).astype(bf)
        m.kv[2, zz, where, :] = jnp.where(lane_kv < HEAD_DIM, turned, 1.0).astype(bf)
        m.kv[3, zz, where, :] = jnp.where(lane_kv < HEAD_DIM, 1.0, packed).astype(bf)

    @pl.when(is_att)
    def _():
        def project_run(zz, carry):
            rows = run_rows(zz)
            product = m.total[rows, 0 : m.att_w.shape[1]].astype(bf)
            m.queries[rows, :] = (product[:, 0:V_DIM].astype(f32) * HEAD_DIM ** (-0.5)).astype(bf)
            for spot in range(2):
                place(zz, spot + 1, product[spot * WINDOW : (spot + 1) * WINDOW, V_DIM:])
            m.rim[zz] = product[length - WINDOW :, V_DIM:]
            return carry

        lax.fori_loop(0, nz, project_run, 0)
        halo_copy.start()

    far = jnp.where(z < PAIR, nz - 1, 0)

    def home(turn):
        near = far + jnp.where(z < PAIR, -1, 1)
        if isinstance(turn, int):
            return (far, near, mate, z)[turn]
        return jnp.where(turn == 0, far, jnp.where(turn == 1, near, jnp.where(turn == 2, mate, z)))

    def core_copy(turn, piece):
        return remote(
            m.core_out.at[turn, piece],
            m.core_in.at[turn, piece],
            m.rc_s.at[0],
            m.rc_r.at[turn, piece],
            device(z, y, x, nc),
        )

    def mix_copy(turn):
        return remote(
            m.mix_far.at[turn], m.mix_in.at[turn], m.rx_s.at[0], m.rx_r.at[turn], device(z, y, nx, c)
        )

    def z_copy(turn, piece, target_z, slot):
        spot = toward(piece)
        return remote(
            m.z_out.at[turn, spot],
            m.z_in.at[slot, spot],
            m.rz_s.at[0],
            m.rz_r.at[slot, spot],
            device(target_z, y, x, c),
        )

    def half_rows(cc):
        return pl.ds(pl.multiple_of(cc * count, count), count)

    def slab_columns(piece):
        return pl.ds(pl.multiple_of(toward(piece) * slab, slab), slab)

    def block_rows(zz, xx):
        return pl.ds(pl.multiple_of(zz * length + xx * WINDOW, WINDOW), WINDOW)

    def take_out(piece):
        for side in (y, ny):
            out_x(piece, side).wait_recv()

    def emit(turn, piece):
        columns = slab_columns(piece)
        m.part[...] = dot_nn(m.mix_near[turn], m.out_w[:, columns]) + dot_nn(
            m.mix_in[turn], m.out_wx[:, columns]
        )
        m.core_out[turn, piece] = m.part[half_rows(nc), :].astype(bf)
        core_copy(turn, piece).start()
        m.keep[turn, piece] = m.part[half_rows(c), :]

    def joined(turn, piece):
        core_copy(turn, piece).wait_recv()
        return m.keep[turn, piece] + m.core_in[turn, piece].astype(f32)

    def pass_sum(turn, piece):
        m.z_out[turn, toward(piece)] = joined(turn, piece).astype(bf)
        z_copy(turn, piece, mate, turn).start()

    def merge_sum(turn, piece):
        z_copy(turn, piece, mate, turn).wait_recv()
        merged = joined(turn, piece) + m.z_in[turn, toward(piece)].astype(f32)
        m.z_out[turn, toward(piece)] = merged.astype(bf)
        z_copy(turn, piece, home(turn), nz - 1).start()

    def first_sums(turn, piece):
        if turn < PAIR:
            pl.when(outer)(lambda: pass_sum(turn, piece))
        elif turn < nz - 1:
            pass_sum(turn, piece)

    early, late = (0, 1), (2, 3)

    def rounds(block):
        for turn in range(nz + 1):
            if turn < nz:
                block(turn)
            if turn == 0:
                perform("v2")
            if turn == 1:
                perform("v3")
                for piece in early:
                    take_out(piece)
            if turn > 0:
                mix_copy(turn - 1).wait_recv()
                for piece in early:
                    emit(turn - 1, piece)
                for piece in early:
                    first_sums(turn - 1, piece)

    for word in AFTER:
        perform(word)

    @pl.when(is_ret)
    def _():
        def inner_run(zz, carry):
            rows = run_rows(zz)
            scores = dot_nt(m.queries[rows, 0:key_size], m.keys[rows, :]) * m.decay[rows, :]
            m.inner[rows, :] = dot_nn(scores.astype(bf), m.values[rows, :])
            return carry

        lax.fori_loop(0, nz, inner_run, 0)
        totals = [
            jnp.sum(m.aux[spot, pl.ds(part_here, 1), :], axis=1, keepdims=True) for spot in range(n)
        ]
        for zz in range(nz):
            state_arrival(zz).wait_recv()
        running = jnp.zeros((key_size, V_DIM), f32)
        for zz in range(nz):
            for yy in range(SIDES):
                m.before[zz, yy] = running
                running = running * jnp.exp(totals[zz * SIDES + yy]) + m.states[zz, yy].astype(f32)

        def finish_block(zz, xx):
            rows = block_rows(zz, xx)
            query = (m.queries[rows, 0:key_size].astype(f32) * m.fade_q[rows, :]).astype(bf)
            state = m.before[zz, y]
            high = state.astype(bf)
            low = (state - high.astype(f32)).astype(bf)
            total = m.inner[rows, :] + (dot_nn(query, high) + dot_nn(query, low))
            total = total * lax.rsqrt(jnp.mean(total * total, axis=-1, keepdims=True) + epsilon)
            return total.astype(bf)

        def both_blocks(turn):
            m.mix_far[turn] = finish_block(home(turn), nx)
            mix_copy(turn).start()
            m.mix_near[turn] = finish_block(home(turn), x)

        rounds(both_blocks)
        for zz in range(nz):
            state_copy(zz).wait_send()

    @pl.when(is_att)
    def _():
        row = lax.broadcasted_iota(jnp.int32, (WINDOW, 2 * WINDOW), 0)
        column = lax.broadcasted_iota(jnp.int32, (WINDOW, 2 * WINDOW), 1)
        band = (column > row) & (column <= row + WINDOW)
        m.bias[0] = jnp.where(band & (column >= WINDOW), 0.0, masked_out)
        m.bias[1] = jnp.where(band, 0.0, masked_out)
        sink_row = m.aux[sp, parts : parts + 1, 0:LANES]
        sink_lane = lax.broadcasted_iota(jnp.int32, (1, LANES), 1)
        heads = V_DIM // HEAD_DIM
        sinks = [
            jnp.sum(
                jnp.where(sink_lane == part_here * heads + head, sink_row, 0.0), axis=1, keepdims=True
            )
            for head in range(heads)
        ]
        def take_halo():
            halo_copy.wait_recv()
            for zz in range(nz):
                place(zz, 0, m.halo[jnp.maximum(zz - 1 + y, 0)])

        pl.when(x == 1)(take_halo)
        def attend_block(zz, xx, target):
            bias = m.bias[jnp.minimum(zz + y + xx, 1)]
            where = pl.ds(pl.multiple_of(xx * WINDOW, WINDOW), 2 * WINDOW)
            rows = block_rows(zz, xx)
            first = lane_kv < HEAD_DIM
            for pair in range(heads // 2):
                lanes = slice(pair * LANES, (pair + 1) * LANES)
                query = m.queries[rows, lanes]
                terms, ends = [], []
                for side in range(2):
                    sink = sinks[pair * 2 + side]
                    scores = dot_nt(query, m.kv[side, zz, where, :]) + bias
                    highest = jnp.maximum(jnp.max(scores, axis=-1, keepdims=True), sink)
                    lifted = jnp.exp(scores - highest).astype(bf)
                    ends.append(jnp.exp(sink - highest))
                    terms.append(dot_nn(lifted, m.kv[2 + side, zz, where, :]))
                below = pltpu.roll(jnp.where(first, terms[1], terms[0]), HEAD_DIM, 1)
                below = below + jnp.where(first, ends[0], ends[1])
                mixed = jnp.where(first, terms[0], terms[1]) / below
                target[:, lanes] = mixed.astype(bf)

        def both_blocks(turn):
            attend_block(home(turn), nx, m.mix_far.at[turn])
            mix_copy(turn).start()
            if turn == 0:
                pl.when(x == 0)(take_halo)
            attend_block(home(turn), x, m.mix_near.at[turn])

        rounds(both_blocks)
        halo_copy.wait_send()

    def merge_sums(piece):
        for turn in range(PAIR):
            merge_sum(turn, piece)

    for piece in early:
        pl.when(inside)(functools.partial(merge_sums, piece))
    for piece in late:
        take_out(piece)
        for turn in range(nz):
            emit(turn, piece)
        for turn in range(nz):
            first_sums(turn, piece)
    for piece in late:
        pl.when(inside)(functools.partial(merge_sums, piece))
    for piece in range(nz):
        total = joined(nz - 1, piece)
        for slot in (nz - 2, nz - 1):
            z_copy(0, piece, mate, slot).wait_recv()
            total = total + m.z_in[slot, toward(piece)].astype(f32)
        columns = slab_columns(piece)
        m.result[:, columns] = total.astype(bf)
        pltpu.make_async_copy(m.result.at[:, columns], out_ref.at[:, columns], m.store.at[0]).start()

    for copy, condition in started:
        if condition is None:
            copy.wait_send()
        else:
            pl.when(condition)(copy.wait_send)
    everything = device(z, y, x, nc)
    remote(m.core_out, m.core_in, m.rc_s.at[0], m.rc_r.at[0, 0], everything).wait_send()
    remote(m.mix_far, m.mix_in, m.rx_s.at[0], m.rx_r.at[0], everything).wait_send()
    remote(m.out_w, m.out_wx, m.ox_s.at[0], m.ox_r.at[0, 0], everything).wait_send()
    sums = m.z_out.at[0 : nz - 1]
    remote(sums, sums, m.rz_s.at[0], m.rz_r.at[0, 0], everything).wait_send()
    pltpu.make_async_copy(m.result, out_ref, m.store.at[0]).wait()


def layer(n, n_tp, tokens, norm_gain, logs, sinks, *weights):
    count, features = tokens.shape
    depth = weights[0].shape[0]
    width = weights[-1].shape[1]
    scratch = layer_scratch(n, n_tp, count, features, depth, width)
    return pl.pallas_call(
        functools.partial(layer_kernel, n, n_tp, tuple(scratch)),
        out_shape=jax.ShapeDtypeStruct((count, n * width), jnp.bfloat16),
        in_specs=[pl.BlockSpec(memory_space=pltpu.HBM)] * (4 + len(weights)),
        out_specs=pl.BlockSpec(memory_space=pltpu.HBM),
        scratch_shapes=list(scratch.values()),
        compiler_params=pltpu.CompilerParams(
            collective_id=3, has_side_effects=True, vmem_limit_bytes=60 * 2**20
        ),
        cost_estimate=pl.CostEstimate(flops=4 * 2**30, bytes_accessed=16 * 2**20, transcendentals=0),
        name="layer",
    )(tokens, norm_gain.reshape(1, -1), logs, sinks.reshape(1, -1), *weights)


def on_device(
    tokens,
    norm_gain,
    ret_query,
    ret_key,
    ret_value,
    log_decay,
    att_query,
    att_key,
    att_value,
    sink_logits,
    ret_out,
    att_out,
):
    n, n_tp = lax.axis_size("sp"), lax.axis_size("tp")
    length = log_decay.shape[1]
    shapes = (
        tokens.shape[0],
        log_decay.shape[0],
        sink_logits.shape[0],
        att_key.shape[1] // HEAD_DIM,
        length,
    )
    if layer_fits(n, n_tp, shapes):
        return layer(
            n, n_tp, tokens, norm_gain, log_decay, sink_logits,
            ret_query, ret_key, ret_value, att_query, att_key.T, att_value.T, ret_out, att_out,
        )
    tok_float = tokens.astype(jnp.float32)
    normed = (
        tok_float
        * lax.rsqrt(jnp.mean(tok_float * tok_float, axis=-1, keepdims=True) + epsilon)
        * norm_gain
    ).astype(jnp.bfloat16)
    weights = (ret_query, ret_key, ret_value, att_query, att_key, att_value)
    widths = [weight.shape[1] for weight in weights]
    points = [sum(widths[:index]) for index in range(1, len(widths))]
    aligned = ret_out.shape[1] % LANES == 0
    local_logs = jnp.sum(log_decay, axis=1)
    log_tile = jnp.broadcast_to(
        jnp.pad(local_logs, (0, -local_logs.shape[0] % 8))[:, None], (-(-local_logs.shape[0] // 8) * 8, LANES)
    )
    projected, logs = project(normed, jnp.concatenate(weights, axis=1), log_tile, n, n_tp)
    logs = logs[:, : local_logs.shape[0], 0]
    sections = jnp.split(projected, points, axis=1)
    tok_count = sections[0].shape[0]
    anchor = lax.axis_index("sp") * tok_count
    positions = anchor + jnp.arange(tok_count, dtype=jnp.int32)
    query_ret = rotate(sections[0].reshape(tok_count, -1, RETAIN_KEY_SIZE), positions).astype(
        jnp.bfloat16
    )
    key_ret = (
        rotate(sections[1].reshape(tok_count, -1, RETAIN_KEY_SIZE), positions)
        * RETAIN_KEY_SIZE ** (-0.5)
    ).astype(jnp.bfloat16)
    value_ret = sections[2].reshape(tok_count, -1, V_DIM)
    stacked = projected[:, points[3] :]
    ret_mix, rim, wholes = retention_path(
        query_ret,
        key_ret,
        value_ret,
        log_decay,
        stacked[tok_count - WINDOW :],
        logs,
        (ret_out, att_out) if aligned else (),
    )
    if not aligned:
        wholes = [
            lax.all_gather(weight, "sp", axis=1, tiled=True)[None] for weight in (ret_out, att_out)
        ]
    att_mix = attention_path(sections[3], stacked, rim, sink_logits, anchor)
    return merge((ret_mix, att_mix), wholes, n_tp)


def solution(mesh):
    in_specs = (
        P(("sp", "tp"), None),
        P(),
        P("sp", "tp"),
        P("sp", "tp"),
        P("sp", "tp"),
        P("tp", "sp"),
        P("sp", "tp"),
        P("sp", "tp"),
        P("sp", "tp"),
        P("tp"),
        P("tp", "sp"),
        P("tp", "sp"),
    )
    out_specs = P(("sp", "tp"), None)
    return jax.shard_map(
        on_device, mesh=mesh, in_specs=in_specs, out_specs=out_specs, check_vma=False
    )
```

```python
import functools
import math

import jax
import jax.numpy as jnp
from jax import lax
from jax.experimental import pallas as pl
from jax.experimental.pallas import tpu as pltpu
from jax.sharding import PartitionSpec as P

MESH = pl.DeviceIdType.MESH
LANES = 128

RETAIN_KEY_SIZE = 128
V_DIM = 256
HEAD_DIM = 64
WINDOW = 128
BLOCK = 128


epsilon = 1e-05
rope_base = 10000.0
masked_out = -1e30


def rotate(values, positions):
    half_dim = values.shape[-1] // 2
    inverse = rope_base ** (-jnp.arange(half_dim, dtype=jnp.float32) / half_dim)
    angles = positions.astype(jnp.float32)[:, None] * inverse[None, :]
    cosine = jnp.cos(angles)[:, None, :]
    sine_part = jnp.sin(angles)[:, None, :]
    first_half = values[..., :half_dim].astype(jnp.float32)
    second_half = values[..., half_dim:].astype(jnp.float32)
    return jnp.concatenate(
        [
            first_half * cosine - second_half * sine_part,
            second_half * cosine + first_half * sine_part,
        ],
        axis=-1,
    )


def retention_path(query_ret, key_ret, value_ret, log_decay, rim, logs, weights):
    tok_count, heads_here = (query_ret.shape[0], query_ret.shape[1])
    blocks = tok_count // BLOCK
    q_blocks = query_ret.reshape(blocks, BLOCK, heads_here, RETAIN_KEY_SIZE)
    k_blocks = key_ret.reshape(blocks, BLOCK, heads_here, RETAIN_KEY_SIZE)
    v_blocks = value_ret.reshape(blocks, BLOCK, heads_here, V_DIM)
    running = jnp.cumsum(log_decay.reshape(heads_here, blocks, BLOCK), axis=-1)
    closing = running[:, :, -1:]
    within = running[:, :, :, None] - running[:, :, None, :]
    causal_mask = jnp.arange(BLOCK)[:, None] >= jnp.arange(BLOCK)[None, :]
    weighting = jnp.where(causal_mask, jnp.exp(jnp.minimum(within, 0.0)), 0.0)
    scores = (
        jnp.einsum("nihd,njhd->hnij", q_blocks, k_blocks, preferred_element_type=jnp.float32)
        * weighting
    )
    in_block = jnp.einsum(
        "hnij,njhv->nihv", scores.astype(jnp.bfloat16), v_blocks, preferred_element_type=jnp.float32
    )
    key_fade = (
        k_blocks.astype(jnp.float32) * jnp.exp(closing - running).transpose(1, 2, 0)[..., None]
    ).astype(jnp.bfloat16)
    contrib = jnp.einsum("njhd,njhv->nhdv", key_fade, v_blocks, preferred_element_type=jnp.float32)
    block_fade = jnp.exp(closing[:, :, 0]).T

    def advance(carried, entry_pair):
        addend, factor = entry_pair
        return (carried * factor[:, None, None] + addend, carried)

    final_state, before = lax.scan(
        advance, jnp.zeros((heads_here, RETAIN_KEY_SIZE, V_DIM), jnp.float32), (contrib, block_fade)
    )
    n = lax.axis_size("sp")
    place = lax.axis_index("sp")
    before_rim, states, *wholes = exchange(
        rim, final_state.astype(jnp.bfloat16).reshape(2, -1, V_DIM), weights, n
    )
    states = states.reshape(n, heads_here, RETAIN_KEY_SIZE, V_DIM)
    spots = jnp.arange(n)
    between = (spots[None, :] > spots[:, None]) & (spots[None, :] < place)
    spans = jnp.sum(jnp.where(between[:, :, None], logs[None], 0.0), axis=1)
    shares = jnp.where((spots < place)[:, None], jnp.exp(spans), 0.0)
    arrived = jnp.sum(shares[:, :, None, None] * states.astype(jnp.float32), axis=0)
    leading = jnp.cumsum(closing[:, :, 0], axis=1) - closing[:, :, 0]
    before = before + arrived[None] * jnp.exp(leading).T[:, :, None, None]
    query_fade = (
        q_blocks.astype(jnp.float32) * jnp.exp(running).transpose(1, 2, 0)[..., None]
    ).astype(jnp.bfloat16)
    carried_term = jnp.einsum(
        "nihd,nhdv->nihv", query_fade.astype(jnp.float32), before, precision=lax.Precision.HIGHEST
    )
    final_product = in_block + carried_term
    final_product = final_product * lax.rsqrt(
        jnp.mean(final_product * final_product, axis=-1, keepdims=True) + epsilon
    )
    return final_product.reshape(tok_count, heads_here * V_DIM).astype(jnp.bfloat16), before_rim, wholes


def attention_path(query_att, stacked, window_rim, sink_logits, anchor):
    tok_count = query_att.shape[0]
    kv_here = stacked.shape[1] // (2 * HEAD_DIM)
    group_size = query_att.shape[1] // (kv_here * HEAD_DIM)
    blocks = tok_count // WINDOW
    extended = jnp.concatenate([window_rim, stacked], axis=0).reshape(
        blocks + 1, WINDOW, 2, kv_here, HEAD_DIM
    )
    paired = jnp.concatenate([extended[:-1], extended[1:]], axis=1)
    keys_pair = paired[:, :, 0]
    values_pair = paired[:, :, 1]
    q_blocks = query_att.reshape(blocks, WINDOW, kv_here, group_size, HEAD_DIM)
    scores = jnp.einsum(
        "nihgd,njhd->nhgij", q_blocks, keys_pair, preferred_element_type=jnp.float32
    ) * HEAD_DIM ** (-0.5)
    query_pos = anchor + (jnp.arange(blocks) * WINDOW)[:, None] + jnp.arange(WINDOW)[None, :]
    key_pos = (
        anchor + (jnp.arange(blocks) * WINDOW - WINDOW)[:, None] + jnp.arange(2 * WINDOW)[None, :]
    )
    allowed = (
        (key_pos[:, None, :] >= 0)
        & (key_pos[:, None, :] <= query_pos[:, :, None])
        & (query_pos[:, :, None] - key_pos[:, None, :] < WINDOW)
    )
    scores = jnp.where(allowed[:, None, None], scores, masked_out)
    sink_logit = sink_logits.reshape(kv_here, group_size)[None, :, :, None]
    highest = jnp.maximum(jnp.max(scores, axis=-1), sink_logit)
    lifted = jnp.exp(scores - highest[..., None])
    denominator = jnp.sum(lifted, axis=-1) + jnp.exp(sink_logit - highest)
    attn_weights = (lifted / denominator[..., None]).astype(jnp.bfloat16)
    final_product = jnp.einsum(
        "nhgij,njhd->nihgd", attn_weights, values_pair, preferred_element_type=jnp.float32
    )
    return final_product.reshape(tok_count, kv_here * group_size * HEAD_DIM).astype(jnp.bfloat16)


def ring_spot(index, count):
    half = count // 2
    return jnp.where(lax.rem(index, 2) == 0, index // 2, count - 1 - index // 2)


def ring_member(spot, count):
    half = count // 2
    return jnp.where(spot < half, 2 * spot, 2 * (count - 1 - spot) + 1)


def project_kernel(n, n_tp, normed_ref, pack_ref, log_ref, out_ref, logs_ref, rows_ref, held, total, sems, tok_sems):
    sp, tp = lax.axis_index("sp"), lax.axis_index("tp")
    depth, width = pack_ref.shape
    count = normed_ref.shape[0]
    half = n // 2
    spot = ring_spot(sp, n)
    ahead = ring_member(lax.rem(spot + 1, n), n)
    behind = ring_member(lax.rem(spot + n - 1, n), n)

    barrier = pltpu.get_barrier_semaphore()
    for peer in (ahead, behind):
        pl.semaphore_signal(barrier, inc=1, device_id=(peer, tp), device_id_type=MESH)
    for step in range(1, n_tp):
        pl.semaphore_signal(
            barrier, inc=1, device_id=(sp, lax.rem(tp + step, n_tp)), device_id_type=MESH
        )
    pl.semaphore_wait(barrier, 2 + n_tp - 1)

    def rows_of(member):
        return pl.ds(pl.multiple_of(member * depth, depth), depth)

    middle = (width // LANES + 1) // 2 * LANES
    spans = (pl.ds(0, middle), pl.ds(middle, width - middle))

    def owner(direction, distance):
        shift = n - distance if direction == 0 else distance
        return ring_member(lax.rem(spot + shift, n), n)

    def send(direction, step, part):
        member = owner(direction, step - 1)
        if part == 2:
            return pltpu.make_async_remote_copy(
                src_ref=log_ref if step == 1 else logs_ref.at[member],
                dst_ref=logs_ref.at[member],
                send_sem=sems.at[0, direction, step - 1, part],
                recv_sem=sems.at[1, direction, step - 1, part],
                device_id=(ahead if direction == 0 else behind, tp),
                device_id_type=MESH,
            )
        source = pack_ref.at[:, spans[part]] if step == 1 else held.at[rows_of(member), spans[part]]
        return pltpu.make_async_remote_copy(
            src_ref=source,
            dst_ref=held.at[rows_of(member), spans[part]],
            send_sem=sems.at[0, direction, step - 1, part],
            recv_sem=sems.at[1, direction, step - 1, part],
            device_id=(ahead if direction == 0 else behind, tp),
            device_id_type=MESH,
        )

    def arrival(direction, step, part):
        member = owner(direction, step)
        if part == 2:
            return pltpu.make_async_remote_copy(
                src_ref=log_ref,
                dst_ref=logs_ref.at[member],
                send_sem=sems.at[0, direction, step - 1, part],
                recv_sem=sems.at[1, direction, step - 1, part],
                device_id=(ahead if direction == 0 else behind, tp),
                device_id_type=MESH,
            )
        return pltpu.make_async_remote_copy(
            src_ref=held.at[rows_of(member), spans[part]],
            dst_ref=held.at[rows_of(member), spans[part]],
            send_sem=sems.at[0, direction, step - 1, part],
            recv_sem=sems.at[1, direction, step - 1, part],
            device_id=(ahead if direction == 0 else behind, tp),
            device_id_type=MESH,
        )

    started = []

    def go(copy):
        copy.start()
        started.append(copy)

    def parts_of(step, direction):
        first = direction
        if step == half:
            return (2, first) if direction == 0 else (first,)
        return (2, first, 1 - first)

    for slot in range(3):
        for direction in range(2):
            parts = parts_of(1, direction)
            if slot < len(parts):
                go(send(direction, 1, parts[slot]))
    tok_here = pl.ds(pl.multiple_of(tp * count, count), count)
    for step in range(1, n_tp):
        go(
            pltpu.make_async_remote_copy(
                src_ref=normed_ref,
                dst_ref=rows_ref.at[tok_here],
                send_sem=tok_sems.at[0, step - 1],
                recv_sem=tok_sems.at[1, step - 1],
                device_id=(sp, lax.rem(tp + step, n_tp)),
                device_id_type=MESH,
            )
        )
    rows_ref[tok_here, :] = normed_ref[...]
    logs_ref[sp] = log_ref[...]
    for step in range(1, n_tp):
        origin = pl.ds(pl.multiple_of(lax.rem(tp + n_tp - step, n_tp) * count, count), count)
        pltpu.make_async_remote_copy(
            src_ref=normed_ref,
            dst_ref=rows_ref.at[origin],
            send_sem=tok_sems.at[0, step - 1],
            recv_sem=tok_sems.at[1, step - 1],
            device_id=(sp, lax.rem(tp + step, n_tp)),
            device_id_type=MESH,
        ).wait_recv()

    blockwise = depth % LANES == 0

    def add(member, weights, first=False):
        columns = pl.ds(pl.multiple_of(member * depth, depth), depth)
        product = jnp.dot(rows_ref[:, columns], weights, preferred_element_type=jnp.float32)
        total[...] = product if first else total[...] + product

    if blockwise:
        add(sp, pack_ref[...], True)
    else:
        held[rows_of(sp), :] = pack_ref[...]
    for step in range(1, half + 1):
        for slot in range(3):
            for direction in range(2):
                parts = parts_of(step, direction)
                if slot < len(parts):
                    arrival(direction, step, parts[slot]).wait_recv()
                    if step < half and parts[slot] in parts_of(step + 1, direction):
                        go(send(direction, step + 1, parts[slot]))
        if blockwise:
            for direction in range(1 if step == half else 2):
                member = owner(direction, step)
                add(member, held[rows_of(member), :])
    if not blockwise:
        total[...] = jnp.dot(rows_ref[...], held[...], preferred_element_type=jnp.float32)
    out_ref[...] = total[...].astype(out_ref.dtype)
    for copy in started:
        copy.wait_send()


def project(normed, pack, logs, n, n_tp):
    depth, width = pack.shape
    count = normed.shape[0]
    features = normed.shape[1]
    vmem = pl.BlockSpec(memory_space=pltpu.VMEM)
    return pl.pallas_call(
        functools.partial(project_kernel, n, n_tp),
        out_shape=(
            jax.ShapeDtypeStruct((n_tp * count, width), jnp.bfloat16),
            jax.ShapeDtypeStruct((n,) + logs.shape, jnp.float32),
        ),
        in_specs=[vmem, vmem, vmem],
        out_specs=(vmem, vmem),
        scratch_shapes=[
            pltpu.VMEM((n_tp * count, features), jnp.bfloat16),
            pltpu.VMEM((n * depth, width), jnp.bfloat16),
            pltpu.VMEM((n_tp * count, width), jnp.float32),
            pltpu.SemaphoreType.DMA((2, 2, n // 2, 3)),
            pltpu.SemaphoreType.DMA((2, n_tp - 1)),
        ],
        compiler_params=pltpu.CompilerParams(
            collective_id=0, has_side_effects=True, vmem_limit_bytes=40 * 2**20
        ),
        cost_estimate=pl.CostEstimate(
            flops=400 * 2**30, bytes_accessed=n * depth * width * 2, transcendentals=0
        ),
        name="project_ring",
    )(normed, pack, logs)


def exchange_kernel(n, extra, rim_ref, state_ref, *refs):
    weight_refs = refs[:extra]
    before_ref, states_ref = refs[extra : extra + 2]
    whole_refs = refs[extra + 2 : 2 * extra + 2]
    sems, rim_sems = refs[2 * extra + 2 :]
    sources = [state_ref.at[0], state_ref.at[1], *weight_refs]
    sp, tp = lax.axis_index("sp"), lax.axis_index("tp")
    half = n // 2
    spot = ring_spot(sp, n)
    ahead = ring_member(lax.rem(spot + 1, n), n)
    behind = ring_member(lax.rem(spot + n - 1, n), n)
    later, earlier = lax.rem(sp + 1, n), lax.rem(sp + n - 1, n)
    barrier = pltpu.get_barrier_semaphore()
    for peer in (ahead, behind, later, earlier):
        pl.semaphore_signal(barrier, inc=1, device_id=(peer, tp), device_id_type=MESH)
    pl.semaphore_wait(barrier, 4)

    def owner(direction, distance):
        shift = n - distance if direction == 0 else distance
        return ring_member(lax.rem(spot + shift, n), n)

    def parts_of(step, direction):
        order = []
        for first in range(0, 2 + extra, 2):
            order.append(first + direction)
            if step < half:
                order.append(first + 1 - direction)
        return order

    def target(member, part):
        return states_ref.at[member, part] if part < 2 else whole_refs[part - 2].at[member]

    def hop(direction, step, part, member, source):
        return pltpu.make_async_remote_copy(
            src_ref=source,
            dst_ref=target(member, part),
            send_sem=sems.at[0, direction, step - 1, part],
            recv_sem=sems.at[1, direction, step - 1, part],
            device_id=(ahead if direction == 0 else behind, tp),
            device_id_type=MESH,
        )

    started = []
    rim = pltpu.make_async_remote_copy(
        src_ref=rim_ref,
        dst_ref=before_ref,
        send_sem=rim_sems.at[0],
        recv_sem=rim_sems.at[1],
        device_id=(later, tp),
        device_id_type=MESH,
    )
    for slot in range(2 + extra):
        for direction in range(2):
            parts = parts_of(1, direction)
            if slot < len(parts):
                copy = hop(direction, 1, parts[slot], sp, sources[parts[slot]])
                copy.start()
                started.append(copy)
    rim.start()
    states_ref[sp] = state_ref[...]
    for whole, piece in zip(whole_refs, weight_refs):
        whole[sp] = piece[...]
    for step in range(1, half + 1):
        for slot in range(2 + extra):
            for direction in range(2):
                parts = parts_of(step, direction)
                if slot < len(parts):
                    part = parts[slot]
                    member = owner(direction, step)
                    hop(direction, step, part, member, sources[part]).wait_recv()
                    if step < half and part in parts_of(step + 1, direction):
                        copy = hop(direction, step + 1, part, member, target(member, part))
                        copy.start()
                        started.append(copy)
    rim.wait()
    for copy in started:
        copy.wait_send()


def exchange(rim, state, weights, n):
    vmem = pl.BlockSpec(memory_space=pltpu.VMEM)
    return pl.pallas_call(
        functools.partial(exchange_kernel, n, len(weights)),
        out_shape=(
            jax.ShapeDtypeStruct(rim.shape, rim.dtype),
            jax.ShapeDtypeStruct((n,) + state.shape, state.dtype),
            *[jax.ShapeDtypeStruct((n,) + weight.shape, weight.dtype) for weight in weights],
        ),
        in_specs=[vmem] * (2 + len(weights)),
        out_specs=(vmem,) * (2 + len(weights)),
        scratch_shapes=[
            pltpu.SemaphoreType.DMA((2, 2, n // 2, 2 + len(weights))),
            pltpu.SemaphoreType.DMA((2,)),
        ],
        compiler_params=pltpu.CompilerParams(
            collective_id=2, has_side_effects=True, vmem_limit_bytes=40 * 2**20
        ),
        cost_estimate=pl.CostEstimate(
            flops=20 * 2**30, bytes_accessed=n * state.size * 2, transcendentals=0
        ),
        name="state_ring",
    )(rim, state, *weights)


def merge_kernel(n_tp, ret_ref, att_ref, ret_out_ref, att_out_ref, out_ref, total, outgoing, incoming, sent, landed, sems):
    sp, tp = lax.axis_index("sp"), lax.axis_index("tp")
    outer, inner = tp // 2, lax.rem(tp, 2)
    groups = n_tp // 2
    count = out_ref.shape[0]
    barrier = pltpu.get_barrier_semaphore()
    mate = outer * 2 + 1 - inner
    pl.semaphore_signal(barrier, inc=1, device_id=(sp, mate), device_id_type=MESH)
    for step in range(1, groups):
        peer = lax.rem(outer + step, groups) * 2 + inner
        pl.semaphore_signal(barrier, inc=1, device_id=(sp, peer), device_id_type=MESH)
    pl.semaphore_wait(barrier, groups)

    blocks, _, width = ret_out_ref.shape

    def partial(side, block):
        return jnp.dot(
            ret_ref[side], ret_out_ref[block], preferred_element_type=jnp.float32
        ) + jnp.dot(att_ref[side], att_out_ref[block], preferred_element_type=jnp.float32)

    for block in range(blocks):
        outgoing[:, block * width : (block + 1) * width] = partial(1 - inner, block).astype(
            jnp.bfloat16
        )
    swap = pltpu.make_async_remote_copy(
        src_ref=outgoing,
        dst_ref=incoming,
        send_sem=sems.at[0, 0],
        recv_sem=sems.at[1, 0],
        device_id=(sp, mate),
        device_id_type=MESH,
    )
    swap.start()
    for block in range(blocks):
        total[:, block * width : (block + 1) * width] = partial(inner, block)
    swap.wait_recv()
    own = total[...] + incoming[...].astype(jnp.float32)
    sent[...] = own.astype(jnp.bfloat16)
    copies = []
    for step in range(1, groups):
        other = lax.rem(outer + step, groups)
        copy = pltpu.make_async_remote_copy(
            src_ref=sent.at[pl.ds(pl.multiple_of(other * count, count), count)],
            dst_ref=landed.at[step - 1],
            send_sem=sems.at[0, step],
            recv_sem=sems.at[1, step],
            device_id=(sp, other * 2 + inner),
            device_id_type=MESH,
        )
        copy.start()
        copies.append(copy)
    mine = sent[pl.ds(pl.multiple_of(outer * count, count), count), :].astype(jnp.float32)
    for step, copy in enumerate(copies):
        copy.wait_recv()
        mine = mine + landed[step].astype(jnp.float32)
    out_ref[...] = mine.astype(out_ref.dtype)
    swap.wait_send()
    for copy in copies:
        copy.wait_send()


def merge(mixes, weights, n_tp):
    rows = mixes[0].shape[0]
    groups = n_tp // 2
    count = rows // n_tp
    width = weights[0].shape[0] * weights[0].shape[2]
    mixes = [
        mix.reshape(groups, 2, count, -1).transpose(1, 0, 2, 3).reshape(2, groups * count, -1)
        for mix in mixes
    ]
    vmem = pl.BlockSpec(memory_space=pltpu.VMEM)
    return pl.pallas_call(
        functools.partial(merge_kernel, n_tp),
        out_shape=jax.ShapeDtypeStruct((count, width), jnp.bfloat16),
        in_specs=[vmem] * 4,
        out_specs=vmem,
        scratch_shapes=[
            pltpu.VMEM((groups * count, width), jnp.float32),
            pltpu.VMEM((groups * count, width), jnp.bfloat16),
            pltpu.VMEM((groups * count, width), jnp.bfloat16),
            pltpu.VMEM((groups * count, width), jnp.bfloat16),
            pltpu.VMEM((max(1, groups - 1), count, width), jnp.bfloat16),
            pltpu.SemaphoreType.DMA((2, groups)),
        ],
        compiler_params=pltpu.CompilerParams(
            collective_id=1, has_side_effects=True, vmem_limit_bytes=40 * 2**20
        ),
        cost_estimate=pl.CostEstimate(
            flops=4 * rows * weights[0].size // 1, bytes_accessed=4 * weights[0].size, transcendentals=0
        ),
        name="merge_scatter",
    )(*mixes, *weights)


ORDER = (
    "s0a", "S0a", "s1a", "T", "p0", "t1", "s2a", "a", "p1", "D", "P0", "t2", "x0", "f2a",
    "s3a", "x1", "p2", "t3", "p3", "u0", "v0", "f3a", "S1a", "S2a", "S3a", "c0", "k0", "m00", "c1", "k1", "m01",
    "m10", "m11", "x2", "x3", "c2", "m02", "m12", "c3", "m03", "m13", "P1", "u1", "k2", "m20", "m21",
    "m22", "m23", "k3", "m30", "m31", "m32", "m33",
)
AFTER = ("v1",)
DURING = (("r2", "y2", "r3", "y3"), (), (), ())
MIXED = ("u2", "v2", "u3", "v3")
SIDES = 2
CORES = 2
PAIR = 2
SLICES = 4
SHARES = 1
OUT = SHARES
SMALL = SHARES + 1


def layer_fits(n, n_tp, shapes):
    count, heads_here, att_here, kv_here, length = shapes
    nz, nx = n // SIDES, n_tp // CORES
    return (
        n == nz * SIDES
        and nx == 2
        and n_tp == nx * CORES
        and nz == 2 * PAIR
        and nz == heads_here * CORES
        and kv_here == 1
        and att_here * HEAD_DIM == heads_here * V_DIM
        and count % 16 == 0
        and n_tp * count == length
        and length == 2 * WINDOW
        and length == 2 * BLOCK
        and nx * WINDOW == length
    )


def layer_scratch(n, n_tp, count, features, depth, width):
    nz = n // SIDES
    length = n_tp * count
    rows = nz * length
    slab = SIDES * width
    att_width = V_DIM + 2 * HEAD_DIM
    ret_width = 2 * RETAIN_KEY_SIZE + V_DIM
    parts = nz // CORES
    bf, f32 = jnp.bfloat16, jnp.float32
    dma = pltpu.SemaphoreType.DMA
    return dict(
        tok=pltpu.VMEM((rows, features), bf),
        ret_pack=pltpu.VMEM((parts, depth, ret_width), bf),
        att_pack=pltpu.VMEM((parts, depth, att_width), bf),
        ret_w=pltpu.VMEM((n * depth, ret_width), bf),
        att_w=pltpu.VMEM((n * depth, att_width), bf),
        out_pack=pltpu.VMEM((2, parts * V_DIM, width), bf),
        out_w=pltpu.VMEM((V_DIM, n * width), bf),
        tokens=pltpu.VMEM((count, features), bf),
        gain=pltpu.VMEM((1, features), f32),
        logs=pltpu.VMEM((parts, length), f32),
        sinks=pltpu.VMEM((1, parts * V_DIM // HEAD_DIM), f32),
        aux_here=pltpu.VMEM((8, length), f32),
        kv_pack=pltpu.VMEM((2 * HEAD_DIM, depth), bf),
        bias=pltpu.VMEM((2, WINDOW, 2 * WINDOW), f32),
        aux=pltpu.VMEM((n, 8, length), f32),
        total=pltpu.VMEM((rows, ret_width), f32),
        cosine=pltpu.VMEM((rows, RETAIN_KEY_SIZE), f32),
        sine=pltpu.VMEM((rows, RETAIN_KEY_SIZE), f32),
        fade_q=pltpu.VMEM((rows, RETAIN_KEY_SIZE), f32),
        fade_k=pltpu.VMEM((rows, RETAIN_KEY_SIZE), f32),
        decay=pltpu.VMEM((rows, length), f32),
        queries=pltpu.VMEM((rows, V_DIM), bf),
        keys=pltpu.VMEM((rows, RETAIN_KEY_SIZE), bf),
        values=pltpu.VMEM((rows, V_DIM), bf),
        inner=pltpu.VMEM((rows, V_DIM), f32),
        states=pltpu.VMEM((nz, SIDES, RETAIN_KEY_SIZE, V_DIM), bf),
        before=pltpu.VMEM((nz, SIDES, RETAIN_KEY_SIZE, V_DIM), f32),
        kv=pltpu.VMEM((4, nz, length + WINDOW, 2 * HEAD_DIM), bf),
        rim=pltpu.VMEM((nz, WINDOW, 2 * HEAD_DIM), bf),
        halo=pltpu.VMEM((nz, WINDOW, 2 * HEAD_DIM), bf),
        mix_far=pltpu.VMEM((nz, WINDOW, V_DIM), bf),
        mix_near=pltpu.VMEM((nz, WINDOW, V_DIM), bf),
        mix_in=pltpu.VMEM((nz, WINDOW, V_DIM), bf),
        out_wx=pltpu.VMEM((V_DIM, n * width), bf),
        part=pltpu.VMEM((nz * WINDOW, slab), f32),
        result=pltpu.VMEM((count, n * width), bf),
        keep=pltpu.VMEM((nz, nz, count, slab), f32),
        core_out=pltpu.VMEM((nz, nz, count, slab), bf),
        core_in=pltpu.VMEM((nz, nz, count, slab), bf),
        z_out=pltpu.VMEM((nz, nz, count, slab), bf),
        z_in=pltpu.VMEM((nz, nz, count, slab), bf),
        tz_s=dma((2, nz)),
        tz_r=dma((nz, SLICES)),
        tx_s=dma((nz,)),
        tx_r=dma((nz, SLICES)),
        tc_s=dma((nz, 2)),
        tc_r=dma((nz, 2)),
        w_s=dma((SHARES + 2, nz, CORES)),
        w_r=dma((SHARES + 2, nz)),
        f_s=dma((SHARES + 2, nz)),
        f_r=dma((SHARES + 2, nz)),
        s_s=dma((nz,)),
        s_r=dma((nz,)),
        h_s=dma((1,)),
        h_r=dma((1,)),
        ox_s=dma((1,)),
        ox_r=dma((nz, SIDES)),
        rc_s=dma((1,)),
        rc_r=dma((nz,)),
        rx_s=dma((1,)),
        rx_r=dma((nz,)),
        rz_s=dma((nz, nz - 1)),
        rz_r=dma((nz, nz)),
        load=dma((8,)),
        store=dma((1,)),
    )


class Named:
    def __init__(self, names, refs):
        for name, ref in zip(names, refs):
            setattr(self, name, ref)


def dot_nt(a, b, **kw):
    return lax.dot_general(a, b, (((1,), (1,)), ((), ())), preferred_element_type=jnp.float32, **kw)


def dot_tn(a, b):
    return lax.dot_general(a, b, (((0,), (0,)), ((), ())), preferred_element_type=jnp.float32)


def dot_nn(a, b):
    return jnp.dot(a, b, preferred_element_type=jnp.float32)


def layer_kernel(n, n_tp, names, *refs):
    (tokens_ref, gain_ref, logs_ref, sinks_ref, rq_ref, rk_ref, rv_ref, aq_ref, ak_ref, av_ref, ro_ref, ao_ref) = refs[:12]
    out_ref = refs[12]
    m = Named(names, refs[13:])
    nz = n // SIDES
    parts = nz // CORES
    count, features = tokens_ref.shape
    depth = rq_ref.shape[0]
    width = out_ref.shape[1] // n
    length = n_tp * count
    slab = SIDES * width
    key_size = RETAIN_KEY_SIZE
    bf, f32 = jnp.bfloat16, jnp.float32

    sp, tp = lax.axis_index("sp"), lax.axis_index("tp")
    z, y = sp // SIDES, lax.rem(sp, SIDES)
    x, c = tp // CORES, lax.rem(tp, CORES)
    ny, nx, nc = 1 - y, 1 - x, 1 - c
    is_ret, is_att = c == 0, c == 1
    source_core = z // parts
    mate = z + 1 - 2 * lax.rem(z, PAIR)
    part_here = lax.rem(z, parts)

    def device(zz, yy, xx, cc):
        return (zz * SIDES + yy, xx * CORES + cc)

    def remote(src, dst, send_sem, recv_sem, target):
        return pltpu.make_async_remote_copy(
            src_ref=src,
            dst_ref=dst,
            send_sem=send_sem,
            recv_sem=recv_sem,
            device_id=target,
            device_id_type=MESH,
        )

    started = []

    def go(copy, condition=None):
        started.append((copy, condition))
        if condition is None:
            copy.start()
        else:
            pl.when(condition)(copy.start)

    def both(*conditions):
        conditions = [cond for cond in conditions if cond is not None]
        if not conditions:
            return None
        result = conditions[0]
        for cond in conditions[1:]:
            result = result & cond
        return result

    def await_recv(copy, condition=None):
        if condition is None:
            copy.wait_recv()
        else:
            pl.when(condition)(copy.wait_recv)

    moves = [
        (tokens_ref, m.tokens, 0),
        (gain_ref, m.gain, 1),
        (logs_ref, m.logs, 2),
        (sinks_ref, m.sinks, 3),
        (ak_ref, m.kv_pack.at[0:HEAD_DIM], 4),
        (av_ref, m.kv_pack.at[HEAD_DIM:], 4),
    ]
    for part in range(parts):
        wide = slice(part * V_DIM, (part + 1) * V_DIM)
        thin = slice(part * key_size, (part + 1) * key_size)
        moves += [
            (rq_ref.at[:, thin], m.ret_pack.at[part, :, 0:key_size], 5),
            (rk_ref.at[:, thin], m.ret_pack.at[part, :, key_size : 2 * key_size], 5),
            (rv_ref.at[:, wide], m.ret_pack.at[part, :, 2 * key_size :], 5),
            (aq_ref.at[:, wide], m.att_pack.at[part, :, 0:V_DIM], 6),
        ]
    moves += [(ro_ref, m.out_pack.at[0], 7), (ao_ref, m.out_pack.at[1], 7)]
    for src, dst, index in moves:
        pltpu.make_async_copy(src, dst, m.load.at[index]).start()

    def loaded(piece, index):
        pltpu.make_async_copy(piece, piece, m.load.at[index]).wait()

    barrier = pltpu.get_barrier_semaphore()
    peers = [device(z, ny, x, c), device(z, y, nx, c), device(z, y, x, nc)]
    for step in range(1, nz):
        for cc in range(CORES):
            peers.append(device(lax.rem(z + step, nz), y, x, cc))
    for peer in peers:
        pl.semaphore_signal(barrier, inc=1, device_id=peer, device_id_type=MESH)

    def token_rows(zz, xx, cc):
        return pl.ds(pl.multiple_of(zz * length + xx * (CORES * count) + cc * count, count), count)

    loaded(m.tokens, 0)
    loaded(m.gain, 1)
    tok_float = m.tokens[...].astype(f32)
    scale = lax.rsqrt(jnp.mean(tok_float * tok_float, axis=-1, keepdims=True) + epsilon)
    m.tok[token_rows(z, x, c), :] = (tok_float * scale * m.gain[...]).astype(bf)
    loaded(m.logs, 2)
    loaded(m.sinks, 3)
    loaded(m.kv_pack, 4)
    loaded(m.ret_pack, 5)
    loaded(m.att_pack.at[:, :, 0:V_DIM], 6)
    loaded(m.out_pack, 7)
    many = m.sinks.shape[1]
    m.aux_here[...] = jnp.zeros_like(m.aux_here)
    m.aux_here[0:parts, :] = m.logs[...]
    m.aux_here[parts : parts + 1, 0:many] = m.sinks[...]
    pair = jnp.transpose(m.kv_pack[...].astype(f32)).astype(bf)
    for part in range(parts):
        m.att_pack[part, :, V_DIM:] = pair
    pl.semaphore_wait(barrier, len(peers))

    def token_at(zz, xx, cc, cut):
        if cut is None:
            return m.tok.at[token_rows(zz, xx, cc)]
        wide = features // SLICES
        return m.tok.at[token_rows(zz, xx, cc), cut * wide : (cut + 1) * wide]

    def token_z(origin, way, cut=None):
        piece = token_at(origin, x, c, cut)
        return remote(
            piece,
            piece,
            m.tz_s.at[way, origin],
            m.tz_r.at[origin, 0 if cut is None else cut],
            device(z + 1 - 2 * way, y, x, c),
        )

    def token_x(origin, side, cut=None):
        piece = token_at(origin, side, c, cut)
        return remote(
            piece, piece, m.tx_s.at[origin], m.tx_r.at[origin, 0 if cut is None else cut], device(z, y, nx, c)
        )

    def token_core(origin, side, core, cut=None):
        piece = token_at(origin, side, core, cut)
        return remote(piece, piece, m.tc_s.at[origin, side], m.tc_r.at[origin, side], device(z, y, x, nc))

    def send_rows(maker, cut, condition, *place):
        copy = maker(*place, cut)
        if condition is None:
            copy.start()
        else:
            pl.when(condition)(copy.start)
        if cut == 0:
            started.append((maker(*place), condition))

    can_go = (z < nz - 1, z > 0)

    def spread(origin, cut, condition, ways):
        for way in ways:
            send_rows(token_z, cut, both(condition, can_go[way]), origin, way)
        send_rows(token_x, cut, condition, origin, x)
        send_rows(token_core, cut, condition, origin, x, c)

    def weight_rows(zz, yy, share):
        start = (zz * SIDES + yy) * depth + share * (depth // SHARES)
        return pl.ds(pl.multiple_of(start, depth // SHARES), depth // SHARES)

    near, distant = c == z // parts, c != z // parts
    outer = (z == 0) | (z == nz - 1)
    inside = jnp.logical_not(outer)

    def toward(step):
        return (z, mate, lax.rem(z + PAIR, nz), nz - 1 - z)[step]

    def send_weights(step, kind, where=None):
        target_z = toward(step)
        part = lax.rem(target_z, parts)
        valid = both(near if step < PAIR else distant, where)
        first = len(started)
        for core in range(CORES):
            target = device(target_z, y, x, core)
            pack = m.ret_pack if core == 0 else m.att_pack
            if kind < SHARES:
                high = depth // SHARES
                src = pack.at[part, kind * high : (kind + 1) * high]
            elif kind == OUT:
                src = m.out_pack.at[core, pl.ds(pl.multiple_of(part * V_DIM, V_DIM), V_DIM)]
            else:
                src = m.aux_here
            dst = weight_piece(kind, z, y, core)
            away = valid if step else valid & (c != core)
            go(remote(src, dst, m.w_s.at[kind, step, core], m.w_r.at[kind, z], target), away)
            if step == 0:

                @pl.when(valid & (c == core))
                def _():
                    dst[...] = src[...]

        return started[first:]

    def finish(copies):
        for entry in copies:
            started[:] = [kept for kept in started if kept is not entry]
            pl.when(entry[1])(entry[0].wait_send)

    def out_columns(zz, yy):
        return pl.ds(pl.multiple_of((zz * SIDES + yy) * width, width), width)

    def weight_piece(kind, zz, yy, core):
        if kind < SHARES:
            return (m.ret_w if core == 0 else m.att_w).at[weight_rows(zz, yy, kind)]
        if kind == OUT:
            return m.out_w.at[:, out_columns(zz, yy)]
        return m.aux.at[zz * SIDES + yy]

    def per_core(kind):
        return ((0, is_ret), (1, is_att)) if kind < SHARES else ((0, None),)

    def pass_weights(kind, step):
        zz = toward(step)
        other = jnp.logical_not((zz == z) & (c == source_core))
        for core, condition in per_core(kind):
            piece = weight_piece(kind, zz, y, core)
            await_recv(
                remote(piece, piece, m.f_s.at[kind, zz], m.w_r.at[kind, zz], device(z, ny, x, c)),
                both(condition, other),
            )
            go(
                remote(piece, piece, m.f_s.at[kind, zz], m.f_r.at[kind, zz], device(z, ny, x, c)),
                condition,
            )

    def take_weights(kind, zz):
        for core, condition in per_core(kind):
            piece = weight_piece(kind, zz, ny, core)
            await_recv(
                remote(piece, piece, m.f_s.at[kind, zz], m.f_r.at[kind, zz], device(z, ny, x, c)), condition
            )

    for step in range(nz):
        send_weights(step, SMALL)
    for cut in range(SLICES):
        spread(z, cut, None, (0, 1))

    def pass_tokens(step):
        for cut in range(SLICES):
            for way in range(2):
                origin = z - step if way == 0 else z + step
                valid = origin >= 0 if way == 0 else origin < nz
                await_recv(token_z(origin, way, cut), valid)
                spread(origin, cut, valid, (way,))

    def across_tokens(step):
        origin = toward(step)
        for cut in range(SLICES):
            await_recv(token_x(origin, nx, cut))
            send_rows(token_core, cut, None, origin, nx, c)

    def tables():
        @pl.when(is_ret)
        def make_tables():
            lane = lax.broadcasted_iota(jnp.int32, (length, key_size), 1)
            row = lax.broadcasted_iota(jnp.int32, (length, key_size), 0)
            half = key_size // 2
            inverse = jnp.exp(
                lax.rem(lane, half).astype(f32) * (-math.log(rope_base) / half)
            )
            sign = jnp.where(lane < half, -1.0, 1.0)

            def table(zz, carry):
                where = pl.ds(pl.multiple_of(zz * length, length), length)
                angles = (row + (zz * SIDES + y) * length).astype(f32) * inverse
                m.cosine[where, :] = jnp.cos(angles)
                m.sine[where, :] = jnp.sin(angles) * sign
                return carry

            lax.fori_loop(0, nz, table, 0)

    def decays():
        for zz in range(nz):
            take_weights(SMALL, zz)

        @pl.when(is_ret)
        def _():
            lower = (
                lax.broadcasted_iota(jnp.int32, (length, length), 0)
                >= lax.broadcasted_iota(jnp.int32, (length, length), 1)
            )
            lower_float = lower.astype(f32)
            mine = [m.aux[zz * SIDES + y, pl.ds(part_here, 1), :] for zz in range(nz)]
            logs = jnp.concatenate(mine * (8 // nz), axis=0)
            by_row = dot_nt(logs, lower_float, precision=lax.Precision.HIGHEST)
            by_column = dot_nt(lower_float, logs, precision=lax.Precision.HIGHEST)
            for zz in range(nz):
                rows = slice(zz * length, (zz + 1) * length)
                column = by_column[:, zz : zz + 1]
                closing = by_column[length - 1 : length, zz : zz + 1]
                within = jnp.minimum(column - by_row[zz : zz + 1, :], 0.0)
                m.decay[rows, :] = jnp.where(lower, jnp.exp(within), 0.0)
                m.fade_q[rows, :] = jnp.broadcast_to(jnp.exp(column), (length, key_size))
                m.fade_k[rows, :] = jnp.broadcast_to(jnp.exp(closing - column), (length, key_size))

    def run_rows(zz):
        return pl.ds(pl.multiple_of(zz * length, length), length)

    def take_tokens(step):
        origin = toward(step)
        for side in (x, nx):
            await_recv(token_core(origin, side, nc))

    def out_x(step, side):
        columns = out_columns(toward(step), side)
        return remote(
            m.out_w.at[:, columns],
            m.out_wx.at[:, columns],
            m.ox_s.at[0],
            m.ox_r.at[step, side],
            device(z, y, nx, c),
        )

    def out_y(step, arrival):
        piece = m.out_w.at[:, out_columns(toward(step), y)]
        return remote(piece, piece, m.f_s.at[OUT, toward(step)], arrival, device(z, ny, x, c))

    fresh = set()

    def project(step, run):
        columns = pl.ds(pl.multiple_of(toward(step) * SIDES * depth, SIDES * depth), SIDES * depth)
        rows = run_rows(toward(run))
        first = run not in fresh
        fresh.add(run)

        def accumulate(held):
            lanes = slice(0, held.shape[1])
            product = dot_nn(m.tok[rows, columns], held[columns, :])
            m.total[rows, lanes] = product if first else m.total[rows, lanes] + product

        pl.when(is_ret)(lambda: accumulate(m.ret_w))
        pl.when(is_att)(lambda: accumulate(m.att_w))

    everyone = dict(a=None, o=outer, i=inside)
    sent = {}
    def perform(word):
        step = int(word[1]) if len(word) > 1 else 0
        if word[0] == "s":
            for kind in range(SHARES):
                sent[word, kind] = send_weights(step, kind, everyone[word[2]])
        elif word[0] == "f":
            for kind in range(SHARES):
                finish(sent["s" + word[1:], kind])
        elif word[0] == "p":
            for kind in range(SHARES):
                pass_weights(kind, step)
        elif word[0] == "S":
            sent[word] = send_weights(step, OUT, everyone[word[2]])
        elif word[0] == "P":
            pass_weights(OUT, step)
        elif word[0] == "t":
            pass_tokens(step)
        elif word[0] == "x":
            across_tokens(step)
        elif word[0] == "r":
            out_y(step, m.w_r.at[OUT, toward(step)]).wait_recv()
        elif word[0] == "y":
            out_y(step, m.f_r.at[OUT, toward(step)]).start()
        elif word[0] == "u":
            out_x(step, y).start()
        elif word[0] == "v":
            take_weights(OUT, toward(step))
            out_x(step, ny).start()
        elif word[0] == "c":
            take_tokens(step)
        elif word[0] == "k":
            for kind in range(SHARES):
                take_weights(kind, toward(step))
        elif word[0] == "m":
            project(step, int(word[2]))
        elif word[0] == "T":
            tables()
        elif word[0] == "D":
            decays()
        elif word[0] == "a":
            for aux_step in range(nz):
                pass_weights(SMALL, aux_step)

    for word in ORDER:
        perform(word)

    def state_copy(zz):
        piece = m.states.at[zz, y]
        return remote(piece, piece, m.s_s.at[zz], m.s_r.at[zz], device(z, ny, x, c))

    def state_arrival(zz):
        piece = m.states.at[zz, ny]
        return remote(piece, piece, m.s_s.at[zz], m.s_r.at[zz], device(z, ny, x, c))

    halo_copy = remote(m.rim, m.halo, m.h_s.at[0], m.h_r.at[0], device(z, ny, x, c))

    @pl.when(is_ret)
    def _():
        def project_run(zz, carry):
            rows = run_rows(zz)
            product = m.total[rows, :].astype(bf)
            cosine, sine = m.cosine[rows, :], m.sine[rows, :]

            def turn(values):
                values = values.astype(f32)
                return values * cosine + pltpu.roll(values, key_size // 2, 1) * sine

            m.queries[rows, 0:key_size] = turn(product[:, 0:key_size]).astype(bf)
            key = (turn(product[:, key_size : 2 * key_size]) * key_size ** (-0.5)).astype(bf)
            m.keys[rows, :] = key
            value = product[:, 2 * key_size :]
            m.values[rows, :] = value
            faded = (key.astype(f32) * m.fade_k[rows, :]).astype(bf)
            m.states[zz, y] = dot_tn(faded, value).astype(bf)
            state_copy(zz).start()
            return carry

        lax.fori_loop(0, nz, project_run, 0)

    lane_kv = lax.broadcasted_iota(jnp.int32, (WINDOW, 2 * HEAD_DIM), 1)

    def place(zz, spot, packed):
        where = pl.ds(spot * WINDOW, WINDOW)
        packed = packed.astype(f32)
        low = jnp.where(lane_kv < HEAD_DIM, packed, 0.0)
        turned = pltpu.roll(packed, HEAD_DIM, 1)
        m.kv[0, zz, where, :] = low.astype(bf)
        m.kv[1, zz, where, :] = pltpu.roll(low, HEAD_DIM, 1).astype(bf)
        m.kv[2, zz, where, :] = jnp.where(lane_kv < HEAD_DIM, turned, 1.0).astype(bf)
        m.kv[3, zz, where, :] = jnp.where(lane_kv < HEAD_DIM, 1.0, packed).astype(bf)

    @pl.when(is_att)
    def _():
        def project_run(zz, carry):
            rows = run_rows(zz)
            product = m.total[rows, 0 : m.att_w.shape[1]].astype(bf)
            m.queries[rows, :] = (product[:, 0:V_DIM].astype(f32) * HEAD_DIM ** (-0.5)).astype(bf)
            for spot in range(2):
                place(zz, spot + 1, product[spot * WINDOW : (spot + 1) * WINDOW, V_DIM:])
            m.rim[zz] = product[length - WINDOW :, V_DIM:]
            return carry

        lax.fori_loop(0, nz, project_run, 0)
        halo_copy.start()

    far = jnp.where(z < PAIR, nz - 1, 0)

    def home(turn):
        near = far + jnp.where(z < PAIR, -1, 1)
        if isinstance(turn, int):
            return (far, near, mate, z)[turn]
        return jnp.where(turn == 0, far, jnp.where(turn == 1, near, jnp.where(turn == 2, mate, z)))

    def core_copy(piece):
        return remote(
            m.core_out.at[piece], m.core_in.at[piece], m.rc_s.at[0], m.rc_r.at[piece], device(z, y, x, nc)
        )

    def mix_copy(turn):
        return remote(
            m.mix_far.at[turn], m.mix_in.at[turn], m.rx_s.at[0], m.rx_r.at[turn], device(z, y, nx, c)
        )

    def z_copy(turn, piece, target_z, slot):
        spot = toward(piece)
        return remote(
            m.z_out.at[turn, spot],
            m.z_in.at[slot, spot],
            m.rz_s.at[spot, turn],
            m.rz_r.at[slot, spot],
            device(target_z, y, x, c),
        )

    def half_rows(turn, cc):
        return pl.ds(pl.multiple_of(turn * WINDOW + cc * count, count), count)

    def slab_columns(piece):
        return pl.ds(pl.multiple_of(toward(piece) * slab, slab), slab)

    def block_rows(zz, xx):
        return pl.ds(pl.multiple_of(zz * length + xx * WINDOW, WINDOW), WINDOW)

    def take_out(piece):
        for side in (y, ny):
            out_x(piece, side).wait_recv()

    def emit(piece):
        columns = slab_columns(piece)
        rows = nz * WINDOW
        m.part[...] = dot_nn(m.mix_near[...].reshape(rows, V_DIM), m.out_w[:, columns]) + dot_nn(
            m.mix_in[...].reshape(rows, V_DIM), m.out_wx[:, columns]
        )
        for turn in range(nz):
            m.core_out[piece, turn] = m.part[half_rows(turn, nc), :].astype(bf)
        core_copy(piece).start()
        for turn in range(nz):
            m.keep[piece, turn] = m.part[half_rows(turn, c), :]

    def joined(turn, piece):
        return m.keep[piece, turn] + m.core_in[piece, turn].astype(f32)

    def pass_sum(turn, piece):
        m.z_out[turn, toward(piece)] = joined(turn, piece).astype(bf)
        z_copy(turn, piece, mate, turn).start()

    def merge_sum(turn, piece):
        z_copy(turn, piece, mate, turn).wait_recv()
        merged = joined(turn, piece) + m.z_in[turn, toward(piece)].astype(f32)
        m.z_out[turn, toward(piece)] = merged.astype(bf)
        z_copy(turn, piece, home(turn), nz - 1).start()

    def rounds(block):
        for turn in range(nz):
            block(turn)
            for word in DURING[turn]:
                perform(word)

    for word in AFTER:
        perform(word)

    @pl.when(is_ret)
    def _():
        def inner_run(zz, carry):
            rows = run_rows(zz)
            scores = dot_nt(m.queries[rows, 0:key_size], m.keys[rows, :]) * m.decay[rows, :]
            m.inner[rows, :] = dot_nn(scores.astype(bf), m.values[rows, :])
            return carry

        lax.fori_loop(0, nz, inner_run, 0)
        totals = [
            jnp.sum(m.aux[spot, pl.ds(part_here, 1), :], axis=1, keepdims=True) for spot in range(n)
        ]
        for zz in range(nz):
            state_arrival(zz).wait_recv()
        running = jnp.zeros((key_size, V_DIM), f32)
        for zz in range(nz):
            for yy in range(SIDES):
                m.before[zz, yy] = running
                running = running * jnp.exp(totals[zz * SIDES + yy]) + m.states[zz, yy].astype(f32)

        def finish_block(zz, xx):
            rows = block_rows(zz, xx)
            query = (m.queries[rows, 0:key_size].astype(f32) * m.fade_q[rows, :]).astype(bf)
            state = m.before[zz, y]
            high = state.astype(bf)
            low = (state - high.astype(f32)).astype(bf)
            total = m.inner[rows, :] + (dot_nn(query, high) + dot_nn(query, low))
            total = total * lax.rsqrt(jnp.mean(total * total, axis=-1, keepdims=True) + epsilon)
            return total.astype(bf)

        def both_blocks(turn):
            m.mix_far[turn] = finish_block(home(turn), nx)
            mix_copy(turn).start()
            m.mix_near[turn] = finish_block(home(turn), x)

        rounds(both_blocks)
        for zz in range(nz):
            state_copy(zz).wait_send()

    @pl.when(is_att)
    def _():
        row = lax.broadcasted_iota(jnp.int32, (WINDOW, 2 * WINDOW), 0)
        column = lax.broadcasted_iota(jnp.int32, (WINDOW, 2 * WINDOW), 1)
        band = (column > row) & (column <= row + WINDOW)
        m.bias[0] = jnp.where(band & (column >= WINDOW), 0.0, masked_out)
        m.bias[1] = jnp.where(band, 0.0, masked_out)
        sink_row = m.aux[sp, parts : parts + 1, 0:LANES]
        sink_lane = lax.broadcasted_iota(jnp.int32, (1, LANES), 1)
        heads = V_DIM // HEAD_DIM
        sinks = [
            jnp.sum(
                jnp.where(sink_lane == part_here * heads + head, sink_row, 0.0), axis=1, keepdims=True
            )
            for head in range(heads)
        ]
        def take_halo():
            halo_copy.wait_recv()
            for zz in range(nz):
                place(zz, 0, m.halo[jnp.maximum(zz - 1 + y, 0)])

        pl.when(x == 1)(take_halo)
        def attend_block(zz, xx, target):
            bias = m.bias[jnp.minimum(zz + y + xx, 1)]
            where = pl.ds(pl.multiple_of(xx * WINDOW, WINDOW), 2 * WINDOW)
            rows = block_rows(zz, xx)
            first = lane_kv < HEAD_DIM
            for pair in range(heads // 2):
                lanes = slice(pair * LANES, (pair + 1) * LANES)
                query = m.queries[rows, lanes]
                terms, ends = [], []
                for side in range(2):
                    sink = sinks[pair * 2 + side]
                    scores = dot_nt(query, m.kv[side, zz, where, :]) + bias
                    highest = jnp.maximum(jnp.max(scores, axis=-1, keepdims=True), sink)
                    lifted = jnp.exp(scores - highest).astype(bf)
                    ends.append(jnp.exp(sink - highest))
                    terms.append(dot_nn(lifted, m.kv[2 + side, zz, where, :]))
                below = pltpu.roll(jnp.where(first, terms[1], terms[0]), HEAD_DIM, 1)
                below = below + jnp.where(first, ends[0], ends[1])
                mixed = jnp.where(first, terms[0], terms[1]) / below
                target[:, lanes] = mixed.astype(bf)

        def both_blocks(turn):
            attend_block(home(turn), nx, m.mix_far.at[turn])
            mix_copy(turn).start()
            if turn == 0:
                pl.when(x == 0)(take_halo)
            attend_block(home(turn), x, m.mix_near.at[turn])

        rounds(both_blocks)
        halo_copy.wait_send()

    def merge_sums(piece):
        for turn in range(PAIR):
            merge_sum(turn, piece)

    def crossing(piece, before=None):
        def paced():
            if before is not None:
                sent(before)
            for turn in range(PAIR):
                pass_sum(turn, piece)

        core_copy(piece).wait_recv()
        pl.when(outer)(paced)

    def sent(piece):
        for turn in range(PAIR):
            z_copy(turn, piece, mate, turn).wait_send()

    def staying(piece):
        pass_sum(nz - 2, piece)

    def second_round(piece):
        pl.when(inside)(functools.partial(merge_sums, piece))

    def make(piece):
        take_out(piece)
        emit(piece)

    for turn in range(nz):
        mix_copy(turn).wait_recv()
    for word in MIXED:
        perform(word)
    make(0)
    make(1)
    crossing(0)
    for piece in range(1, nz):
        crossing(piece, piece - 1)
        pl.when(inside)(functools.partial(staying, piece - 1))
        second_round(piece - 1)
        if piece + 1 < nz:
            make(piece + 1)

    def last_sums():
        sent(nz - 1)
        for piece in range(nz):
            staying(piece)

    pl.when(outer)(last_sums)
    pl.when(inside)(functools.partial(staying, nz - 1))
    second_round(nz - 1)
    for piece in range(nz):
        total = joined(nz - 1, piece)
        for slot in (nz - 2, nz - 1):
            z_copy(0, piece, mate, slot).wait_recv()
            total = total + m.z_in[slot, toward(piece)].astype(f32)
        columns = slab_columns(piece)
        m.result[:, columns] = total.astype(bf)
        pltpu.make_async_copy(m.result.at[:, columns], out_ref.at[:, columns], m.store.at[0]).start()

    for step in range(PAIR, nz):
        out_y(step, m.f_r.at[OUT, toward(step)]).wait_send()
    for copy, condition in started:
        if condition is None:
            copy.wait_send()
        else:
            pl.when(condition)(copy.wait_send)
    everything = device(z, y, x, nc)
    remote(m.core_out, m.core_in, m.rc_s.at[0], m.rc_r.at[0], everything).wait_send()
    remote(m.mix_far, m.mix_in, m.rx_s.at[0], m.rx_r.at[0], everything).wait_send()
    remote(m.out_w, m.out_wx, m.ox_s.at[0], m.ox_r.at[0, 0], everything).wait_send()
    for piece in range(nz):
        pl.when(inside)(functools.partial(sent, piece))
        z_copy(nz - 2, piece, mate, nz - 2).wait_send()
    pltpu.make_async_copy(m.result, out_ref, m.store.at[0]).wait()


def layer(n, n_tp, tokens, norm_gain, logs, sinks, *weights):
    count, features = tokens.shape
    depth = weights[0].shape[0]
    width = weights[-1].shape[1]
    scratch = layer_scratch(n, n_tp, count, features, depth, width)
    return pl.pallas_call(
        functools.partial(layer_kernel, n, n_tp, tuple(scratch)),
        out_shape=jax.ShapeDtypeStruct((count, n * width), jnp.bfloat16),
        in_specs=[pl.BlockSpec(memory_space=pltpu.HBM)] * (4 + len(weights)),
        out_specs=pl.BlockSpec(memory_space=pltpu.HBM),
        scratch_shapes=list(scratch.values()),
        compiler_params=pltpu.CompilerParams(
            collective_id=3, has_side_effects=True, vmem_limit_bytes=60 * 2**20
        ),
        cost_estimate=pl.CostEstimate(flops=4 * 2**30, bytes_accessed=16 * 2**20, transcendentals=0),
        name="layer",
    )(tokens, norm_gain.reshape(1, -1), logs, sinks.reshape(1, -1), *weights)


def on_device(
    tokens,
    norm_gain,
    ret_query,
    ret_key,
    ret_value,
    log_decay,
    att_query,
    att_key,
    att_value,
    sink_logits,
    ret_out,
    att_out,
):
    n, n_tp = lax.axis_size("sp"), lax.axis_size("tp")
    length = log_decay.shape[1]
    shapes = (
        tokens.shape[0],
        log_decay.shape[0],
        sink_logits.shape[0],
        att_key.shape[1] // HEAD_DIM,
        length,
    )
    if layer_fits(n, n_tp, shapes):
        return layer(
            n, n_tp, tokens, norm_gain, log_decay, sink_logits,
            ret_query, ret_key, ret_value, att_query, att_key.T, att_value.T, ret_out, att_out,
        )
    tok_float = tokens.astype(jnp.float32)
    normed = (
        tok_float
        * lax.rsqrt(jnp.mean(tok_float * tok_float, axis=-1, keepdims=True) + epsilon)
        * norm_gain
    ).astype(jnp.bfloat16)
    weights = (ret_query, ret_key, ret_value, att_query, att_key, att_value)
    widths = [weight.shape[1] for weight in weights]
    points = [sum(widths[:index]) for index in range(1, len(widths))]
    aligned = ret_out.shape[1] % LANES == 0
    local_logs = jnp.sum(log_decay, axis=1)
    log_tile = jnp.broadcast_to(
        jnp.pad(local_logs, (0, -local_logs.shape[0] % 8))[:, None], (-(-local_logs.shape[0] // 8) * 8, LANES)
    )
    projected, logs = project(normed, jnp.concatenate(weights, axis=1), log_tile, n, n_tp)
    logs = logs[:, : local_logs.shape[0], 0]
    sections = jnp.split(projected, points, axis=1)
    tok_count = sections[0].shape[0]
    anchor = lax.axis_index("sp") * tok_count
    positions = anchor + jnp.arange(tok_count, dtype=jnp.int32)
    query_ret = rotate(sections[0].reshape(tok_count, -1, RETAIN_KEY_SIZE), positions).astype(
        jnp.bfloat16
    )
    key_ret = (
        rotate(sections[1].reshape(tok_count, -1, RETAIN_KEY_SIZE), positions)
        * RETAIN_KEY_SIZE ** (-0.5)
    ).astype(jnp.bfloat16)
    value_ret = sections[2].reshape(tok_count, -1, V_DIM)
    stacked = projected[:, points[3] :]
    ret_mix, rim, wholes = retention_path(
        query_ret,
        key_ret,
        value_ret,
        log_decay,
        stacked[tok_count - WINDOW :],
        logs,
        (ret_out, att_out) if aligned else (),
    )
    if not aligned:
        wholes = [
            lax.all_gather(weight, "sp", axis=1, tiled=True)[None] for weight in (ret_out, att_out)
        ]
    att_mix = attention_path(sections[3], stacked, rim, sink_logits, anchor)
    return merge((ret_mix, att_mix), wholes, n_tp)


def solution(mesh):
    in_specs = (
        P(("sp", "tp"), None),
        P(),
        P("sp", "tp"),
        P("sp", "tp"),
        P("sp", "tp"),
        P("tp", "sp"),
        P("sp", "tp"),
        P("sp", "tp"),
        P("sp", "tp"),
        P("tp"),
        P("tp", "sp"),
        P("tp", "sp"),
    )
    out_specs = P(("sp", "tp"), None)
    return jax.shard_map(
        on_device, mesh=mesh, in_specs=in_specs, out_specs=out_specs, check_vma=False
    )
```

```python
import functools
import math

import jax
import jax.numpy as jnp
from jax import lax
from jax.experimental import pallas as pl
from jax.experimental.pallas import tpu as pltpu
from jax.sharding import PartitionSpec as P

MESH = pl.DeviceIdType.MESH
LANES = 128

RETAIN_KEY_SIZE = 128
V_DIM = 256
HEAD_DIM = 64
WINDOW = 128
BLOCK = 128


epsilon = 1e-05
rope_base = 10000.0
masked_out = -1e30


def rotate(values, positions):
    half_dim = values.shape[-1] // 2
    inverse = rope_base ** (-jnp.arange(half_dim, dtype=jnp.float32) / half_dim)
    angles = positions.astype(jnp.float32)[:, None] * inverse[None, :]
    cosine = jnp.cos(angles)[:, None, :]
    sine_part = jnp.sin(angles)[:, None, :]
    first_half = values[..., :half_dim].astype(jnp.float32)
    second_half = values[..., half_dim:].astype(jnp.float32)
    return jnp.concatenate(
        [
            first_half * cosine - second_half * sine_part,
            second_half * cosine + first_half * sine_part,
        ],
        axis=-1,
    )


def retention_path(query_ret, key_ret, value_ret, log_decay, rim, logs, weights):
    tok_count, heads_here = (query_ret.shape[0], query_ret.shape[1])
    blocks = tok_count // BLOCK
    q_blocks = query_ret.reshape(blocks, BLOCK, heads_here, RETAIN_KEY_SIZE)
    k_blocks = key_ret.reshape(blocks, BLOCK, heads_here, RETAIN_KEY_SIZE)
    v_blocks = value_ret.reshape(blocks, BLOCK, heads_here, V_DIM)
    running = jnp.cumsum(log_decay.reshape(heads_here, blocks, BLOCK), axis=-1)
    closing = running[:, :, -1:]
    within = running[:, :, :, None] - running[:, :, None, :]
    causal_mask = jnp.arange(BLOCK)[:, None] >= jnp.arange(BLOCK)[None, :]
    weighting = jnp.where(causal_mask, jnp.exp(jnp.minimum(within, 0.0)), 0.0)
    scores = (
        jnp.einsum("nihd,njhd->hnij", q_blocks, k_blocks, preferred_element_type=jnp.float32)
        * weighting
    )
    in_block = jnp.einsum(
        "hnij,njhv->nihv", scores.astype(jnp.bfloat16), v_blocks, preferred_element_type=jnp.float32
    )
    key_fade = (
        k_blocks.astype(jnp.float32) * jnp.exp(closing - running).transpose(1, 2, 0)[..., None]
    ).astype(jnp.bfloat16)
    contrib = jnp.einsum("njhd,njhv->nhdv", key_fade, v_blocks, preferred_element_type=jnp.float32)
    block_fade = jnp.exp(closing[:, :, 0]).T

    def advance(carried, entry_pair):
        addend, factor = entry_pair
        return (carried * factor[:, None, None] + addend, carried)

    final_state, before = lax.scan(
        advance, jnp.zeros((heads_here, RETAIN_KEY_SIZE, V_DIM), jnp.float32), (contrib, block_fade)
    )
    n = lax.axis_size("sp")
    place = lax.axis_index("sp")
    before_rim, states, *wholes = exchange(
        rim, final_state.astype(jnp.bfloat16).reshape(2, -1, V_DIM), weights, n
    )
    states = states.reshape(n, heads_here, RETAIN_KEY_SIZE, V_DIM)
    spots = jnp.arange(n)
    between = (spots[None, :] > spots[:, None]) & (spots[None, :] < place)
    spans = jnp.sum(jnp.where(between[:, :, None], logs[None], 0.0), axis=1)
    shares = jnp.where((spots < place)[:, None], jnp.exp(spans), 0.0)
    arrived = jnp.sum(shares[:, :, None, None] * states.astype(jnp.float32), axis=0)
    leading = jnp.cumsum(closing[:, :, 0], axis=1) - closing[:, :, 0]
    before = before + arrived[None] * jnp.exp(leading).T[:, :, None, None]
    query_fade = (
        q_blocks.astype(jnp.float32) * jnp.exp(running).transpose(1, 2, 0)[..., None]
    ).astype(jnp.bfloat16)
    carried_term = jnp.einsum(
        "nihd,nhdv->nihv", query_fade.astype(jnp.float32), before, precision=lax.Precision.HIGHEST
    )
    final_product = in_block + carried_term
    final_product = final_product * lax.rsqrt(
        jnp.mean(final_product * final_product, axis=-1, keepdims=True) + epsilon
    )
    return final_product.reshape(tok_count, heads_here * V_DIM).astype(jnp.bfloat16), before_rim, wholes


def attention_path(query_att, stacked, window_rim, sink_logits, anchor):
    tok_count = query_att.shape[0]
    kv_here = stacked.shape[1] // (2 * HEAD_DIM)
    group_size = query_att.shape[1] // (kv_here * HEAD_DIM)
    blocks = tok_count // WINDOW
    extended = jnp.concatenate([window_rim, stacked], axis=0).reshape(
        blocks + 1, WINDOW, 2, kv_here, HEAD_DIM
    )
    paired = jnp.concatenate([extended[:-1], extended[1:]], axis=1)
    keys_pair = paired[:, :, 0]
    values_pair = paired[:, :, 1]
    q_blocks = query_att.reshape(blocks, WINDOW, kv_here, group_size, HEAD_DIM)
    scores = jnp.einsum(
        "nihgd,njhd->nhgij", q_blocks, keys_pair, preferred_element_type=jnp.float32
    ) * HEAD_DIM ** (-0.5)
    query_pos = anchor + (jnp.arange(blocks) * WINDOW)[:, None] + jnp.arange(WINDOW)[None, :]
    key_pos = (
        anchor + (jnp.arange(blocks) * WINDOW - WINDOW)[:, None] + jnp.arange(2 * WINDOW)[None, :]
    )
    allowed = (
        (key_pos[:, None, :] >= 0)
        & (key_pos[:, None, :] <= query_pos[:, :, None])
        & (query_pos[:, :, None] - key_pos[:, None, :] < WINDOW)
    )
    scores = jnp.where(allowed[:, None, None], scores, masked_out)
    sink_logit = sink_logits.reshape(kv_here, group_size)[None, :, :, None]
    highest = jnp.maximum(jnp.max(scores, axis=-1), sink_logit)
    lifted = jnp.exp(scores - highest[..., None])
    denominator = jnp.sum(lifted, axis=-1) + jnp.exp(sink_logit - highest)
    attn_weights = (lifted / denominator[..., None]).astype(jnp.bfloat16)
    final_product = jnp.einsum(
        "nhgij,njhd->nihgd", attn_weights, values_pair, preferred_element_type=jnp.float32
    )
    return final_product.reshape(tok_count, kv_here * group_size * HEAD_DIM).astype(jnp.bfloat16)


def ring_spot(index, count):
    half = count // 2
    return jnp.where(lax.rem(index, 2) == 0, index // 2, count - 1 - index // 2)


def ring_member(spot, count):
    half = count // 2
    return jnp.where(spot < half, 2 * spot, 2 * (count - 1 - spot) + 1)


def project_kernel(n, n_tp, normed_ref, pack_ref, log_ref, out_ref, logs_ref, rows_ref, held, total, sems, tok_sems):
    sp, tp = lax.axis_index("sp"), lax.axis_index("tp")
    depth, width = pack_ref.shape
    count = normed_ref.shape[0]
    half = n // 2
    spot = ring_spot(sp, n)
    ahead = ring_member(lax.rem(spot + 1, n), n)
    behind = ring_member(lax.rem(spot + n - 1, n), n)

    barrier = pltpu.get_barrier_semaphore()
    for peer in (ahead, behind):
        pl.semaphore_signal(barrier, inc=1, device_id=(peer, tp), device_id_type=MESH)
    for step in range(1, n_tp):
        pl.semaphore_signal(
            barrier, inc=1, device_id=(sp, lax.rem(tp + step, n_tp)), device_id_type=MESH
        )
    pl.semaphore_wait(barrier, 2 + n_tp - 1)

    def rows_of(member):
        return pl.ds(pl.multiple_of(member * depth, depth), depth)

    middle = (width // LANES + 1) // 2 * LANES
    spans = (pl.ds(0, middle), pl.ds(middle, width - middle))

    def owner(direction, distance):
        shift = n - distance if direction == 0 else distance
        return ring_member(lax.rem(spot + shift, n), n)

    def send(direction, step, part):
        member = owner(direction, step - 1)
        if part == 2:
            return pltpu.make_async_remote_copy(
                src_ref=log_ref if step == 1 else logs_ref.at[member],
                dst_ref=logs_ref.at[member],
                send_sem=sems.at[0, direction, step - 1, part],
                recv_sem=sems.at[1, direction, step - 1, part],
                device_id=(ahead if direction == 0 else behind, tp),
                device_id_type=MESH,
            )
        source = pack_ref.at[:, spans[part]] if step == 1 else held.at[rows_of(member), spans[part]]
        return pltpu.make_async_remote_copy(
            src_ref=source,
            dst_ref=held.at[rows_of(member), spans[part]],
            send_sem=sems.at[0, direction, step - 1, part],
            recv_sem=sems.at[1, direction, step - 1, part],
            device_id=(ahead if direction == 0 else behind, tp),
            device_id_type=MESH,
        )

    def arrival(direction, step, part):
        member = owner(direction, step)
        if part == 2:
            return pltpu.make_async_remote_copy(
                src_ref=log_ref,
                dst_ref=logs_ref.at[member],
                send_sem=sems.at[0, direction, step - 1, part],
                recv_sem=sems.at[1, direction, step - 1, part],
                device_id=(ahead if direction == 0 else behind, tp),
                device_id_type=MESH,
            )
        return pltpu.make_async_remote_copy(
            src_ref=held.at[rows_of(member), spans[part]],
            dst_ref=held.at[rows_of(member), spans[part]],
            send_sem=sems.at[0, direction, step - 1, part],
            recv_sem=sems.at[1, direction, step - 1, part],
            device_id=(ahead if direction == 0 else behind, tp),
            device_id_type=MESH,
        )

    started = []

    def go(copy):
        copy.start()
        started.append(copy)

    def parts_of(step, direction):
        first = direction
        if step == half:
            return (2, first) if direction == 0 else (first,)
        return (2, first, 1 - first)

    for slot in range(3):
        for direction in range(2):
            parts = parts_of(1, direction)
            if slot < len(parts):
                go(send(direction, 1, parts[slot]))
    tok_here = pl.ds(pl.multiple_of(tp * count, count), count)
    for step in range(1, n_tp):
        go(
            pltpu.make_async_remote_copy(
                src_ref=normed_ref,
                dst_ref=rows_ref.at[tok_here],
                send_sem=tok_sems.at[0, step - 1],
                recv_sem=tok_sems.at[1, step - 1],
                device_id=(sp, lax.rem(tp + step, n_tp)),
                device_id_type=MESH,
            )
        )
    rows_ref[tok_here, :] = normed_ref[...]
    logs_ref[sp] = log_ref[...]
    for step in range(1, n_tp):
        origin = pl.ds(pl.multiple_of(lax.rem(tp + n_tp - step, n_tp) * count, count), count)
        pltpu.make_async_remote_copy(
            src_ref=normed_ref,
            dst_ref=rows_ref.at[origin],
            send_sem=tok_sems.at[0, step - 1],
            recv_sem=tok_sems.at[1, step - 1],
            device_id=(sp, lax.rem(tp + step, n_tp)),
            device_id_type=MESH,
        ).wait_recv()

    blockwise = depth % LANES == 0

    def add(member, weights, first=False):
        columns = pl.ds(pl.multiple_of(member * depth, depth), depth)
        product = jnp.dot(rows_ref[:, columns], weights, preferred_element_type=jnp.float32)
        total[...] = product if first else total[...] + product

    if blockwise:
        add(sp, pack_ref[...], True)
    else:
        held[rows_of(sp), :] = pack_ref[...]
    for step in range(1, half + 1):
        for slot in range(3):
            for direction in range(2):
                parts = parts_of(step, direction)
                if slot < len(parts):
                    arrival(direction, step, parts[slot]).wait_recv()
                    if step < half and parts[slot] in parts_of(step + 1, direction):
                        go(send(direction, step + 1, parts[slot]))
        if blockwise:
            for direction in range(1 if step == half else 2):
                member = owner(direction, step)
                add(member, held[rows_of(member), :])
    if not blockwise:
        total[...] = jnp.dot(rows_ref[...], held[...], preferred_element_type=jnp.float32)
    out_ref[...] = total[...].astype(out_ref.dtype)
    for copy in started:
        copy.wait_send()


def project(normed, pack, logs, n, n_tp):
    depth, width = pack.shape
    count = normed.shape[0]
    features = normed.shape[1]
    vmem = pl.BlockSpec(memory_space=pltpu.VMEM)
    return pl.pallas_call(
        functools.partial(project_kernel, n, n_tp),
        out_shape=(
            jax.ShapeDtypeStruct((n_tp * count, width), jnp.bfloat16),
            jax.ShapeDtypeStruct((n,) + logs.shape, jnp.float32),
        ),
        in_specs=[vmem, vmem, vmem],
        out_specs=(vmem, vmem),
        scratch_shapes=[
            pltpu.VMEM((n_tp * count, features), jnp.bfloat16),
            pltpu.VMEM((n * depth, width), jnp.bfloat16),
            pltpu.VMEM((n_tp * count, width), jnp.float32),
            pltpu.SemaphoreType.DMA((2, 2, n // 2, 3)),
            pltpu.SemaphoreType.DMA((2, n_tp - 1)),
        ],
        compiler_params=pltpu.CompilerParams(
            collective_id=0, has_side_effects=True, vmem_limit_bytes=40 * 2**20
        ),
        cost_estimate=pl.CostEstimate(
            flops=400 * 2**30, bytes_accessed=n * depth * width * 2, transcendentals=0
        ),
        name="project_ring",
    )(normed, pack, logs)


def exchange_kernel(n, extra, rim_ref, state_ref, *refs):
    weight_refs = refs[:extra]
    before_ref, states_ref = refs[extra : extra + 2]
    whole_refs = refs[extra + 2 : 2 * extra + 2]
    sems, rim_sems = refs[2 * extra + 2 :]
    sources = [state_ref.at[0], state_ref.at[1], *weight_refs]
    sp, tp = lax.axis_index("sp"), lax.axis_index("tp")
    half = n // 2
    spot = ring_spot(sp, n)
    ahead = ring_member(lax.rem(spot + 1, n), n)
    behind = ring_member(lax.rem(spot + n - 1, n), n)
    later, earlier = lax.rem(sp + 1, n), lax.rem(sp + n - 1, n)
    barrier = pltpu.get_barrier_semaphore()
    for peer in (ahead, behind, later, earlier):
        pl.semaphore_signal(barrier, inc=1, device_id=(peer, tp), device_id_type=MESH)
    pl.semaphore_wait(barrier, 4)

    def owner(direction, distance):
        shift = n - distance if direction == 0 else distance
        return ring_member(lax.rem(spot + shift, n), n)

    def parts_of(step, direction):
        order = []
        for first in range(0, 2 + extra, 2):
            order.append(first + direction)
            if step < half:
                order.append(first + 1 - direction)
        return order

    def target(member, part):
        return states_ref.at[member, part] if part < 2 else whole_refs[part - 2].at[member]

    def hop(direction, step, part, member, source):
        return pltpu.make_async_remote_copy(
            src_ref=source,
            dst_ref=target(member, part),
            send_sem=sems.at[0, direction, step - 1, part],
            recv_sem=sems.at[1, direction, step - 1, part],
            device_id=(ahead if direction == 0 else behind, tp),
            device_id_type=MESH,
        )

    started = []
    rim = pltpu.make_async_remote_copy(
        src_ref=rim_ref,
        dst_ref=before_ref,
        send_sem=rim_sems.at[0],
        recv_sem=rim_sems.at[1],
        device_id=(later, tp),
        device_id_type=MESH,
    )
    for slot in range(2 + extra):
        for direction in range(2):
            parts = parts_of(1, direction)
            if slot < len(parts):
                copy = hop(direction, 1, parts[slot], sp, sources[parts[slot]])
                copy.start()
                started.append(copy)
    rim.start()
    states_ref[sp] = state_ref[...]
    for whole, piece in zip(whole_refs, weight_refs):
        whole[sp] = piece[...]
    for step in range(1, half + 1):
        for slot in range(2 + extra):
            for direction in range(2):
                parts = parts_of(step, direction)
                if slot < len(parts):
                    part = parts[slot]
                    member = owner(direction, step)
                    hop(direction, step, part, member, sources[part]).wait_recv()
                    if step < half and part in parts_of(step + 1, direction):
                        copy = hop(direction, step + 1, part, member, target(member, part))
                        copy.start()
                        started.append(copy)
    rim.wait()
    for copy in started:
        copy.wait_send()


def exchange(rim, state, weights, n):
    vmem = pl.BlockSpec(memory_space=pltpu.VMEM)
    return pl.pallas_call(
        functools.partial(exchange_kernel, n, len(weights)),
        out_shape=(
            jax.ShapeDtypeStruct(rim.shape, rim.dtype),
            jax.ShapeDtypeStruct((n,) + state.shape, state.dtype),
            *[jax.ShapeDtypeStruct((n,) + weight.shape, weight.dtype) for weight in weights],
        ),
        in_specs=[vmem] * (2 + len(weights)),
        out_specs=(vmem,) * (2 + len(weights)),
        scratch_shapes=[
            pltpu.SemaphoreType.DMA((2, 2, n // 2, 2 + len(weights))),
            pltpu.SemaphoreType.DMA((2,)),
        ],
        compiler_params=pltpu.CompilerParams(
            collective_id=2, has_side_effects=True, vmem_limit_bytes=40 * 2**20
        ),
        cost_estimate=pl.CostEstimate(
            flops=20 * 2**30, bytes_accessed=n * state.size * 2, transcendentals=0
        ),
        name="state_ring",
    )(rim, state, *weights)


def merge_kernel(n_tp, ret_ref, att_ref, ret_out_ref, att_out_ref, out_ref, total, outgoing, incoming, sent, landed, sems):
    sp, tp = lax.axis_index("sp"), lax.axis_index("tp")
    outer, inner = tp // 2, lax.rem(tp, 2)
    groups = n_tp // 2
    count = out_ref.shape[0]
    barrier = pltpu.get_barrier_semaphore()
    mate = outer * 2 + 1 - inner
    pl.semaphore_signal(barrier, inc=1, device_id=(sp, mate), device_id_type=MESH)
    for step in range(1, groups):
        peer = lax.rem(outer + step, groups) * 2 + inner
        pl.semaphore_signal(barrier, inc=1, device_id=(sp, peer), device_id_type=MESH)
    pl.semaphore_wait(barrier, groups)

    blocks, _, width = ret_out_ref.shape

    def partial(side, block):
        return jnp.dot(
            ret_ref[side], ret_out_ref[block], preferred_element_type=jnp.float32
        ) + jnp.dot(att_ref[side], att_out_ref[block], preferred_element_type=jnp.float32)

    for block in range(blocks):
        outgoing[:, block * width : (block + 1) * width] = partial(1 - inner, block).astype(
            jnp.bfloat16
        )
    swap = pltpu.make_async_remote_copy(
        src_ref=outgoing,
        dst_ref=incoming,
        send_sem=sems.at[0, 0],
        recv_sem=sems.at[1, 0],
        device_id=(sp, mate),
        device_id_type=MESH,
    )
    swap.start()
    for block in range(blocks):
        total[:, block * width : (block + 1) * width] = partial(inner, block)
    swap.wait_recv()
    own = total[...] + incoming[...].astype(jnp.float32)
    sent[...] = own.astype(jnp.bfloat16)
    copies = []
    for step in range(1, groups):
        other = lax.rem(outer + step, groups)
        copy = pltpu.make_async_remote_copy(
            src_ref=sent.at[pl.ds(pl.multiple_of(other * count, count), count)],
            dst_ref=landed.at[step - 1],
            send_sem=sems.at[0, step],
            recv_sem=sems.at[1, step],
            device_id=(sp, other * 2 + inner),
            device_id_type=MESH,
        )
        copy.start()
        copies.append(copy)
    mine = sent[pl.ds(pl.multiple_of(outer * count, count), count), :].astype(jnp.float32)
    for step, copy in enumerate(copies):
        copy.wait_recv()
        mine = mine + landed[step].astype(jnp.float32)
    out_ref[...] = mine.astype(out_ref.dtype)
    swap.wait_send()
    for copy in copies:
        copy.wait_send()


def merge(mixes, weights, n_tp):
    rows = mixes[0].shape[0]
    groups = n_tp // 2
    count = rows // n_tp
    width = weights[0].shape[0] * weights[0].shape[2]
    mixes = [
        mix.reshape(groups, 2, count, -1).transpose(1, 0, 2, 3).reshape(2, groups * count, -1)
        for mix in mixes
    ]
    vmem = pl.BlockSpec(memory_space=pltpu.VMEM)
    return pl.pallas_call(
        functools.partial(merge_kernel, n_tp),
        out_shape=jax.ShapeDtypeStruct((count, width), jnp.bfloat16),
        in_specs=[vmem] * 4,
        out_specs=vmem,
        scratch_shapes=[
            pltpu.VMEM((groups * count, width), jnp.float32),
            pltpu.VMEM((groups * count, width), jnp.bfloat16),
            pltpu.VMEM((groups * count, width), jnp.bfloat16),
            pltpu.VMEM((groups * count, width), jnp.bfloat16),
            pltpu.VMEM((max(1, groups - 1), count, width), jnp.bfloat16),
            pltpu.SemaphoreType.DMA((2, groups)),
        ],
        compiler_params=pltpu.CompilerParams(
            collective_id=1, has_side_effects=True, vmem_limit_bytes=40 * 2**20
        ),
        cost_estimate=pl.CostEstimate(
            flops=4 * rows * weights[0].size // 1, bytes_accessed=4 * weights[0].size, transcendentals=0
        ),
        name="merge_scatter",
    )(*mixes, *weights)


ORDER = (
    "s0a", "S0a", "s1a", "T", "p0", "t1", "s2a", "a", "p1", "D", "P0", "t2", "x0", "f2a",
    "s3a", "x1", "p2", "t3", "p3", "u0", "v0", "f3a", "S1a", "S2a", "S3a", "c0", "k0", "m00", "c1", "k1", "m01",
    "m10", "m11", "x2", "x3", "c2", "m02", "m12", "c3", "m03", "m13", "P1", "u1", "k2", "m20", "m21",
    "m22", "m23", "k3", "m30", "m31", "m32", "m33",
)
AFTER = ("v1",)
DURING = ("r2", "y2", "r3", "y3")
MIXED = ("u2", "v2", "u3", "v3")
SIDES = 2
CORES = 2
PAIR = 2
SLICES = 4
SHARES = 1
OUT = SHARES
SMALL = SHARES + 1


def layer_fits(n, n_tp, shapes):
    count, heads_here, att_here, kv_here, length = shapes
    nz, nx = n // SIDES, n_tp // CORES
    return (
        n == nz * SIDES
        and nx == 2
        and n_tp == nx * CORES
        and nz == 2 * PAIR
        and nz == heads_here * CORES
        and kv_here == 1
        and att_here * HEAD_DIM == heads_here * V_DIM
        and count % 16 == 0
        and n_tp * count == length
        and length == 2 * WINDOW
        and length == 2 * BLOCK
        and nx * WINDOW == length
    )


def layer_scratch(n, n_tp, count, features, depth, width):
    nz = n // SIDES
    length = n_tp * count
    rows = nz * length
    slab = SIDES * width
    att_width = V_DIM + 2 * HEAD_DIM
    ret_width = 2 * RETAIN_KEY_SIZE + V_DIM
    parts = nz // CORES
    bf, f32 = jnp.bfloat16, jnp.float32
    dma = pltpu.SemaphoreType.DMA
    return dict(
        tok=pltpu.VMEM((rows, features), bf),
        ret_pack=pltpu.VMEM((parts, depth, ret_width), bf),
        att_pack=pltpu.VMEM((parts, depth, att_width), bf),
        ret_w=pltpu.VMEM((n * depth, ret_width), bf),
        att_w=pltpu.VMEM((n * depth, att_width), bf),
        out_pack=pltpu.VMEM((2, parts * V_DIM, width), bf),
        out_w=pltpu.VMEM((V_DIM, n * width), bf),
        tokens=pltpu.VMEM((count, features), bf),
        gain=pltpu.VMEM((1, features), f32),
        logs=pltpu.VMEM((parts, length), f32),
        sinks=pltpu.VMEM((1, parts * V_DIM // HEAD_DIM), f32),
        aux_here=pltpu.VMEM((8, length), f32),
        kv_pack=pltpu.VMEM((2 * HEAD_DIM, depth), bf),
        bias=pltpu.VMEM((2, WINDOW, 2 * WINDOW), f32),
        aux=pltpu.VMEM((n, 8, length), f32),
        total=pltpu.VMEM((rows, ret_width), f32),
        cosine=pltpu.VMEM((rows, RETAIN_KEY_SIZE), f32),
        sine=pltpu.VMEM((rows, RETAIN_KEY_SIZE), f32),
        fade_q=pltpu.VMEM((rows, RETAIN_KEY_SIZE), f32),
        fade_k=pltpu.VMEM((rows, RETAIN_KEY_SIZE), f32),
        decay=pltpu.VMEM((rows, length), f32),
        queries=pltpu.VMEM((rows, V_DIM), bf),
        keys=pltpu.VMEM((rows, RETAIN_KEY_SIZE), bf),
        values=pltpu.VMEM((rows, V_DIM), bf),
        inner=pltpu.VMEM((rows, V_DIM), f32),
        states=pltpu.VMEM((nz, SIDES, RETAIN_KEY_SIZE, V_DIM), bf),
        before=pltpu.VMEM((nz, SIDES, RETAIN_KEY_SIZE, V_DIM), f32),
        kv=pltpu.VMEM((4, nz, length + WINDOW, 2 * HEAD_DIM), bf),
        rim=pltpu.VMEM((nz, WINDOW, 2 * HEAD_DIM), bf),
        halo=pltpu.VMEM((nz, WINDOW, 2 * HEAD_DIM), bf),
        mixes=pltpu.VMEM((2, nz, WINDOW, V_DIM), bf),
        mix_in=pltpu.VMEM((nz, WINDOW, V_DIM), bf),
        out_wx=pltpu.VMEM((V_DIM, n * width), bf),
        part=pltpu.VMEM((nz * WINDOW, slab), f32),
        result=pltpu.VMEM((count, n * width), bf),
        keep=pltpu.VMEM((nz, nz, count, slab), f32),
        core_out=pltpu.VMEM((nz, nz, count, slab), bf),
        core_in=pltpu.VMEM((nz, nz, count, slab), bf),
        z_out=pltpu.VMEM((nz, nz, count, slab), bf),
        z_in=pltpu.VMEM((nz, nz, count, slab), bf),
        tz_s=dma((2, nz)),
        tz_r=dma((nz, SLICES)),
        tx_s=dma((nz,)),
        tx_r=dma((nz, SLICES)),
        tc_s=dma((nz, 2)),
        tc_r=dma((nz, 2)),
        w_s=dma((SHARES + 2, nz, CORES)),
        w_r=dma((SHARES + 2, nz)),
        f_s=dma((SHARES + 2, nz)),
        f_r=dma((SHARES + 2, nz)),
        s_s=dma((nz,)),
        s_r=dma((nz,)),
        h_s=dma((1,)),
        h_r=dma((1,)),
        ox_s=dma((1,)),
        ox_r=dma((nz, SIDES)),
        rc_s=dma((1,)),
        rc_r=dma((nz,)),
        rx_s=dma((1,)),
        rx_r=dma((nz,)),
        rz_s=dma((nz, nz - 1)),
        rz_r=dma((nz, nz)),
        load=dma((8,)),
        store=dma((1,)),
    )


class Named:
    def __init__(self, names, refs):
        for name, ref in zip(names, refs):
            setattr(self, name, ref)


def dot_nt(a, b, **kw):
    return lax.dot_general(a, b, (((1,), (1,)), ((), ())), preferred_element_type=jnp.float32, **kw)


def dot_tn(a, b):
    return lax.dot_general(a, b, (((0,), (0,)), ((), ())), preferred_element_type=jnp.float32)


def dot_nn(a, b):
    return jnp.dot(a, b, preferred_element_type=jnp.float32)


def layer_kernel(n, n_tp, names, *refs):
    (tokens_ref, gain_ref, logs_ref, sinks_ref, rq_ref, rk_ref, rv_ref, aq_ref, ak_ref, av_ref, ro_ref, ao_ref) = refs[:12]
    out_ref = refs[12]
    m = Named(names, refs[13:])
    nz = n // SIDES
    parts = nz // CORES
    count, features = tokens_ref.shape
    depth = rq_ref.shape[0]
    width = out_ref.shape[1] // n
    length = n_tp * count
    slab = SIDES * width
    key_size = RETAIN_KEY_SIZE
    bf, f32 = jnp.bfloat16, jnp.float32

    sp, tp = lax.axis_index("sp"), lax.axis_index("tp")
    z, y = sp // SIDES, lax.rem(sp, SIDES)
    x, c = tp // CORES, lax.rem(tp, CORES)
    ny, nx, nc = 1 - y, 1 - x, 1 - c
    is_ret, is_att = c == 0, c == 1
    source_core = z // parts
    mate = z + 1 - 2 * lax.rem(z, PAIR)
    part_here = lax.rem(z, parts)

    def device(zz, yy, xx, cc):
        return (zz * SIDES + yy, xx * CORES + cc)

    def remote(src, dst, send_sem, recv_sem, target):
        return pltpu.make_async_remote_copy(
            src_ref=src,
            dst_ref=dst,
            send_sem=send_sem,
            recv_sem=recv_sem,
            device_id=target,
            device_id_type=MESH,
        )

    started = []

    def go(copy, condition=None):
        started.append((copy, condition))
        if condition is None:
            copy.start()
        else:
            pl.when(condition)(copy.start)

    def both(*conditions):
        conditions = [cond for cond in conditions if cond is not None]
        if not conditions:
            return None
        result = conditions[0]
        for cond in conditions[1:]:
            result = result & cond
        return result

    def await_recv(copy, condition=None):
        if condition is None:
            copy.wait_recv()
        else:
            pl.when(condition)(copy.wait_recv)

    moves = [
        (tokens_ref, m.tokens, 0),
        (gain_ref, m.gain, 1),
        (logs_ref, m.logs, 2),
        (sinks_ref, m.sinks, 3),
        (ak_ref, m.kv_pack.at[0:HEAD_DIM], 4),
        (av_ref, m.kv_pack.at[HEAD_DIM:], 4),
    ]
    for part in range(parts):
        wide = slice(part * V_DIM, (part + 1) * V_DIM)
        thin = slice(part * key_size, (part + 1) * key_size)
        moves += [
            (rq_ref.at[:, thin], m.ret_pack.at[part, :, 0:key_size], 5),
            (rk_ref.at[:, thin], m.ret_pack.at[part, :, key_size : 2 * key_size], 5),
            (rv_ref.at[:, wide], m.ret_pack.at[part, :, 2 * key_size :], 5),
            (aq_ref.at[:, wide], m.att_pack.at[part, :, 0:V_DIM], 6),
        ]
    moves += [(ro_ref, m.out_pack.at[0], 7), (ao_ref, m.out_pack.at[1], 7)]
    for src, dst, index in moves:
        pltpu.make_async_copy(src, dst, m.load.at[index]).start()

    def loaded(piece, index):
        pltpu.make_async_copy(piece, piece, m.load.at[index]).wait()

    barrier = pltpu.get_barrier_semaphore()
    peers = [device(z, ny, x, c), device(z, y, nx, c), device(z, y, x, nc)]
    for step in range(1, nz):
        for cc in range(CORES):
            peers.append(device(lax.rem(z + step, nz), y, x, cc))
    for peer in peers:
        pl.semaphore_signal(barrier, inc=1, device_id=peer, device_id_type=MESH)

    def token_rows(zz, xx, cc):
        return pl.ds(pl.multiple_of(zz * length + xx * (CORES * count) + cc * count, count), count)

    loaded(m.tokens, 0)
    loaded(m.gain, 1)
    tok_float = m.tokens[...].astype(f32)
    scale = lax.rsqrt(jnp.mean(tok_float * tok_float, axis=-1, keepdims=True) + epsilon)
    m.tok[token_rows(z, x, c), :] = (tok_float * scale * m.gain[...]).astype(bf)
    loaded(m.logs, 2)
    loaded(m.sinks, 3)
    loaded(m.kv_pack, 4)
    loaded(m.ret_pack, 5)
    loaded(m.att_pack.at[:, :, 0:V_DIM], 6)
    loaded(m.out_pack, 7)
    many = m.sinks.shape[1]
    m.aux_here[...] = jnp.zeros_like(m.aux_here)
    m.aux_here[0:parts, :] = m.logs[...]
    m.aux_here[parts : parts + 1, 0:many] = m.sinks[...]
    pair = jnp.transpose(m.kv_pack[...].astype(f32)).astype(bf)
    for part in range(parts):
        m.att_pack[part, :, V_DIM:] = pair
    pl.semaphore_wait(barrier, len(peers))

    def token_at(zz, xx, cc, cut):
        if cut is None:
            return m.tok.at[token_rows(zz, xx, cc)]
        wide = features // SLICES
        return m.tok.at[token_rows(zz, xx, cc), cut * wide : (cut + 1) * wide]

    def token_z(origin, way, cut=None):
        piece = token_at(origin, x, c, cut)
        return remote(
            piece,
            piece,
            m.tz_s.at[way, origin],
            m.tz_r.at[origin, 0 if cut is None else cut],
            device(z + 1 - 2 * way, y, x, c),
        )

    def token_x(origin, side, cut=None):
        piece = token_at(origin, side, c, cut)
        return remote(
            piece, piece, m.tx_s.at[origin], m.tx_r.at[origin, 0 if cut is None else cut], device(z, y, nx, c)
        )

    def token_core(origin, side, core, cut=None):
        piece = token_at(origin, side, core, cut)
        return remote(piece, piece, m.tc_s.at[origin, side], m.tc_r.at[origin, side], device(z, y, x, nc))

    def send_rows(maker, cut, condition, *place):
        copy = maker(*place, cut)
        if condition is None:
            copy.start()
        else:
            pl.when(condition)(copy.start)
        if cut == 0:
            started.append((maker(*place), condition))

    can_go = (z < nz - 1, z > 0)

    def spread(origin, cut, condition, ways):
        for way in ways:
            send_rows(token_z, cut, both(condition, can_go[way]), origin, way)
        send_rows(token_x, cut, condition, origin, x)
        send_rows(token_core, cut, condition, origin, x, c)

    def weight_rows(zz, yy, share):
        start = (zz * SIDES + yy) * depth + share * (depth // SHARES)
        return pl.ds(pl.multiple_of(start, depth // SHARES), depth // SHARES)

    near, distant = c == z // parts, c != z // parts
    outer = (z == 0) | (z == nz - 1)
    inside = jnp.logical_not(outer)

    def toward(step):
        return (z, mate, lax.rem(z + PAIR, nz), nz - 1 - z)[step]

    def send_weights(step, kind, where=None):
        target_z = toward(step)
        part = lax.rem(target_z, parts)
        valid = both(near if step < PAIR else distant, where)
        first = len(started)
        for core in range(CORES):
            target = device(target_z, y, x, core)
            pack = m.ret_pack if core == 0 else m.att_pack
            if kind < SHARES:
                high = depth // SHARES
                src = pack.at[part, kind * high : (kind + 1) * high]
            elif kind == OUT:
                src = m.out_pack.at[core, pl.ds(pl.multiple_of(part * V_DIM, V_DIM), V_DIM)]
            else:
                src = m.aux_here
            dst = weight_piece(kind, z, y, core)
            away = valid if step else valid & (c != core)
            go(remote(src, dst, m.w_s.at[kind, step, core], m.w_r.at[kind, z], target), away)
            if step == 0:

                @pl.when(valid & (c == core))
                def _():
                    dst[...] = src[...]

        return started[first:]

    def finish(copies):
        for entry in copies:
            started[:] = [kept for kept in started if kept is not entry]
            pl.when(entry[1])(entry[0].wait_send)

    def out_columns(zz, yy):
        return pl.ds(pl.multiple_of((zz * SIDES + yy) * width, width), width)

    def weight_piece(kind, zz, yy, core):
        if kind < SHARES:
            return (m.ret_w if core == 0 else m.att_w).at[weight_rows(zz, yy, kind)]
        if kind == OUT:
            return m.out_w.at[:, out_columns(zz, yy)]
        return m.aux.at[zz * SIDES + yy]

    def per_core(kind):
        return ((0, is_ret), (1, is_att)) if kind < SHARES else ((0, None),)

    def pass_weights(kind, step):
        zz = toward(step)
        other = jnp.logical_not((zz == z) & (c == source_core))
        for core, condition in per_core(kind):
            piece = weight_piece(kind, zz, y, core)
            await_recv(
                remote(piece, piece, m.f_s.at[kind, zz], m.w_r.at[kind, zz], device(z, ny, x, c)),
                both(condition, other),
            )
            go(
                remote(piece, piece, m.f_s.at[kind, zz], m.f_r.at[kind, zz], device(z, ny, x, c)),
                condition,
            )

    def take_weights(kind, zz):
        for core, condition in per_core(kind):
            piece = weight_piece(kind, zz, ny, core)
            await_recv(
                remote(piece, piece, m.f_s.at[kind, zz], m.f_r.at[kind, zz], device(z, ny, x, c)), condition
            )

    for step in range(nz):
        send_weights(step, SMALL)
    for cut in range(SLICES):
        spread(z, cut, None, (0, 1))

    def pass_tokens(step):
        for cut in range(SLICES):
            for way in range(2):
                origin = z - step if way == 0 else z + step
                valid = origin >= 0 if way == 0 else origin < nz
                await_recv(token_z(origin, way, cut), valid)
                spread(origin, cut, valid, (way,))

    def across_tokens(step):
        origin = toward(step)
        for cut in range(SLICES):
            await_recv(token_x(origin, nx, cut))
            send_rows(token_core, cut, None, origin, nx, c)

    def tables():
        @pl.when(is_ret)
        def make_tables():
            lane = lax.broadcasted_iota(jnp.int32, (length, key_size), 1)
            row = lax.broadcasted_iota(jnp.int32, (length, key_size), 0)
            half = key_size // 2
            inverse = jnp.exp(
                lax.rem(lane, half).astype(f32) * (-math.log(rope_base) / half)
            )
            sign = jnp.where(lane < half, -1.0, 1.0)

            def table(zz, carry):
                where = pl.ds(pl.multiple_of(zz * length, length), length)
                angles = (row + (zz * SIDES + y) * length).astype(f32) * inverse
                m.cosine[where, :] = jnp.cos(angles)
                m.sine[where, :] = jnp.sin(angles) * sign
                return carry

            lax.fori_loop(0, nz, table, 0)

    def decays():
        for zz in range(nz):
            take_weights(SMALL, zz)

        @pl.when(is_ret)
        def _():
            lower = (
                lax.broadcasted_iota(jnp.int32, (length, length), 0)
                >= lax.broadcasted_iota(jnp.int32, (length, length), 1)
            )
            lower_float = lower.astype(f32)
            mine = [m.aux[zz * SIDES + y, pl.ds(part_here, 1), :] for zz in range(nz)]
            logs = jnp.concatenate(mine * (8 // nz), axis=0)
            by_row = dot_nt(logs, lower_float, precision=lax.Precision.HIGHEST)
            by_column = dot_nt(lower_float, logs, precision=lax.Precision.HIGHEST)
            for zz in range(nz):
                rows = slice(zz * length, (zz + 1) * length)
                column = by_column[:, zz : zz + 1]
                closing = by_column[length - 1 : length, zz : zz + 1]
                within = jnp.minimum(column - by_row[zz : zz + 1, :], 0.0)
                m.decay[rows, :] = jnp.where(lower, jnp.exp(within), 0.0)
                m.fade_q[rows, :] = jnp.broadcast_to(jnp.exp(column), (length, key_size))
                m.fade_k[rows, :] = jnp.broadcast_to(jnp.exp(closing - column), (length, key_size))

    def run_rows(zz):
        return pl.ds(pl.multiple_of(zz * length, length), length)

    def take_tokens(step):
        origin = toward(step)
        for side in (x, nx):
            await_recv(token_core(origin, side, nc))

    def out_x(step, side):
        columns = out_columns(toward(step), side)
        return remote(
            m.out_w.at[:, columns],
            m.out_wx.at[:, columns],
            m.ox_s.at[0],
            m.ox_r.at[step, side],
            device(z, y, nx, c),
        )

    def out_y(step, arrival):
        piece = m.out_w.at[:, out_columns(toward(step), y)]
        return remote(piece, piece, m.f_s.at[OUT, toward(step)], arrival, device(z, ny, x, c))

    fresh = set()

    def project(step, run):
        columns = pl.ds(pl.multiple_of(toward(step) * SIDES * depth, SIDES * depth), SIDES * depth)
        rows = run_rows(toward(run))
        first = run not in fresh
        fresh.add(run)

        def accumulate(held):
            lanes = slice(0, held.shape[1])
            product = dot_nn(m.tok[rows, columns], held[columns, :])
            m.total[rows, lanes] = product if first else m.total[rows, lanes] + product

        pl.when(is_ret)(lambda: accumulate(m.ret_w))
        pl.when(is_att)(lambda: accumulate(m.att_w))

    everyone = dict(a=None, o=outer, i=inside)
    sent = {}
    def perform(word):
        step = int(word[1]) if len(word) > 1 else 0
        if word[0] == "s":
            for kind in range(SHARES):
                sent[word, kind] = send_weights(step, kind, everyone[word[2]])
        elif word[0] == "f":
            for kind in range(SHARES):
                finish(sent["s" + word[1:], kind])
        elif word[0] == "p":
            for kind in range(SHARES):
                pass_weights(kind, step)
        elif word[0] == "S":
            sent[word] = send_weights(step, OUT, everyone[word[2]])
        elif word[0] == "P":
            pass_weights(OUT, step)
        elif word[0] == "t":
            pass_tokens(step)
        elif word[0] == "x":
            across_tokens(step)
        elif word[0] == "r":
            out_y(step, m.w_r.at[OUT, toward(step)]).wait_recv()
        elif word[0] == "y":
            out_y(step, m.f_r.at[OUT, toward(step)]).start()
        elif word[0] == "u":
            out_x(step, y).start()
        elif word[0] == "v":
            take_weights(OUT, toward(step))
            out_x(step, ny).start()
        elif word[0] == "c":
            take_tokens(step)
        elif word[0] == "k":
            for kind in range(SHARES):
                take_weights(kind, toward(step))
        elif word[0] == "m":
            project(step, int(word[2]))
        elif word[0] == "T":
            tables()
        elif word[0] == "D":
            decays()
        elif word[0] == "a":
            for aux_step in range(nz):
                pass_weights(SMALL, aux_step)

    for word in ORDER:
        perform(word)

    def state_copy(zz):
        piece = m.states.at[zz, y]
        return remote(piece, piece, m.s_s.at[zz], m.s_r.at[zz], device(z, ny, x, c))

    def state_arrival(zz):
        piece = m.states.at[zz, ny]
        return remote(piece, piece, m.s_s.at[zz], m.s_r.at[zz], device(z, ny, x, c))

    halo_copy = remote(m.rim, m.halo, m.h_s.at[0], m.h_r.at[0], device(z, ny, x, c))

    @pl.when(is_ret)
    def _():
        def project_run(zz, carry):
            rows = run_rows(zz)
            product = m.total[rows, :].astype(bf)
            cosine, sine = m.cosine[rows, :], m.sine[rows, :]

            def turn(values):
                values = values.astype(f32)
                return values * cosine + pltpu.roll(values, key_size // 2, 1) * sine

            m.queries[rows, 0:key_size] = turn(product[:, 0:key_size]).astype(bf)
            key = (turn(product[:, key_size : 2 * key_size]) * key_size ** (-0.5)).astype(bf)
            m.keys[rows, :] = key
            value = product[:, 2 * key_size :]
            m.values[rows, :] = value
            faded = (key.astype(f32) * m.fade_k[rows, :]).astype(bf)
            m.states[zz, y] = dot_tn(faded, value).astype(bf)
            state_copy(zz).start()
            return carry

        lax.fori_loop(0, nz, project_run, 0)

    lane_kv = lax.broadcasted_iota(jnp.int32, (WINDOW, 2 * HEAD_DIM), 1)

    def place(zz, spot, packed):
        where = pl.ds(spot * WINDOW, WINDOW)
        packed = packed.astype(f32)
        low = jnp.where(lane_kv < HEAD_DIM, packed, 0.0)
        turned = pltpu.roll(packed, HEAD_DIM, 1)
        m.kv[0, zz, where, :] = low.astype(bf)
        m.kv[1, zz, where, :] = pltpu.roll(low, HEAD_DIM, 1).astype(bf)
        m.kv[2, zz, where, :] = jnp.where(lane_kv < HEAD_DIM, turned, 1.0).astype(bf)
        m.kv[3, zz, where, :] = jnp.where(lane_kv < HEAD_DIM, 1.0, packed).astype(bf)

    @pl.when(is_att)
    def _():
        def project_run(zz, carry):
            rows = run_rows(zz)
            product = m.total[rows, 0 : m.att_w.shape[1]].astype(bf)
            m.queries[rows, :] = (product[:, 0:V_DIM].astype(f32) * HEAD_DIM ** (-0.5)).astype(bf)
            for spot in range(2):
                place(zz, spot + 1, product[spot * WINDOW : (spot + 1) * WINDOW, V_DIM:])
            m.rim[zz] = product[length - WINDOW :, V_DIM:]
            return carry

        lax.fori_loop(0, nz, project_run, 0)
        halo_copy.start()

    far = jnp.where(z < PAIR, nz - 1, 0)

    def home(turn):
        near = far + jnp.where(z < PAIR, -1, 1)
        if isinstance(turn, int):
            return (far, near, mate, z)[turn]
        return jnp.where(turn == 0, far, jnp.where(turn == 1, near, jnp.where(turn == 2, mate, z)))

    def core_copy(piece):
        return remote(
            m.core_out.at[piece], m.core_in.at[piece], m.rc_s.at[0], m.rc_r.at[piece], device(z, y, x, nc)
        )

    def mix_copy(turn):
        return remote(
            m.mixes.at[0, turn], m.mix_in.at[turn], m.rx_s.at[0], m.rx_r.at[turn], device(z, y, nx, c)
        )

    def z_copy(turn, piece, target_z, slot):
        spot = toward(piece)
        return remote(
            m.z_out.at[turn, spot],
            m.z_in.at[slot, spot],
            m.rz_s.at[spot, turn],
            m.rz_r.at[slot, spot],
            device(target_z, y, x, c),
        )

    def half_rows(turn, cc):
        return pl.ds(pl.multiple_of(turn * WINDOW + cc * count, count), count)

    def slab_columns(piece):
        return pl.ds(pl.multiple_of(toward(piece) * slab, slab), slab)

    def block_rows(zz, xx):
        return pl.ds(pl.multiple_of(zz * length + xx * WINDOW, WINDOW), WINDOW)

    def take_out(piece):
        for side in (y, ny):
            out_x(piece, side).wait_recv()

    def emit(piece):
        columns = slab_columns(piece)
        rows = nz * WINDOW
        m.part[...] = dot_nn(m.mixes[1].reshape(rows, V_DIM), m.out_w[:, columns]) + dot_nn(
            m.mix_in[...].reshape(rows, V_DIM), m.out_wx[:, columns]
        )
        for turn in range(nz):
            m.core_out[piece, turn] = m.part[half_rows(turn, nc), :].astype(bf)
        core_copy(piece).start()
        for turn in range(nz):
            m.keep[piece, turn] = m.part[half_rows(turn, c), :]

    def joined(turn, piece):
        return m.keep[piece, turn] + m.core_in[piece, turn].astype(f32)

    def pass_sum(turn, piece):
        m.z_out[turn, toward(piece)] = joined(turn, piece).astype(bf)
        z_copy(turn, piece, mate, turn).start()

    def merge_sum(turn, piece):
        z_copy(turn, piece, mate, turn).wait_recv()
        merged = joined(turn, piece) + m.z_in[turn, toward(piece)].astype(f32)
        m.z_out[turn, toward(piece)] = merged.astype(bf)
        z_copy(turn, piece, home(turn), nz - 1).start()

    def between():
        for word in DURING:
            perform(word)

    for word in AFTER:
        perform(word)

    @pl.when(is_ret)
    def _():
        def inner_run(zz, carry):
            rows = run_rows(zz)
            scores = dot_nt(m.queries[rows, 0:key_size], m.keys[rows, :]) * m.decay[rows, :]
            m.inner[rows, :] = dot_nn(scores.astype(bf), m.values[rows, :])
            return carry

        lax.fori_loop(0, nz, inner_run, 0)
        totals = [
            jnp.sum(m.aux[spot, pl.ds(part_here, 1), :], axis=1, keepdims=True) for spot in range(n)
        ]
        for zz in range(nz):
            state_arrival(zz).wait_recv()
        running = jnp.zeros((key_size, V_DIM), f32)
        for zz in range(nz):
            for yy in range(SIDES):
                m.before[zz, yy] = running
                running = running * jnp.exp(totals[zz * SIDES + yy]) + m.states[zz, yy].astype(f32)

        def finish_block(zz, xx):
            rows = block_rows(zz, xx)
            query = (m.queries[rows, 0:key_size].astype(f32) * m.fade_q[rows, :]).astype(bf)
            state = m.before[zz, y]
            high = state.astype(bf)
            low = (state - high.astype(f32)).astype(bf)
            total = m.inner[rows, :] + (dot_nn(query, high) + dot_nn(query, low))
            total = total * lax.rsqrt(jnp.mean(total * total, axis=-1, keepdims=True) + epsilon)
            return total.astype(bf)

        for turn in range(nz):
            m.mixes[0, turn] = finish_block(home(turn), nx)
            mix_copy(turn).start()
        between()
        for turn in range(nz):
            m.mixes[1, turn] = finish_block(home(turn), x)
        for zz in range(nz):
            state_copy(zz).wait_send()

    @pl.when(is_att)
    def _():
        row = lax.broadcasted_iota(jnp.int32, (WINDOW, 2 * WINDOW), 0)
        column = lax.broadcasted_iota(jnp.int32, (WINDOW, 2 * WINDOW), 1)
        band = (column > row) & (column <= row + WINDOW)
        m.bias[0] = jnp.where(band & (column >= WINDOW), 0.0, masked_out)
        m.bias[1] = jnp.where(band, 0.0, masked_out)
        sink_row = m.aux[sp, parts : parts + 1, 0:LANES]
        sink_lane = lax.broadcasted_iota(jnp.int32, (1, LANES), 1)
        heads = V_DIM // HEAD_DIM
        sinks = [
            jnp.sum(
                jnp.where(sink_lane == part_here * heads + head, sink_row, 0.0), axis=1, keepdims=True
            )
            for head in range(heads)
        ]
        def take_halo():
            halo_copy.wait_recv()
            for zz in range(nz):
                place(zz, 0, m.halo[jnp.maximum(zz - 1 + y, 0)])

        def attend_block(turn, xx):
            zz, slot = home(turn), x if xx == 1 else nx
            bias = m.bias[jnp.minimum(zz + y + xx, 1)]
            where = pl.ds(xx * WINDOW, 2 * WINDOW)
            rows = block_rows(zz, xx)
            first = lane_kv < HEAD_DIM
            for pair in range(heads // 2):
                lanes = slice(pair * LANES, (pair + 1) * LANES)
                query = m.queries[rows, lanes]
                terms, ends = [], []
                for side in range(2):
                    sink = sinks[pair * 2 + side]
                    scores = dot_nt(query, m.kv[side, zz, where, :]) + bias
                    highest = jnp.maximum(jnp.max(scores, axis=-1, keepdims=True), sink)
                    lifted = jnp.exp(scores - highest).astype(bf)
                    ends.append(jnp.exp(sink - highest))
                    terms.append(dot_nn(lifted, m.kv[2 + side, zz, where, :]))
                below = pltpu.roll(jnp.where(first, terms[1], terms[0]), HEAD_DIM, 1)
                below = below + jnp.where(first, ends[0], ends[1])
                mixed = jnp.where(first, terms[0], terms[1]) / below
                m.mixes[slot, turn, :, lanes] = mixed.astype(bf)
            pl.when(x != xx)(mix_copy(turn).start)

        for turn in range(nz):
            attend_block(turn, 1)
        take_halo()
        between()
        for turn in range(nz):
            attend_block(turn, 0)
        halo_copy.wait_send()

    def merge_sums(piece):
        for turn in range(PAIR):
            merge_sum(turn, piece)

    def crossing(piece, before=None):
        def paced():
            if before is not None:
                sent(before)
            for turn in range(PAIR):
                pass_sum(turn, piece)

        core_copy(piece).wait_recv()
        pl.when(outer)(paced)

    def sent(piece):
        for turn in range(PAIR):
            z_copy(turn, piece, mate, turn).wait_send()

    def staying(piece):
        pass_sum(nz - 2, piece)

    def second_round(piece):
        pl.when(inside)(functools.partial(merge_sums, piece))

    def make(piece):
        take_out(piece)
        emit(piece)

    for turn in range(nz):
        mix_copy(turn).wait_recv()
    for word in MIXED:
        perform(word)
    make(0)
    make(1)
    crossing(0)
    for piece in range(1, nz):
        crossing(piece, piece - 1)
        pl.when(inside)(functools.partial(staying, piece - 1))
        second_round(piece - 1)
        if piece + 1 < nz:
            make(piece + 1)

    def last_sums():
        sent(nz - 1)
        for piece in range(nz):
            staying(piece)

    pl.when(outer)(last_sums)
    pl.when(inside)(functools.partial(staying, nz - 1))
    second_round(nz - 1)
    for piece in range(nz):
        total = joined(nz - 1, piece)
        for slot in (nz - 2, nz - 1):
            z_copy(0, piece, mate, slot).wait_recv()
            total = total + m.z_in[slot, toward(piece)].astype(f32)
        columns = slab_columns(piece)
        m.result[:, columns] = total.astype(bf)
        pltpu.make_async_copy(m.result.at[:, columns], out_ref.at[:, columns], m.store.at[0]).start()

    for step in range(PAIR, nz):
        out_y(step, m.f_r.at[OUT, toward(step)]).wait_send()
    for copy, condition in started:
        if condition is None:
            copy.wait_send()
        else:
            pl.when(condition)(copy.wait_send)
    everything = device(z, y, x, nc)
    remote(m.core_out, m.core_in, m.rc_s.at[0], m.rc_r.at[0], everything).wait_send()
    remote(m.mixes.at[0], m.mix_in, m.rx_s.at[0], m.rx_r.at[0], everything).wait_send()
    remote(m.out_w, m.out_wx, m.ox_s.at[0], m.ox_r.at[0, 0], everything).wait_send()
    for piece in range(nz):
        pl.when(inside)(functools.partial(sent, piece))
        z_copy(nz - 2, piece, mate, nz - 2).wait_send()
    pltpu.make_async_copy(m.result, out_ref, m.store.at[0]).wait()


def layer(n, n_tp, tokens, norm_gain, logs, sinks, *weights):
    count, features = tokens.shape
    depth = weights[0].shape[0]
    width = weights[-1].shape[1]
    scratch = layer_scratch(n, n_tp, count, features, depth, width)
    return pl.pallas_call(
        functools.partial(layer_kernel, n, n_tp, tuple(scratch)),
        out_shape=jax.ShapeDtypeStruct((count, n * width), jnp.bfloat16),
        in_specs=[pl.BlockSpec(memory_space=pltpu.HBM)] * (4 + len(weights)),
        out_specs=pl.BlockSpec(memory_space=pltpu.HBM),
        scratch_shapes=list(scratch.values()),
        compiler_params=pltpu.CompilerParams(
            collective_id=3, has_side_effects=True, vmem_limit_bytes=60 * 2**20
        ),
        cost_estimate=pl.CostEstimate(flops=4 * 2**30, bytes_accessed=16 * 2**20, transcendentals=0),
        name="layer",
    )(tokens, norm_gain.reshape(1, -1), logs, sinks.reshape(1, -1), *weights)


def on_device(
    tokens,
    norm_gain,
    ret_query,
    ret_key,
    ret_value,
    log_decay,
    att_query,
    att_key,
    att_value,
    sink_logits,
    ret_out,
    att_out,
):
    n, n_tp = lax.axis_size("sp"), lax.axis_size("tp")
    length = log_decay.shape[1]
    shapes = (
        tokens.shape[0],
        log_decay.shape[0],
        sink_logits.shape[0],
        att_key.shape[1] // HEAD_DIM,
        length,
    )
    if layer_fits(n, n_tp, shapes):
        return layer(
            n, n_tp, tokens, norm_gain, log_decay, sink_logits,
            ret_query, ret_key, ret_value, att_query, att_key.T, att_value.T, ret_out, att_out,
        )
    tok_float = tokens.astype(jnp.float32)
    normed = (
        tok_float
        * lax.rsqrt(jnp.mean(tok_float * tok_float, axis=-1, keepdims=True) + epsilon)
        * norm_gain
    ).astype(jnp.bfloat16)
    weights = (ret_query, ret_key, ret_value, att_query, att_key, att_value)
    widths = [weight.shape[1] for weight in weights]
    points = [sum(widths[:index]) for index in range(1, len(widths))]
    aligned = ret_out.shape[1] % LANES == 0
    local_logs = jnp.sum(log_decay, axis=1)
    log_tile = jnp.broadcast_to(
        jnp.pad(local_logs, (0, -local_logs.shape[0] % 8))[:, None], (-(-local_logs.shape[0] // 8) * 8, LANES)
    )
    projected, logs = project(normed, jnp.concatenate(weights, axis=1), log_tile, n, n_tp)
    logs = logs[:, : local_logs.shape[0], 0]
    sections = jnp.split(projected, points, axis=1)
    tok_count = sections[0].shape[0]
    anchor = lax.axis_index("sp") * tok_count
    positions = anchor + jnp.arange(tok_count, dtype=jnp.int32)
    query_ret = rotate(sections[0].reshape(tok_count, -1, RETAIN_KEY_SIZE), positions).astype(
        jnp.bfloat16
    )
    key_ret = (
        rotate(sections[1].reshape(tok_count, -1, RETAIN_KEY_SIZE), positions)
        * RETAIN_KEY_SIZE ** (-0.5)
    ).astype(jnp.bfloat16)
    value_ret = sections[2].reshape(tok_count, -1, V_DIM)
    stacked = projected[:, points[3] :]
    ret_mix, rim, wholes = retention_path(
        query_ret,
        key_ret,
        value_ret,
        log_decay,
        stacked[tok_count - WINDOW :],
        logs,
        (ret_out, att_out) if aligned else (),
    )
    if not aligned:
        wholes = [
            lax.all_gather(weight, "sp", axis=1, tiled=True)[None] for weight in (ret_out, att_out)
        ]
    att_mix = attention_path(sections[3], stacked, rim, sink_logits, anchor)
    return merge((ret_mix, att_mix), wholes, n_tp)


def solution(mesh):
    in_specs = (
        P(("sp", "tp"), None),
        P(),
        P("sp", "tp"),
        P("sp", "tp"),
        P("sp", "tp"),
        P("tp", "sp"),
        P("sp", "tp"),
        P("sp", "tp"),
        P("sp", "tp"),
        P("tp"),
        P("tp", "sp"),
        P("tp", "sp"),
    )
    out_specs = P(("sp", "tp"), None)
    return jax.shard_map(
        on_device, mesh=mesh, in_specs=in_specs, out_specs=out_specs, check_vma=False
    )
```
